512 devices in a mesh: sp: 32 (over z, core), tp: 16 (over y, x).
Axes of the slice: x: 4, y: 4, z: 16, core: 2. Of those that a mesh axis runs over, the one named last changes fastest.
Arguments:
- residual: bfloat16 [8192, 2048], P('sp'), may hold values from -6 to 6
- queries: bfloat16 [8192, 16, 128], P('sp', 'tp'), may hold values from -256 to 256
- key_vectors: bfloat16 [8192, 16, 128], P('sp', 'tp'), may hold values from -5.3 to 5.3
- value_rows: bfloat16 [8192, 16, 128], P('sp', 'tp'), may hold values from -6 to 6
- head_lambda: float32 [16], P('tp'), may hold values from 0.3 to 0.8
- head_gain: float32 [128], replicated, may hold values from 0.1 to 1.9
- out_weight: bfloat16 [2048, 2048], P('tp'), may hold values from -0.125 to 0.125
- ffn_gain: float32 [2048], replicated, may hold values from 0.1 to 1.9
- expert_gate: bfloat16 [32, 2048, 4096], P('sp', None, 'tp'), may hold values from -0.125 to 0.125
- expert_up: bfloat16 [32, 2048, 4096], P('sp', None, 'tp'), may hold values from -0.125 to 0.125
- expert_down: bfloat16 [32, 4096, 2048], P('sp', None, 'tp'), may hold values from -0.09375 to 0.09375
- routing: int32 [8192, 2], P('sp'), may hold values from 0 to 31, as said below
- route_weight: float32 [8192, 2], P('sp'), may hold values from 0.1 to 0.9
Outputs:
- layer_out: bfloat16 [8192, 2048], P('sp')
The draws below stay inside these ranges and needn't reach their ends.
Inputs may be any that keep to these rules, and one draw needn't show every extreme that they name: `routing`: each row names two different experts of one group of 8 consecutive experts. In each aligned block of 256 rows no expert is named by more than 32 rows, and in every block some expert is named by exactly 32 rows.
All inputs are finite; a program needn't handle non-finite values.
Results may differ from the reference program's by a relative error of at most 0.015.
Values may be sent and summed in bfloat16 or wider, within the bound.
No kernel may reach another device: no remote copies, remote signals or barrier semaphores. Data moves between devices by JAX's collectives and lax.ppermute only.
A program may use at most 64 MiB of HBM per device.

```python
import math
import jax
import jax.numpy as jnp
from jax import lax

D = 2048
HEADS = 16
QK = 64
HV = 128
FF = 4096
GROUPS = 4
TOP = 2
T_SP = 256
SEQ = 8192
EXPERTS = 32
CAP = 32
N_SP = 32


def drawn(key):
    spread = 1.3
    base_key, query_key = jax.random.split(jax.random.fold_in(key, 5), 2)
    width = 2 * QK
    key_array = spread * jax.random.truncated_normal(base_key, -4.0, 4.0, (SEQ, HEADS, width), jnp.float32)
    query_array = spread * jax.random.truncated_normal(query_key, -4.0, 4.0, (SEQ, HEADS, width), jnp.float32)
    return (query_array, key_array)


def draw_queries(key, part):
    return drawn(key)[0].astype(jnp.bfloat16)


def draw_key_vectors(key, part):
    return drawn(key)[1].astype(jnp.bfloat16)


def draw_routing(key, part):
    per_group = EXPERTS // GROUPS
    block_count = SEQ // T_SP
    order_key, inner_key, rank_key = jax.random.split(jax.random.fold_in(key, 11), 3)
    group_order = jax.random.permutation(order_key, GROUPS).astype(jnp.int32)
    inner_order = jax.vmap(lambda sub_key: jax.random.permutation(sub_key, per_group))(jax.random.split(inner_key, GROUPS)).astype(jnp.int32)
    rank_table = jax.vmap(lambda sub_key: jax.random.permutation(sub_key, T_SP))(jax.random.split(rank_key, block_count)).astype(jnp.int32).reshape(-1)
    half_mark = T_SP // 2
    rank_level = (rank_table >= half_mark).astype(jnp.int32) + (rank_table >= half_mark + T_SP // 4).astype(jnp.int32) + (rank_table >= half_mark + T_SP // 4 + T_SP // 8).astype(jnp.int32)
    offsets = jnp.array([0, T_SP // 2, 3 * T_SP // 4, 7 * T_SP // 8], jnp.int32)
    within = rank_table - offsets[rank_level]
    first_pick = within % per_group
    step_size = 1 + within // per_group % max(per_group - 1, 1)
    second_pick = (first_pick + step_size) % per_group
    group_id = group_order[rank_level]
    first_expert = group_id * per_group + inner_order[group_id, first_pick]
    second_expert = group_id * per_group + inner_order[group_id, second_pick]
    return jnp.stack([first_expert, second_expert], axis=1).astype(jnp.int32)


def block_levels(rng, shape, shards, least, high):
    loudness = 1.0
    for axis_at, parts in shards:
        draws = jax.random.uniform(jax.random.fold_in(jax.random.fold_in(rng, 6), axis_at), (parts,), jnp.float32, least / len(shards), high / len(shards))
        loudness = loudness * jnp.repeat(jnp.exp(draws), shape[axis_at] // parts).reshape((-1,) + (1,) * (len(shape) - 1 - axis_at))
    return loudness


def scatter_about(rng, extent, scale, most, cuts=(), held_as=jnp.bfloat16):
    level = block_levels(rng, extent, cuts, -0.22, 0.18) if cuts else 1.0
    drawn = jax.random.normal(rng, extent, jnp.float32) * scale * level
    return jnp.minimum(jnp.maximum(drawn, -most), most).astype(held_as)


def setup_inputs(seed: int = 0) -> dict:
    keys = jax.random.split(jax.random.key(seed), 14)
    residual = scatter_about(keys[0], (SEQ, D), 1.0, 6.0, ((0, 32),))
    queries = draw_queries(jax.random.fold_in(keys[13], 71), 0)
    key_vectors = draw_key_vectors(jax.random.fold_in(keys[13], 71), 0)
    value_rows = scatter_about(keys[3], (SEQ, HEADS, HV), 1.0, 6.0, ((0, 32), (1, 16)))
    head_lambda = jnp.clip(0.3 + 0.5 * jax.random.uniform(keys[4], (HEADS,), jnp.float32) ** block_levels(keys[4], (HEADS,), ((0, 16),), -0.2, 0.2), 0.3, 0.8)
    head_gain = jnp.clip(1.0 + 0.18 * jax.random.normal(keys[5], (HV,), jnp.float32), 0.1, 1.9)
    out_weight = scatter_about(keys[6], (HEADS * HV, D), (HEADS * HV) ** -0.5, 0.125, ((0, 16),))
    ffn_gain = jnp.clip(1.0 + 0.18 * jax.random.normal(keys[7], (D,), jnp.float32), 0.1, 1.9)
    expert_gate = scatter_about(keys[8], (EXPERTS, D, FF), D ** -0.5, 0.125, ((0, 32), (2, 16)))
    expert_up = scatter_about(keys[9], (EXPERTS, D, FF), D ** -0.5, 0.125, ((0, 32), (2, 16)))
    expert_down = scatter_about(keys[10], (EXPERTS, FF, D), FF ** -0.5, 0.09375, ((0, 32), (2, 16)))
    routing = draw_routing(jax.random.fold_in(keys[13], 71), 0)
    route_weight = jnp.clip(0.1 + 0.79999997 * jax.random.uniform(keys[12], (SEQ, TOP), jnp.float32) ** block_levels(keys[12], (SEQ, TOP), ((0, 32),), -0.2, 0.2), 0.1, 0.9)
    return {"residual": residual, "queries": queries, "key_vectors": key_vectors, "value_rows": value_rows, "head_lambda": head_lambda, "head_gain": head_gain, "out_weight": out_weight, "ffn_gain": ffn_gain, "expert_gate": expert_gate, "expert_up": expert_up, "expert_down": expert_down, "routing": routing, "route_weight": route_weight}


norm_eps = 1e-06

def differential(queries, key_vectors, value_rows, head_lambda, head_gain):
    seq_len = queries.shape[0]
    block_len = math.gcd(seq_len, 512)
    score_scale = QK ** (-0.5)
    key_float = key_vectors.astype(jnp.float32)
    value_float = value_rows.astype(jnp.float32)
    key_pos = jnp.arange(seq_len, dtype=jnp.int32)

    def one_map(query_part, key_part, query_pos):
        scores = jnp.einsum('qhd,khd->hqk', query_part, key_part) * score_scale
        masked = jnp.where(key_pos[None, None, :] <= query_pos[None, :, None], scores, -jnp.inf)
        highest = lax.optimization_barrier(jnp.max(masked, axis=-1, keepdims=True))
        weights = jnp.exp(masked - highest)
        totals = lax.optimization_barrier(jnp.sum(weights, axis=-1))
        rounded = lax.optimization_barrier(weights.astype(jnp.bfloat16)).astype(jnp.float32)
        blended = jnp.einsum('hqk,khe->qhe', rounded, value_float)
        return blended / jnp.transpose(totals)[:, :, None]

    def one_block(block_index):
        first_row = block_index * block_len
        query_rows = lax.dynamic_slice_in_dim(queries, first_row, block_len, 0).astype(jnp.float32)
        query_pos = first_row + jnp.arange(block_len, dtype=jnp.int32)
        first_map = one_map(query_rows[:, :, :QK], key_float[:, :, :QK], query_pos)
        second_map = one_map(query_rows[:, :, QK:], key_float[:, :, QK:], query_pos)
        return first_map - head_lambda[None, :, None] * second_map
    blocks_out = lax.map(one_block, jnp.arange(seq_len // block_len, dtype=jnp.int32))
    combined = blocks_out.reshape(seq_len, HEADS, HV)
    normed = combined * lax.rsqrt(lax.optimization_barrier(jnp.mean(combined * combined, axis=-1, keepdims=True)) + norm_eps) * head_gain
    return normed.astype(jnp.bfloat16).reshape(seq_len, HEADS * HV)

def reference(residual, queries, key_vectors, value_rows, head_lambda, head_gain, out_weight, ffn_gain, expert_gate, expert_up, expert_down, routing, route_weight):
    attended = differential(queries, key_vectors, value_rows, head_lambda, head_gain)
    stream = residual.astype(jnp.float32) + jnp.dot(attended, out_weight, preferred_element_type=jnp.float32)
    normed = (stream * lax.rsqrt(lax.optimization_barrier(jnp.mean(stream * stream, axis=-1, keepdims=True)) + norm_eps) * ffn_gain).astype(jnp.bfloat16)
    slot_count = N_SP * CAP

    def expert_step(totals, stacked):
        gate_weight, up_weight, down_weight, expert_id = stacked
        chosen = jnp.any(routing == expert_id, axis=1)
        token_ids = jnp.nonzero(chosen, size=slot_count, fill_value=0)[0].astype(jnp.int32)
        live_slot = jnp.arange(slot_count, dtype=jnp.int32) < jnp.sum(chosen.astype(jnp.int32))
        picked = normed[token_ids]
        gate_part = jnp.dot(picked, gate_weight, preferred_element_type=jnp.float32)
        up_part = jnp.dot(picked, up_weight, preferred_element_type=jnp.float32)
        inner_act = (jax.nn.silu(gate_part) * up_part).astype(jnp.bfloat16)
        result = jnp.dot(inner_act, down_weight, preferred_element_type=jnp.float32).astype(jnp.bfloat16)
        factor = lax.optimization_barrier(jnp.sum(jnp.where(routing[token_ids] == expert_id, route_weight[token_ids], jnp.zeros_like(route_weight[token_ids])), axis=1))
        factor = jnp.where(live_slot, factor, jnp.zeros_like(factor))
        return (totals.at[token_ids].add(factor[:, None] * result.astype(jnp.float32)), None)
    moe_sum, _ = lax.scan(expert_step, jnp.zeros((SEQ, D), jnp.float32), (expert_gate, expert_up, expert_down, jnp.arange(EXPERTS, dtype=jnp.int32)))
    return (stream + moe_sum).astype(jnp.bfloat16)
```

```python
import jax
import jax.numpy as jnp
from jax import lax
from jax.experimental import pallas as pl
from jax.experimental.pallas import tpu as pltpu
from jax.sharding import PartitionSpec as P

norm_eps = 1e-06
KEY_BLOCK = 1024
GROUPS = 4


def attention_body(where_ref, lam_ref, q_ref, kv_ref, gain_ref, out_ref, stacked, highest, accum):
    step = pl.program_id(0)
    tok = q_ref.shape[0]
    width = q_ref.shape[1]
    first_query = where_ref[0] * tok
    last_step = (first_query + tok - 1) // KEY_BLOCK

    @pl.when(step == 0)
    def _():
        scaled = q_ref[...] * jnp.asarray((width // 2) ** -0.5, jnp.bfloat16)
        low = lax.broadcasted_iota(jnp.int32, scaled.shape, 1) < width // 2
        zero = jnp.zeros_like(scaled)
        stacked[:tok] = jnp.where(low, scaled, zero)
        stacked[tok:] = jnp.where(low, zero, scaled)
        highest[...] = jnp.full(highest.shape, -1e30, jnp.float32)
        accum[...] = jnp.zeros(accum.shape, jnp.float32)

    def update(masked):
        values = kv_ref[1]
        scores = lax.dot_general(
            stacked[...], kv_ref[0], (((1,), (1,)), ((), ())), preferred_element_type=jnp.float32
        )
        if masked:
            row = lax.broadcasted_iota(jnp.int32, scores.shape, 0)
            col = lax.broadcasted_iota(jnp.int32, scores.shape, 1)
            limit = jnp.where(row >= tok, row - tok, row) + (first_query - step * KEY_BLOCK)
            scores = jnp.where(col <= limit, scores, -1e30)
        before = highest[...]
        now = jnp.maximum(before, jnp.max(scores, axis=1, keepdims=True))
        weights = jnp.exp(scores - now[:, :1])
        shrink = jnp.exp(before - now)[:, :1]
        wide = jnp.concatenate([values, jnp.ones_like(values)], axis=1)
        blended = jnp.dot(weights.astype(jnp.bfloat16), wide, preferred_element_type=jnp.float32)
        accum[...] = accum[...] * shrink + blended
        highest[...] = now

    @pl.when(step < last_step)
    def _():
        update(False)

    @pl.when(step == last_step)
    def _():
        update(True)
        both = accum[:, :width] / accum[:, width:]
        combined = both[:tok] - lam_ref[0] * both[tok:]
        square = jnp.mean(combined * combined, axis=1, keepdims=True)
        out_ref[...] = (combined * lax.rsqrt(square + norm_eps) * gain_ref[...]).astype(jnp.bfloat16)


def attention(where, lam, q, kv, gain):
    tok, width = q.shape
    steps = kv.shape[1] // KEY_BLOCK

    def kv_at(j, where_ref, lam_ref):
        return (0, jnp.minimum(j, (where_ref[0] * tok + tok - 1) // KEY_BLOCK), 0)

    def fixed(j, where_ref, lam_ref):
        return (0, 0)

    grid = pltpu.PrefetchScalarGridSpec(
        num_scalar_prefetch=2,
        grid=(steps,),
        in_specs=[
            pl.BlockSpec((tok, width), fixed),
            pl.BlockSpec((2, KEY_BLOCK, width), kv_at),
            pl.BlockSpec((1, width), fixed),
        ],
        out_specs=pl.BlockSpec((tok, width), fixed),
        scratch_shapes=[
            pltpu.VMEM((2 * tok, width), jnp.bfloat16),
            pltpu.VMEM((2 * tok, 128), jnp.float32),
            pltpu.VMEM((2 * tok, 2 * width), jnp.float32),
        ],
    )
    return pl.pallas_call(
        attention_body,
        grid_spec=grid,
        out_shape=jax.ShapeDtypeStruct((tok, width), jnp.bfloat16),
        compiler_params=pltpu.CompilerParams(
            dimension_semantics=("arbitrary",), vmem_limit_bytes=48 * 2**20
        ),
        name="attention",
    )(where, lam, q, kv, gain)


def expert_body(rows_ref, gain_ref, gate_ref, up_ref, down_ref, out_ref):
    rows = rows_ref[...].astype(jnp.float32)
    square = jnp.mean(rows * rows, axis=1, keepdims=True)
    normed = (rows * lax.rsqrt(square + norm_eps) * gain_ref[...]).astype(jnp.bfloat16)
    gate = jnp.dot(normed, gate_ref[...], preferred_element_type=jnp.float32)
    up = jnp.dot(normed, up_ref[...], preferred_element_type=jnp.float32)
    hidden = (gate / (1.0 + jnp.exp(-gate)) * up).astype(jnp.bfloat16)
    peers = out_ref.shape[0]
    share = out_ref.shape[2]
    part = jnp.dot(hidden, down_ref[...], preferred_element_type=jnp.float32).astype(jnp.bfloat16)
    for p in range(peers):
        out_ref[p] = part[:, p * share : (p + 1) * share]


def expert(rows, gain, gate, up, down, peers):
    count, model = rows.shape
    hidden = gate.shape[1]
    share = model // peers
    tile = 256
    return pl.pallas_call(
        expert_body,
        grid=(count // tile,),
        in_specs=[
            pl.BlockSpec((tile, model), lambda i: (i, 0)),
            pl.BlockSpec((1, model), lambda i: (0, 0)),
            pl.BlockSpec((model, hidden), lambda i: (0, 0)),
            pl.BlockSpec((model, hidden), lambda i: (0, 0)),
            pl.BlockSpec((hidden, model), lambda i: (0, 0)),
        ],
        out_specs=pl.BlockSpec((peers, tile, share), lambda i: (0, i, 0)),
        out_shape=jax.ShapeDtypeStruct((peers, count, share), jnp.bfloat16),
        compiler_params=pltpu.CompilerParams(
            dimension_semantics=("arbitrary",), vmem_limit_bytes=48 * 2**20
        ),
        name="expert",
    )(rows, gain, gate, up, down)


def shards(
    residual,
    queries,
    key_vectors,
    value_rows,
    head_lambda,
    head_gain,
    out_weight,
    ffn_gain,
    expert_gate,
    expert_up,
    expert_down,
    routing,
    route_weight,
):
    tok, _, width = queries.shape
    experts = lax.axis_size("sp")
    peers = lax.axis_size("tp")
    model = residual.shape[1]
    share = model // peers
    where = lax.axis_index("sp").astype(jnp.int32)[None]
    column = lax.axis_index("tp") * share
    kv = jnp.stack([key_vectors[:, 0], value_rows[:, 0]])
    kv_all = lax.all_gather(kv, "sp", axis=1, tiled=True)

    out_cols = lax.all_to_all(
        out_weight.reshape(width, peers, share).swapaxes(0, 1), "tp", 0, 0, tiled=True
    ).reshape(peers * width, share)
    hidden = expert_gate.shape[2]
    down_rows = lax.all_to_all(
        expert_down[0].reshape(peers, hidden, share), "tp", 0, 0, tiled=True
    )
    down_rows = down_rows.swapaxes(0, 1).reshape(hidden, model)

    capacity = tok // (experts // GROUPS)
    named = routing[:, :, None] == jnp.arange(experts, dtype=jnp.int32)
    member = jnp.any(named, axis=1)
    order = jnp.arange(tok, dtype=jnp.int32)
    strict = (order[None, :] < order[:, None]).astype(jnp.bfloat16)
    earlier = jnp.dot(
        strict, member.astype(jnp.bfloat16), preferred_element_type=jnp.float32
    ).astype(jnp.int32)
    slot = jnp.arange(capacity, dtype=jnp.int32)
    at_slot = earlier[:, :, None] == slot
    send = (member[:, :, None] & at_slot).reshape(tok, experts * capacity).astype(jnp.bfloat16)
    take = [
        (named[:, k, :, None] & at_slot).reshape(tok, experts * capacity).astype(jnp.bfloat16)
        for k in range(routing.shape[1])
    ]

    attended = attention(where, head_lambda, queries[:, 0], kv_all, head_gain[None])
    heads = lax.all_gather(attended, "tp", axis=1, tiled=True)
    own_stream = lax.dynamic_slice_in_dim(residual, column, share, 1).astype(jnp.float32) + jnp.dot(
        heads, out_cols, preferred_element_type=jnp.float32
    )

    outgoing = lax.dot_general(
        send, own_stream.astype(jnp.bfloat16), (((0,), (0,)), ((), ())),
        preferred_element_type=jnp.float32,
    ).astype(jnp.bfloat16)
    landed = lax.all_to_all(
        outgoing.reshape(experts, capacity, share), "sp", 0, 0, tiled=True
    ).reshape(experts * capacity, share)
    rows = lax.all_gather(landed, "tp", axis=1, tiled=True)
    parts = expert(rows, ffn_gain[None], expert_gate[0], expert_up[0], down_rows, peers)
    expert_out = lax.psum_scatter(parts, "tp", scatter_dimension=0, tiled=True)
    back = lax.all_to_all(
        expert_out.reshape(experts, capacity, share), "sp", 0, 0, tiled=True
    ).reshape(experts * capacity, share)
    moe = sum(
        route_weight[:, k : k + 1] * jnp.dot(take[k], back, preferred_element_type=jnp.float32)
        for k in range(routing.shape[1])
    )
    own_out = (own_stream + moe).astype(jnp.bfloat16)
    return lax.all_gather(own_out, "tp", axis=1, tiled=True)


def solution(mesh):
    in_specs = (
        P("sp", None),
        P("sp", "tp", None),
        P("sp", "tp", None),
        P("sp", "tp", None),
        P("tp"),
        P(),
        P("tp", None),
        P(),
        P("sp", None, "tp"),
        P("sp", None, "tp"),
        P("sp", None, "tp"),
        P("sp", None),
        P("sp", None),
    )
    return jax.shard_map(
        shards, mesh=mesh, in_specs=in_specs, out_specs=P("sp", None), check_vma=False
    )
```

```python
import jax
import jax.numpy as jnp
from jax import lax
from jax.experimental import pallas as pl
from jax.experimental.pallas import tpu as pltpu
from jax.sharding import PartitionSpec as P

norm_eps = 1e-06
KEY_BLOCK = 1024
GROUPS = 4


def attention_body(where_ref, lam_ref, q_ref, kv_ref, gain_ref, out_ref, stacked, highest, accum):
    step = pl.program_id(0)
    tok = q_ref.shape[0]
    width = q_ref.shape[1]
    first_query = where_ref[0] * tok
    last_step = (first_query + tok - 1) // KEY_BLOCK

    @pl.when(step == 0)
    def _():
        scaled = q_ref[...] * jnp.asarray((width // 2) ** -0.5, jnp.bfloat16)
        low = lax.broadcasted_iota(jnp.int32, scaled.shape, 1) < width // 2
        zero = jnp.zeros_like(scaled)
        stacked[:tok] = jnp.where(low, scaled, zero)
        stacked[tok:] = jnp.where(low, zero, scaled)
        highest[...] = jnp.full(highest.shape, -1e30, jnp.float32)
        accum[...] = jnp.zeros(accum.shape, jnp.float32)

    def update(masked):
        values = kv_ref[1]
        scores = lax.dot_general(
            stacked[...], kv_ref[0], (((1,), (1,)), ((), ())), preferred_element_type=jnp.float32
        )
        if masked:
            row = lax.broadcasted_iota(jnp.int32, scores.shape, 0)
            col = lax.broadcasted_iota(jnp.int32, scores.shape, 1)
            limit = jnp.where(row >= tok, row - tok, row) + (first_query - step * KEY_BLOCK)
            scores = jnp.where(col <= limit, scores, -1e30)
        before = highest[...]
        now = jnp.maximum(before, jnp.max(scores, axis=1, keepdims=True))
        weights = jnp.exp(scores - now[:, :1])
        shrink = jnp.exp(before - now)[:, :1]
        wide = jnp.concatenate([values, jnp.ones_like(values)], axis=1)
        blended = jnp.dot(weights.astype(jnp.bfloat16), wide, preferred_element_type=jnp.float32)
        accum[...] = accum[...] * shrink + blended
        highest[...] = now

    @pl.when(step < last_step)
    def _():
        update(False)

    @pl.when(step == last_step)
    def _():
        update(True)
        both = accum[:, :width] / accum[:, width:]
        combined = both[:tok] - lam_ref[0] * both[tok:]
        square = jnp.mean(combined * combined, axis=1, keepdims=True)
        out_ref[...] = (combined * lax.rsqrt(square + norm_eps) * gain_ref[...]).astype(jnp.bfloat16)


def attention(where, lam, q, kv, gain):
    tok, width = q.shape
    steps = kv.shape[1] // KEY_BLOCK

    def kv_at(j, where_ref, lam_ref):
        return (0, jnp.minimum(j, (where_ref[0] * tok + tok - 1) // KEY_BLOCK), 0)

    def fixed(j, where_ref, lam_ref):
        return (0, 0)

    grid = pltpu.PrefetchScalarGridSpec(
        num_scalar_prefetch=2,
        grid=(steps,),
        in_specs=[
            pl.BlockSpec((tok, width), fixed),
            pl.BlockSpec((2, KEY_BLOCK, width), kv_at),
            pl.BlockSpec((1, width), fixed),
        ],
        out_specs=pl.BlockSpec((tok, width), fixed),
        scratch_shapes=[
            pltpu.VMEM((2 * tok, width), jnp.bfloat16),
            pltpu.VMEM((2 * tok, 128), jnp.float32),
            pltpu.VMEM((2 * tok, 2 * width), jnp.float32),
        ],
    )
    return pl.pallas_call(
        attention_body,
        grid_spec=grid,
        out_shape=jax.ShapeDtypeStruct((tok, width), jnp.bfloat16),
        compiler_params=pltpu.CompilerParams(
            dimension_semantics=("arbitrary",), vmem_limit_bytes=24 * 2**20
        ),
        name="attention",
    )(where, lam, q, kv, gain)


def project_body(column_ref, heads_ref, weight_ref, residual_ref, send_ref, stream_ref, out_ref):
    total = residual_ref[...].astype(jnp.float32)
    for p in range(0, heads_ref.shape[0], 2):
        both = jnp.concatenate([heads_ref[p], heads_ref[p + 1]], axis=1)
        rows = jnp.concatenate([weight_ref[p], weight_ref[p + 1]], axis=0)
        total += jnp.dot(both, rows, preferred_element_type=jnp.float32)
    stream_ref[...] = total
    picked = jnp.dot(send_ref[...], total.astype(jnp.bfloat16), preferred_element_type=jnp.float32)
    out_ref[...] = picked.astype(jnp.bfloat16)


def project(column, heads, weight, residual, send):
    peers, tok, width = heads.shape
    share = weight.shape[2]
    slots = send.shape[0]

    def whole(rank):
        return lambda i, column_ref: (0,) * rank

    grid = pltpu.PrefetchScalarGridSpec(
        num_scalar_prefetch=1,
        grid=(1,),
        in_specs=[
            pl.BlockSpec((peers, tok, width), whole(3)),
            pl.BlockSpec((peers, width, share), whole(3)),
            pl.BlockSpec((tok, share), lambda i, column_ref: (0, column_ref[0])),
            pl.BlockSpec((slots, tok), whole(2)),
        ],
        out_specs=[pl.BlockSpec((tok, share), whole(2)), pl.BlockSpec((slots, share), whole(2))],
    )
    return pl.pallas_call(
        project_body,
        grid_spec=grid,
        out_shape=[
            jax.ShapeDtypeStruct((tok, share), jnp.float32),
            jax.ShapeDtypeStruct((slots, share), jnp.bfloat16),
        ],
        compiler_params=pltpu.CompilerParams(vmem_limit_bytes=16 * 2**20),
        name="project",
    )(column, heads, weight, residual, send)


def expert_body(x_ref, rows_ref, gain_ref, *refs):
    pieces = (len(refs) - 4) // 2
    gates, ups, down_ref, out_ref = refs[:pieces], refs[pieces:-4], refs[-4], refs[-3]
    normed_ref, accum = refs[-2:]
    peers, count, share = rows_ref.shape
    hidden = gates[0].shape[1]
    total = jnp.zeros((count, 1), jnp.float32)
    for p in range(peers):
        part = rows_ref[p].astype(jnp.float32)
        total += jnp.sum(part * part, axis=1, keepdims=True)
    scale = lax.rsqrt(total / (peers * share) + norm_eps)
    for p in range(peers):
        cols = slice(p * share, (p + 1) * share)
        normed_ref[:, cols] = (rows_ref[p].astype(jnp.float32) * scale * gain_ref[:, cols]).astype(
            jnp.bfloat16
        )
    for k in range(pieces):
        normed = normed_ref[...]
        gate = jnp.dot(normed, gates[k][...], preferred_element_type=jnp.float32)
        up = jnp.dot(normed, ups[k][...], preferred_element_type=jnp.float32)
        act = (gate / (1.0 + jnp.exp(-gate)) * up).astype(jnp.bfloat16)
        source = lax.rem(x_ref[0] + (pieces - k), pieces)
        down = down_ref[pl.ds(pl.multiple_of(source * hidden, hidden), hidden), :]
        part = jnp.dot(act, down, preferred_element_type=jnp.float32)
        if k == 0:
            accum[...] = part
        elif k < pieces - 1:
            accum[...] += part
        else:
            done = (accum[...] + part).astype(jnp.bfloat16)
            for p in range(peers):
                out_ref[p] = done[:, p * share : (p + 1) * share]


def expert(x, rows, gain, gates, ups, down):
    peers, count, share = rows.shape
    vmem = pl.BlockSpec(memory_space=pltpu.VMEM)
    return pl.pallas_call(
        expert_body,
        in_specs=[pl.BlockSpec(memory_space=pltpu.SMEM)] + [vmem] * (3 + len(gates) + len(ups)),
        out_specs=vmem,
        out_shape=jax.ShapeDtypeStruct((peers, count, share), jnp.bfloat16),
        scratch_shapes=[
            pltpu.VMEM((count, peers * share), jnp.bfloat16),
            pltpu.VMEM((count, peers * share), jnp.float32),
        ],
        compiler_params=pltpu.CompilerParams(vmem_limit_bytes=40 * 2**20),
        name="expert",
    )(x, rows, gain, *gates, *ups, down)


def from_everyone(array, axes):
    peers = lax.axis_size(axes)
    return lax.all_to_all(
        jnp.broadcast_to(array[None], (peers, *array.shape)), axes, 0, 0, tiled=True
    )


def shards(
    residual,
    queries,
    key_vectors,
    value_rows,
    head_lambda,
    head_gain,
    out_weight,
    ffn_gain,
    expert_gate,
    expert_up,
    expert_down,
    routing,
    route_weight,
):
    tok, _, width = queries.shape
    experts = lax.axis_size("sp")
    across = lax.axis_size("x")
    along = lax.axis_size("y")
    peers = across * along
    model = residual.shape[1]
    share = model // peers
    hidden = expert_gate.shape[2]
    where = lax.axis_index("sp").astype(jnp.int32)[None]
    column = (lax.axis_index("y") * across + lax.axis_index("x")).astype(jnp.int32)[None]
    x_at = lax.axis_index("x").astype(jnp.int32)[None]
    kv = jnp.stack([key_vectors[:, 0], value_rows[:, 0]])
    kv_all = lax.all_gather(kv, "sp", axis=1, tiled=True)

    ahead = [(i, (i + 1) % across) for i in range(across)]
    behind = [(i, (i - 1) % across) for i in range(across)]
    gate, up = expert_gate[0], expert_up[0]
    gate_1, up_1 = lax.ppermute(gate, "x", ahead), lax.ppermute(up, "x", ahead)
    gate_3, up_3 = lax.ppermute(gate, "x", behind), lax.ppermute(up, "x", behind)
    gate_2, up_2 = lax.ppermute(gate_1, "x", ahead), lax.ppermute(up_3, "x", behind)
    gates, ups = [gate, gate_1, gate_2, gate_3], [up, up_1, up_2, up_3]

    down = expert_down[0].reshape(along, across * hidden, share)
    down = jnp.broadcast_to(down[:, None], (along, across, across * hidden, share))
    down = lax.all_to_all(
        down.reshape(peers, across * hidden, share), ("y", "x"), 0, 0, tiled=True
    )
    down = down.swapaxes(0, 1).reshape(across * hidden, model)
    out_cols = lax.all_to_all(
        out_weight.reshape(width, peers, share).swapaxes(0, 1), ("y", "x"), 0, 0, tiled=True
    )

    capacity = tok // (experts // GROUPS)
    order = jnp.arange(tok, dtype=jnp.int32)
    ids = jnp.arange(experts, dtype=jnp.int32)
    named = routing[:, :, None] == ids
    member = jnp.any(named, axis=1)
    strict = (order[None, :] < order[:, None]).astype(jnp.bfloat16)
    earlier = jnp.dot(
        strict, member.astype(jnp.bfloat16), preferred_element_type=jnp.float32
    ).astype(jnp.int32)
    slot = jnp.arange(capacity, dtype=jnp.int32)
    send = (member.T[:, None, :] & (earlier.T[:, None, :] == slot[None, :, None])).reshape(
        experts * capacity, tok
    )
    send = send.astype(jnp.bfloat16)
    take = [
        (named[:, k, :, None] & (earlier[:, :, None] == slot))
        .reshape(tok, experts * capacity)
        .astype(jnp.bfloat16)
        for k in range(routing.shape[1])
    ]

    attended = attention(where, head_lambda, queries[:, 0], kv_all, head_gain[None])
    heads = from_everyone(attended, ("y", "x"))
    own_stream, outgoing = project(column, heads, out_cols, residual, send)
    landed = lax.all_to_all(
        outgoing.reshape(experts, capacity, share), "sp", 0, 0, tiled=True
    )
    count = experts * capacity // across
    quarters = jnp.broadcast_to(
        landed.reshape(1, across, count, share), (along, across, count, share)
    )
    rows = lax.all_to_all(quarters.reshape(peers, count, share), ("y", "x"), 0, 0, tiled=True)
    parts = expert(x_at, rows, ffn_gain[None], gates, ups, down)
    arrived = lax.all_to_all(parts, ("y", "x"), 0, 0, tiled=True)
    expert_out = (
        arrived.reshape(along, across * count, share).astype(jnp.float32).sum(axis=0)
    ).astype(jnp.bfloat16)
    back = lax.all_to_all(
        expert_out.reshape(experts, capacity, share), "sp", 0, 0, tiled=True
    ).reshape(experts * capacity, share)
    moe = sum(
        route_weight[:, k : k + 1] * jnp.dot(take[k], back, preferred_element_type=jnp.float32)
        for k in range(routing.shape[1])
    )
    own_out = (own_stream + moe).astype(jnp.bfloat16)
    whole = from_everyone(own_out, ("y", "x"))
    return whole.swapaxes(0, 1).reshape(tok, model)


def solution(mesh):
    sizes = mesh.devices.shape
    y = int(sizes[1] ** 0.5)
    split = jax.sharding.Mesh(
        mesh.devices.reshape(sizes[0], y, sizes[1] // y), ("sp", "y", "x")
    )
    tp = ("y", "x")
    in_specs = (
        P("sp", None),
        P("sp", tp, None),
        P("sp", tp, None),
        P("sp", tp, None),
        P(tp),
        P(),
        P(tp, None),
        P(),
        P("sp", None, tp),
        P("sp", None, tp),
        P("sp", None, tp),
        P("sp", None),
        P("sp", None),
    )
    return jax.shard_map(
        shards, mesh=split, in_specs=in_specs, out_specs=P("sp", None), check_vma=False
    )
```

```python
import jax
import jax.numpy as jnp
from jax import lax
from jax.experimental import pallas as pl
from jax.experimental.pallas import tpu as pltpu
from jax.sharding import PartitionSpec as P

norm_eps = 1e-06
KEY_BLOCK = 2048
ROW_BLOCK = 128
SHIFT = 4096.0
GROUPS = 4


def attention_body(where_ref, lam_ref, q_ref, kv_ref, gain_ref, weight_ref, out_ref, stacked, highest, accum):
    tok, width = q_ref.shape
    first_query = where_ref[0] * tok
    last = (first_query + tok - 1) // KEY_BLOCK
    scaled = q_ref[...] * jnp.asarray((width // 2) ** -0.5, jnp.bfloat16)
    low = lax.broadcasted_iota(jnp.int32, scaled.shape, 1) < width // 2
    zero = jnp.zeros_like(scaled)
    stacked[:tok] = jnp.where(low, scaled, zero)
    stacked[tok:] = jnp.where(low, zero, scaled)
    highest[...] = jnp.full(highest.shape, -1e30, jnp.float32)
    accum[...] = jnp.zeros(accum.shape, jnp.float32)

    def update(step, masked):
        block = kv_ref[pl.ds(pl.multiple_of(step * KEY_BLOCK, KEY_BLOCK), KEY_BLOCK), :]
        keys, values = block[:, :width], block[:, width:]
        wide = jnp.concatenate([values, jnp.ones_like(values)], axis=1)
        for at in range(0, 2 * tok, ROW_BLOCK):
            rows = slice(at, at + ROW_BLOCK)
            scores = lax.dot_general(
                stacked[rows], keys, (((1,), (1,)), ((), ())), preferred_element_type=jnp.float32
            )
            if masked:
                row = lax.broadcasted_iota(jnp.int32, scores.shape, 0) + at % tok
                col = lax.broadcasted_iota(jnp.int32, scores.shape, 1)
                scores = jnp.where(
                    col - row <= first_query - step * KEY_BLOCK, scores, -1e30
                )
            before = highest[rows]
            now = jnp.maximum(before, jnp.max(scores, axis=1, keepdims=True))
            weights = jnp.exp(scores - now[:, :1])
            shrink = jnp.exp(before - now)[:, :1]
            blended = jnp.dot(weights.astype(jnp.bfloat16), wide, preferred_element_type=jnp.float32)
            accum[rows] = accum[rows] * shrink + blended
            highest[rows] = now

    def whole(step, carry):
        update(step, False)
        return carry

    lax.fori_loop(0, last, whole, 0)
    update(last, True)
    both = accum[:, :width] / accum[:, width:]
    combined = both[:tok] - lam_ref[0] * both[tok:]
    square = jnp.mean(combined * combined, axis=1, keepdims=True)
    attended = (combined * lax.rsqrt(square + norm_eps) * gain_ref[...]).astype(jnp.bfloat16)
    part = jnp.dot(attended, weight_ref[...], preferred_element_type=jnp.float32)
    share = out_ref.shape[2]
    for p in range(out_ref.shape[0]):
        out_ref[p] = part[:, p * share : (p + 1) * share].astype(jnp.bfloat16)


def attention(where, lam, q, kv, gain, weight, peers):
    tok, width = q.shape
    share = weight.shape[1] // peers
    vmem = pl.BlockSpec(memory_space=pltpu.VMEM)
    smem = pl.BlockSpec(memory_space=pltpu.SMEM)
    return pl.pallas_call(
        attention_body,
        in_specs=[smem, smem, vmem, vmem, vmem, vmem],
        out_specs=vmem,
        out_shape=jax.ShapeDtypeStruct((peers, tok, share), jnp.bfloat16),
        scratch_shapes=[
            pltpu.VMEM((2 * tok, width), jnp.bfloat16),
            pltpu.VMEM((2 * tok, 128), jnp.float32),
            pltpu.VMEM((2 * tok, 2 * width), jnp.float32),
        ],
        compiler_params=pltpu.CompilerParams(vmem_limit_bytes=24 * 2**20),
        name="attention",
    )(where, lam, q, kv, gain, weight)


def project_body(column_ref, parts_ref, residual_ref, send_ref, stream_ref, out_ref):
    total = residual_ref[...].astype(jnp.float32)
    for p in range(parts_ref.shape[0]):
        total += parts_ref[p].astype(jnp.float32)
    stream_ref[...] = total
    picked = jnp.dot(send_ref[...], total.astype(jnp.bfloat16), preferred_element_type=jnp.float32)
    out_ref[...] = picked.astype(jnp.bfloat16)


def project(column, parts, residual, send):
    peers, tok, share = parts.shape
    slots = send.shape[0]

    def whole(rank):
        return lambda i, column_ref: (0,) * rank

    grid = pltpu.PrefetchScalarGridSpec(
        num_scalar_prefetch=1,
        grid=(1,),
        in_specs=[
            pl.BlockSpec((peers, tok, share), whole(3)),
            pl.BlockSpec((tok, share), lambda i, column_ref: (0, column_ref[0])),
            pl.BlockSpec((slots, tok), whole(2)),
        ],
        out_specs=[pl.BlockSpec((tok, share), whole(2)), pl.BlockSpec((slots, share), whole(2))],
    )
    return pl.pallas_call(
        project_body,
        grid_spec=grid,
        out_shape=[
            jax.ShapeDtypeStruct((tok, share), jnp.float32),
            jax.ShapeDtypeStruct((slots, share), jnp.bfloat16),
        ],
        compiler_params=pltpu.CompilerParams(vmem_limit_bytes=16 * 2**20),
        name="project",
    )(column, parts, residual, send)


def hidden_body(rows_ref, gain_ref, gate_ref, up_ref, out_ref):
    rows = rows_ref[...].astype(jnp.float32)
    square = jnp.mean(rows * rows, axis=1, keepdims=True)
    normed = (rows * lax.rsqrt(square + norm_eps) * gain_ref[...]).astype(jnp.bfloat16)
    gate = jnp.dot(normed, gate_ref[...], preferred_element_type=jnp.float32)
    up = jnp.dot(normed, up_ref[...], preferred_element_type=jnp.float32)
    out_ref[...] = (gate / (1.0 + jnp.exp(-gate)) * up).astype(jnp.bfloat16)


def hidden_units(rows, gain, gate, up):
    count, model = rows.shape
    hidden = gate.shape[1]
    tile = 256
    return pl.pallas_call(
        hidden_body,
        grid=(count // tile,),
        in_specs=[
            pl.BlockSpec((tile, model), lambda i: (i, 0)),
            pl.BlockSpec((1, model), lambda i: (0, 0)),
            pl.BlockSpec((model, hidden), lambda i: (0, 0)),
            pl.BlockSpec((model, hidden), lambda i: (0, 0)),
        ],
        out_specs=pl.BlockSpec((tile, hidden), lambda i: (i, 0)),
        out_shape=jax.ShapeDtypeStruct((count, hidden), jnp.bfloat16),
        compiler_params=pltpu.CompilerParams(vmem_limit_bytes=24 * 2**20),
        name="hidden",
    )(rows, gain, gate, up)


def gathered(array, axes, axis, scale):
    sent = (array.astype(jnp.float32) * scale).astype(jnp.float16)
    whole = lax.all_gather(sent, axes, axis=axis, tiled=True)
    return (whole.astype(jnp.float32) * (1.0 / scale)).astype(jnp.bfloat16)


def from_everyone(array, axes):
    peers = lax.axis_size(axes)
    return lax.all_to_all(
        jnp.broadcast_to(array[None], (peers, *array.shape)), axes, 0, 0, tiled=True
    )


def shards(
    residual,
    queries,
    key_vectors,
    value_rows,
    head_lambda,
    head_gain,
    out_weight,
    ffn_gain,
    expert_gate,
    expert_up,
    expert_down,
    routing,
    route_weight,
):
    tok, _, width = queries.shape
    experts = lax.axis_size("sp")
    peers = lax.axis_size("tp")
    model = residual.shape[1]
    share = model // peers
    where = lax.axis_index("sp").astype(jnp.int32)[None]
    column = lax.axis_index("tp").astype(jnp.int32)[None]
    kv = jnp.concatenate([key_vectors[:, 0], value_rows[:, 0]], axis=1)
    kv_all = gathered(kv, "sp", 0, SHIFT)

    capacity = tok // (experts // GROUPS)
    order = jnp.arange(tok, dtype=jnp.int32)
    ids = jnp.arange(experts, dtype=jnp.int32)
    named = routing[:, :, None] == ids
    member = jnp.any(named, axis=1)
    strict = (order[None, :] < order[:, None]).astype(jnp.bfloat16)
    earlier = jnp.dot(
        strict, member.astype(jnp.bfloat16), preferred_element_type=jnp.float32
    ).astype(jnp.int32)
    slot = jnp.arange(capacity, dtype=jnp.int32)
    send = (member.T[:, None, :] & (earlier.T[:, None, :] == slot[None, :, None])).reshape(
        experts * capacity, tok
    )
    send = send.astype(jnp.bfloat16)
    take = [
        (named[:, k, :, None] & (earlier[:, :, None] == slot))
        .reshape(tok, experts * capacity)
        .astype(jnp.bfloat16)
        for k in range(routing.shape[1])
    ]

    partial = attention(
        where, head_lambda, queries[:, 0], kv_all, head_gain[None], out_weight, peers
    )
    parts = lax.all_to_all(partial, "tp", 0, 0, tiled=True)
    own_stream, outgoing = project(column, parts, residual, send)
    landed = lax.all_to_all(
        outgoing.reshape(experts, capacity, share), "sp", 0, 0, tiled=True
    )
    rows = gathered(landed.reshape(experts * capacity, share), "tp", 1, 64.0)
    units = hidden_units(rows, ffn_gain[None], expert_gate[0], expert_up[0])
    all_units = gathered(units, "tp", 1, 0.25)
    expert_out = jnp.dot(
        all_units, expert_down[0], preferred_element_type=jnp.float32
    ).astype(jnp.bfloat16)
    back = lax.all_to_all(
        expert_out.reshape(experts, capacity, share), "sp", 0, 0, tiled=True
    ).reshape(experts * capacity, share)
    moe = sum(
        route_weight[:, k : k + 1] * jnp.dot(take[k], back, preferred_element_type=jnp.float32)
        for k in range(routing.shape[1])
    )
    own_out = (own_stream + moe).astype(jnp.bfloat16)
    whole = from_everyone(own_out, "tp")
    return whole.swapaxes(0, 1).reshape(tok, model)


def solution(mesh):
    in_specs = (
        P("sp", None),
        P("sp", "tp", None),
        P("sp", "tp", None),
        P("sp", "tp", None),
        P("tp"),
        P(),
        P("tp", None),
        P(),
        P("sp", None, "tp"),
        P("sp", None, "tp"),
        P("sp", None, "tp"),
        P("sp", None),
        P("sp", None),
    )
    return jax.shard_map(
        shards, mesh=mesh, in_specs=in_specs, out_specs=P("sp", None), check_vma=False
    )
```

```python
import jax
import jax.numpy as jnp
from jax import lax
from jax.experimental import pallas as pl
from jax.experimental.pallas import tpu as pltpu
from jax.sharding import PartitionSpec as P

norm_eps = 1e-06
KEY_BLOCK = 2048
ROW_BLOCK = 128
SHIFT = 4096.0
GROUPS = 4


def attention_body(where_ref, lam_ref, q_ref, kv_ref, gain_ref, weight_ref, out_ref, stacked, highest, accum):
    tok, width = q_ref.shape
    first_query = where_ref[0] * tok
    last = (first_query + tok - 1) // KEY_BLOCK
    scaled = q_ref[...] * jnp.asarray((width // 2) ** -0.5, jnp.bfloat16)
    low = lax.broadcasted_iota(jnp.int32, scaled.shape, 1) < width // 2
    zero = jnp.zeros_like(scaled)
    stacked[:tok] = jnp.where(low, scaled, zero)
    stacked[tok:] = jnp.where(low, zero, scaled)
    highest[...] = jnp.full(highest.shape, -1e30, jnp.float32)
    accum[...] = jnp.zeros(accum.shape, jnp.float32)

    def update(step, masked):
        block = kv_ref[pl.ds(pl.multiple_of(step * KEY_BLOCK, KEY_BLOCK), KEY_BLOCK), :]
        keys, values = block[:, :width], block[:, width:]
        wide = jnp.concatenate([values, jnp.ones_like(values)], axis=1)
        for at in range(0, 2 * tok, ROW_BLOCK):
            rows = slice(at, at + ROW_BLOCK)
            scores = lax.dot_general(
                stacked[rows], keys, (((1,), (1,)), ((), ())), preferred_element_type=jnp.float32
            )
            if masked:
                row = lax.broadcasted_iota(jnp.int32, scores.shape, 0) + at % tok
                col = lax.broadcasted_iota(jnp.int32, scores.shape, 1)
                scores = jnp.where(
                    col - row <= first_query - step * KEY_BLOCK, scores, -1e30
                )
            before = highest[rows]
            now = jnp.maximum(before, jnp.max(scores, axis=1, keepdims=True))
            weights = jnp.exp(scores - now[:, :1])
            shrink = jnp.exp(before - now)[:, :1]
            blended = jnp.dot(weights.astype(jnp.bfloat16), wide, preferred_element_type=jnp.float32)
            accum[rows] = accum[rows] * shrink + blended
            highest[rows] = now

    def whole(step, carry):
        update(step, False)
        return carry

    lax.fori_loop(0, last, whole, 0)
    update(last, True)
    both = accum[:, :width] / accum[:, width:]
    combined = both[:tok] - lam_ref[0] * both[tok:]
    square = jnp.mean(combined * combined, axis=1, keepdims=True)
    attended = (combined * lax.rsqrt(square + norm_eps) * gain_ref[...]).astype(jnp.bfloat16)
    part = jnp.dot(attended, weight_ref[...], preferred_element_type=jnp.float32)
    share = out_ref.shape[2]
    for p in range(out_ref.shape[0]):
        out_ref[p] = part[:, p * share : (p + 1) * share].astype(jnp.bfloat16)


def attention(where, lam, q, kv, gain, weight, peers):
    tok, width = q.shape
    share = weight.shape[1] // peers
    vmem = pl.BlockSpec(memory_space=pltpu.VMEM)
    smem = pl.BlockSpec(memory_space=pltpu.SMEM)
    return pl.pallas_call(
        attention_body,
        in_specs=[smem, smem, vmem, vmem, vmem, vmem],
        out_specs=vmem,
        out_shape=jax.ShapeDtypeStruct((peers, tok, share), jnp.bfloat16),
        scratch_shapes=[
            pltpu.VMEM((2 * tok, width), jnp.bfloat16),
            pltpu.VMEM((2 * tok, 128), jnp.float32),
            pltpu.VMEM((2 * tok, 2 * width), jnp.float32),
        ],
        compiler_params=pltpu.CompilerParams(vmem_limit_bytes=24 * 2**20),
        name="attention",
    )(where, lam, q, kv, gain, weight)


def project_body(parts_ref, residual_ref, send_ref, stream_ref, out_ref):
    total = residual_ref[...].astype(jnp.float32)
    for p in range(parts_ref.shape[0]):
        total += parts_ref[p].astype(jnp.float32)
    stream_ref[...] = total
    picked = jnp.dot(send_ref[...], total.astype(jnp.bfloat16), preferred_element_type=jnp.float32)
    out_ref[...] = picked.astype(jnp.bfloat16)


def project(parts, residual, send):
    _, tok, share = parts.shape
    slots = send.shape[0]
    vmem = pl.BlockSpec(memory_space=pltpu.VMEM)
    return pl.pallas_call(
        project_body,
        in_specs=[vmem] * 3,
        out_specs=[vmem] * 2,
        out_shape=[
            jax.ShapeDtypeStruct((tok, share), jnp.float32),
            jax.ShapeDtypeStruct((slots, share), jnp.bfloat16),
        ],
        compiler_params=pltpu.CompilerParams(vmem_limit_bytes=16 * 2**20),
        name="project",
    )(parts, residual, send)


def hidden_body(x_ref, rows_ref, gain_ref, gate_ref, up_ref, left_ref, right_ref, gate_2_ref, up_2_ref, out_ref, normed_ref):
    peers, count, share = rows_ref.shape
    pieces = out_ref.shape[0]
    total = jnp.zeros((count, 1), jnp.float32)
    for p in range(peers):
        part = rows_ref[p].astype(jnp.float32)
        total += jnp.sum(part * part, axis=1, keepdims=True)
    scale = lax.rsqrt(total / (peers * share) + norm_eps)
    for p in range(peers):
        cols = slice(p * share, (p + 1) * share)
        normed_ref[:, cols] = (rows_ref[p].astype(jnp.float32) * scale * gain_ref[:, cols]).astype(
            jnp.bfloat16
        )
    own = (gate_ref, up_ref)
    right = (right_ref.at[0], right_ref.at[1])
    left = (left_ref.at[0], left_ref.at[1])
    for ahead, (gates, ups) in enumerate((own, right, (gate_2_ref, up_2_ref), left)):
        normed = normed_ref[...]
        gate = jnp.dot(normed, gates[...], preferred_element_type=jnp.float32)
        up = jnp.dot(normed, ups[...], preferred_element_type=jnp.float32)
        act = gate / (1.0 + jnp.exp(-gate)) * up
        out_ref[lax.rem(x_ref[0] + ahead, pieces)] = act.astype(jnp.bfloat16)


def hidden_units(x, rows, gain, *weights):
    peers, count, share = rows.shape
    hidden = weights[0].shape[1]
    vmem = pl.BlockSpec(memory_space=pltpu.VMEM)
    return pl.pallas_call(
        hidden_body,
        in_specs=[pl.BlockSpec(memory_space=pltpu.SMEM)] + [vmem] * (2 + len(weights)),
        out_specs=vmem,
        out_shape=jax.ShapeDtypeStruct((4, count, hidden), jnp.bfloat16),
        scratch_shapes=[pltpu.VMEM((count, peers * share), jnp.bfloat16)],
        compiler_params=pltpu.CompilerParams(vmem_limit_bytes=24 * 2**20),
        name="hidden",
    )(x, rows, gain, *weights)


def down_body(x_ref, units_ref, own_ref, right_ref, low_ref, high_ref, left_ref, out_ref):
    blocks, count, hidden = units_ref.shape
    pieces = out_ref.shape[0]
    share = own_ref.shape[1]
    half = blocks // 2
    first = jnp.zeros((count, 2 * share), jnp.float32)
    second = jnp.zeros((count, 2 * share), jnp.float32)
    for p in range(blocks):
        rows = slice(p * hidden, (p + 1) * hidden)
        part = slice(p % half * hidden, (p % half + 1) * hidden)
        units = units_ref[p]
        far = (low_ref if p < half else high_ref)[part]
        near = jnp.concatenate([own_ref[rows], right_ref[rows]], axis=1)
        rest = jnp.concatenate([far, left_ref[rows]], axis=1)
        first += jnp.dot(units, near, preferred_element_type=jnp.float32)
        second += jnp.dot(units, rest, preferred_element_type=jnp.float32)
    at = [lax.rem(x_ref[0] + ahead, pieces) for ahead in range(pieces)]
    out_ref[at[0]] = first[:, :share].astype(jnp.bfloat16)
    out_ref[at[1]] = first[:, share:].astype(jnp.bfloat16)
    out_ref[at[2]] = second[:, :share].astype(jnp.bfloat16)
    out_ref[at[3]] = second[:, share:].astype(jnp.bfloat16)


def down_product(x, units, *downs):
    _, count, _ = units.shape
    share = downs[0].shape[1]
    vmem = pl.BlockSpec(memory_space=pltpu.VMEM)
    return pl.pallas_call(
        down_body,
        in_specs=[pl.BlockSpec(memory_space=pltpu.SMEM)] + [vmem] * (1 + len(downs)),
        out_specs=vmem,
        out_shape=jax.ShapeDtypeStruct((4, count, share), jnp.bfloat16),
        compiler_params=pltpu.CompilerParams(vmem_limit_bytes=24 * 2**20),
        name="down",
    )(x, units, *downs)


def gathered(array, axes, axis, scale):
    sent = (array.astype(jnp.float32) * scale).astype(jnp.float16)
    whole = lax.all_gather(sent, axes, axis=axis, tiled=True)
    return (whole.astype(jnp.float32) * (1.0 / scale)).astype(jnp.bfloat16)


def from_everyone(array, axes):
    peers = lax.axis_size(axes)
    return lax.all_to_all(
        jnp.broadcast_to(array[None], (peers, *array.shape)), axes, 0, 0, tiled=True
    )


def shards(
    residual,
    queries,
    key_vectors,
    value_rows,
    head_lambda,
    head_gain,
    out_weight,
    ffn_gain,
    expert_gate,
    expert_up,
    expert_down,
    routing,
    route_weight,
):
    tok, _, _ = queries.shape
    experts = lax.axis_size("sp")
    across = lax.axis_size("x")
    along = lax.axis_size("y")
    tp = ("y", "x")
    peers = across * along
    model = residual.shape[1]
    share = model // peers
    where = lax.axis_index("sp").astype(jnp.int32)[None]
    x_at = lax.axis_index("x").astype(jnp.int32)[None]
    column = (lax.axis_index("y") * across + lax.axis_index("x")) * share

    ahead = [(i, (i + 1) % across) for i in range(across)]
    behind = [(i, (i - 1) % across) for i in range(across)]
    gate, up, down = expert_gate[0], expert_up[0], expert_down[0]
    both = jnp.stack([gate, up])
    left = lax.ppermute(both, "x", ahead)
    right = lax.ppermute(both, "x", behind)
    gate_2 = lax.ppermute(left[0], "x", ahead)
    up_2 = lax.ppermute(right[1], "x", behind)
    half = down.shape[0] // 2
    down_left = lax.ppermute(down, "x", ahead)
    down_right = lax.ppermute(down, "x", behind)
    down_low = lax.ppermute(down_left[:half], "x", ahead)
    down_high = lax.ppermute(down_right[half:], "x", behind)

    kv = jnp.concatenate([key_vectors[:, 0], value_rows[:, 0]], axis=1)
    kv_all = gathered(kv, "sp", 0, SHIFT)
    own_residual = lax.dynamic_slice_in_dim(residual, column, share, 1)

    capacity = tok // (experts // GROUPS)
    order = jnp.arange(tok, dtype=jnp.int32)
    ids = jnp.arange(experts, dtype=jnp.int32)
    named = routing[:, :, None] == ids
    member = jnp.any(named, axis=1)
    strict = (order[None, :] < order[:, None]).astype(jnp.bfloat16)
    earlier = jnp.dot(
        strict, member.astype(jnp.bfloat16), preferred_element_type=jnp.float32
    ).astype(jnp.int32)
    slot = jnp.arange(capacity, dtype=jnp.int32)
    send = (member.T[:, None, :] & (earlier.T[:, None, :] == slot[None, :, None])).reshape(
        experts * capacity, tok
    )
    send = send.astype(jnp.bfloat16)
    take = [
        (named[:, k, :, None] & (earlier[:, :, None] == slot))
        .reshape(tok, experts * capacity)
        .astype(jnp.bfloat16)
        for k in range(routing.shape[1])
    ]

    partial = attention(
        where, head_lambda, queries[:, 0], kv_all, head_gain[None], out_weight, peers
    )
    parts = lax.all_to_all(partial, tp, 0, 0, tiled=True)
    own_stream, outgoing = project(parts, own_residual, send)
    landed = lax.all_to_all(
        outgoing.reshape(experts, capacity, share), "sp", 0, 0, tiled=True
    )
    count = experts * capacity // across
    quarters = jnp.broadcast_to(
        landed.reshape(1, across, count, share), (along, across, count, share)
    )
    rows = lax.all_to_all(quarters.reshape(peers, count, share), tp, 0, 0, tiled=True)
    units = hidden_units(
        x_at, rows, ffn_gain[None], gate, up, left, right, gate_2, up_2
    )
    all_units = gathered(units, "y", 0, 0.25)
    made = down_product(x_at, all_units, down, down_right, down_low, down_high, down_left)
    expert_out = lax.all_to_all(made, "x", 0, 0, tiled=True)
    back = lax.all_to_all(
        expert_out.reshape(experts, capacity, share), "sp", 0, 0, tiled=True
    ).reshape(experts * capacity, share)
    moe = sum(
        route_weight[:, k : k + 1] * jnp.dot(take[k], back, preferred_element_type=jnp.float32)
        for k in range(routing.shape[1])
    )
    own_out = (own_stream + moe).astype(jnp.bfloat16)
    whole = from_everyone(own_out, tp)
    return whole.swapaxes(0, 1).reshape(tok, model)


def solution(mesh):
    sizes = mesh.devices.shape
    split = jax.sharding.Mesh(
        mesh.devices.reshape(sizes[0], sizes[1] // 4, 4), ("sp", "y", "x")
    )
    tp = ("y", "x")
    in_specs = (
        P("sp", None),
        P("sp", tp, None),
        P("sp", tp, None),
        P("sp", tp, None),
        P(tp),
        P(),
        P(tp, None),
        P(),
        P("sp", None, tp),
        P("sp", None, tp),
        P("sp", None, tp),
        P("sp", None),
        P("sp", None),
    )
    return jax.shard_map(
        shards, mesh=split, in_specs=in_specs, out_specs=P("sp", None), check_vma=False
    )
```

```python
import jax
import jax.numpy as jnp
from jax import lax
from jax.experimental import pallas as pl
from jax.experimental.pallas import tpu as pltpu
from jax.sharding import PartitionSpec as P

norm_eps = 1e-06
KEY_BLOCK = 2048
ROW_BLOCK = 128
SHIFT = 4096.0
GROUPS = 4


def attention_body(where_ref, lam_ref, q_ref, kv_ref, gain_ref, weight_ref, out_ref, stacked, highest, accum, parts, sems):
    tok, width = q_ref.shape
    first_query = where_ref[0] * tok
    last = (first_query + tok - 1) // KEY_BLOCK
    scaled = q_ref[...] * jnp.asarray((width // 2) ** -0.5, jnp.bfloat16)
    low = lax.broadcasted_iota(jnp.int32, scaled.shape, 1) < width // 2
    zero = jnp.zeros_like(scaled)
    stacked[:tok] = jnp.where(low, scaled, zero)
    stacked[tok:] = jnp.where(low, zero, scaled)
    highest[...] = jnp.full(highest.shape, -1e30, jnp.float32)
    accum[...] = jnp.zeros(accum.shape, jnp.float32)

    def update(step, masked):
        block = kv_ref[pl.ds(pl.multiple_of(step * KEY_BLOCK, KEY_BLOCK), KEY_BLOCK), :]
        keys, values = block[:, :width], block[:, width:]
        wide = jnp.concatenate([values, jnp.ones_like(values)], axis=1)
        for at in range(0, 2 * tok, ROW_BLOCK):
            rows = slice(at, at + ROW_BLOCK)
            scores = lax.dot_general(
                stacked[rows], keys, (((1,), (1,)), ((), ())), preferred_element_type=jnp.float32
            )
            if masked:
                row = lax.broadcasted_iota(jnp.int32, scores.shape, 0) + at % tok
                col = lax.broadcasted_iota(jnp.int32, scores.shape, 1)
                scores = jnp.where(
                    col - row <= first_query - step * KEY_BLOCK, scores, -1e30
                )
            before = highest[rows]
            now = jnp.maximum(before, jnp.max(scores, axis=1, keepdims=True))
            weights = jnp.exp(scores - now[:, :1])
            shrink = jnp.exp(before - now)[:, :1]
            blended = jnp.dot(weights.astype(jnp.bfloat16), wide, preferred_element_type=jnp.float32)
            accum[rows] = accum[rows] * shrink + blended
            highest[rows] = now

    def whole(step, carry):
        update(step, False)
        return carry

    lax.fori_loop(0, last, whole, 0)
    update(last, True)
    both = accum[:, :width] / accum[:, width:]
    combined = both[:tok] - lam_ref[0] * both[tok:]
    square = jnp.mean(combined * combined, axis=1, keepdims=True)
    attended = (combined * lax.rsqrt(square + norm_eps) * gain_ref[...]).astype(jnp.bfloat16)
    share = out_ref.shape[2]
    copies = []
    for p in range(0, out_ref.shape[0], 2):
        cols = weight_ref[:, p * share : (p + 2) * share]
        part = jnp.dot(attended, cols, preferred_element_type=jnp.float32).astype(jnp.bfloat16)
        parts[p] = part[:, :share]
        parts[p + 1] = part[:, share:]
        copy = pltpu.make_async_copy(
            parts.at[pl.ds(p, 2)], out_ref.at[pl.ds(p, 2)], sems.at[p // 2]
        )
        copy.start()
        copies.append(copy)
    for copy in copies:
        copy.wait()


def attention(where, lam, q, kv, gain, weight, peers):
    tok, width = q.shape
    share = weight.shape[1] // peers
    vmem = pl.BlockSpec(memory_space=pltpu.VMEM)
    smem = pl.BlockSpec(memory_space=pltpu.SMEM)
    return pl.pallas_call(
        attention_body,
        in_specs=[smem, smem, vmem, vmem, vmem, vmem],
        out_specs=pl.BlockSpec(memory_space=pl.ANY),
        out_shape=jax.ShapeDtypeStruct((peers, tok, share), jnp.bfloat16),
        scratch_shapes=[
            pltpu.VMEM((2 * tok, width), jnp.bfloat16),
            pltpu.VMEM((2 * tok, 128), jnp.float32),
            pltpu.VMEM((2 * tok, 2 * width), jnp.float32),
            pltpu.VMEM((peers, tok, share), jnp.bfloat16),
            pltpu.SemaphoreType.DMA((peers // 2,)),
        ],
        compiler_params=pltpu.CompilerParams(vmem_limit_bytes=24 * 2**20),
        name="attention",
    )(where, lam, q, kv, gain, weight)


def pack_body(gate_ref, up_ref, out_ref, sems):
    width = out_ref.shape[2]
    copies = []
    for k, source in enumerate((gate_ref, gate_ref, up_ref, up_ref)):
        cols = source.at[:, pl.ds(k % 2 * width, width)]
        copies.append(pltpu.make_async_copy(cols, out_ref.at[k], sems.at[k]))
    for copy in copies:
        copy.start()
    for copy in copies:
        copy.wait()


def pack(gate, up):
    model, hidden = gate.shape
    anywhere = pl.BlockSpec(memory_space=pl.ANY)
    return pl.pallas_call(
        pack_body,
        in_specs=[anywhere] * 2,
        out_specs=anywhere,
        out_shape=jax.ShapeDtypeStruct((4, model, hidden // 2), gate.dtype),
        scratch_shapes=[pltpu.SemaphoreType.DMA((4,))],
        name="pack",
    )(gate, up)


def project_body(parts_ref, residual_ref, place_ref, stream_ref, out_ref):
    total = residual_ref[...].astype(jnp.float32)
    for p in range(parts_ref.shape[0]):
        total += parts_ref[p].astype(jnp.float32)
    stream_ref[...] = total
    rows = total.astype(jnp.bfloat16)
    experts, tok = place_ref.shape
    capacity = out_ref.shape[0] // experts
    slot = lax.broadcasted_iota(jnp.int32, (capacity, tok), 0)
    for first in range(0, experts, 8):
        send = [
            jnp.where(place_ref[e : e + 1, :] == slot, 1.0, 0.0).astype(jnp.bfloat16)
            for e in range(first, first + 8)
        ]
        picked = jnp.dot(jnp.concatenate(send, axis=0), rows, preferred_element_type=jnp.float32)
        out_ref[first * capacity : (first + 8) * capacity] = picked.astype(jnp.bfloat16)


def project(parts, residual, place):
    _, tok, share = parts.shape
    experts = place.shape[0]
    slots = tok // (experts // GROUPS) * experts
    vmem = pl.BlockSpec(memory_space=pltpu.VMEM)
    return pl.pallas_call(
        project_body,
        in_specs=[vmem] * 3,
        out_specs=[vmem] * 2,
        out_shape=[
            jax.ShapeDtypeStruct((tok, share), jnp.float32),
            jax.ShapeDtypeStruct((slots, share), jnp.bfloat16),
        ],
        compiler_params=pltpu.CompilerParams(vmem_limit_bytes=16 * 2**20),
        name="project",
    )(parts, residual, place)


def hidden_body(x_ref, rows_ref, gain_ref, gate_ref, up_ref, left_ref, right_ref, gate_2_ref, up_2_ref, out_ref, normed_ref, weights, sems):
    peers, count, share = rows_ref.shape
    pieces = out_ref.shape[0]
    width = weights.shape[3]
    low, high = pl.ds(0, width), pl.ds(width, width)
    near, far = pl.ds(0, 2), pl.ds(2, 2)
    groups = [
        [(right_ref, weights.at[1])],
        [(gate_2_ref, weights.at[2, near]), (up_2_ref, weights.at[2, far])],
        [(left_ref, weights.at[3])],
        [
            (gate_ref.at[:, low], weights.at[0, 0]),
            (gate_ref.at[:, high], weights.at[0, 1]),
            (up_ref.at[:, low], weights.at[0, 2]),
            (up_ref.at[:, high], weights.at[0, 3]),
        ],
    ]
    copies, at = [], 0
    for group in groups:
        started = []
        for source, target in group:
            copy = pltpu.make_async_copy(source, target, sems.at[at])
            copy.start()
            started.append(copy)
            at += 1
        copies.append(started)
    total = jnp.zeros((count, 1), jnp.float32)
    for p in range(peers):
        part = rows_ref[p].astype(jnp.float32)
        total += jnp.sum(part * part, axis=1, keepdims=True)
    scale = lax.rsqrt(total / (peers * share) + norm_eps)
    for p in range(peers):
        cols = slice(p * share, (p + 1) * share)
        normed_ref[:, cols] = (rows_ref[p].astype(jnp.float32) * scale * gain_ref[:, cols]).astype(
            jnp.bfloat16
        )
    for ahead, started in zip((1, 2, 3, 0), copies):
        for copy in started:
            copy.wait()
        normed = normed_ref[...]
        gates = jnp.concatenate([weights[ahead, 0], weights[ahead, 1]], axis=1)
        ups = jnp.concatenate([weights[ahead, 2], weights[ahead, 3]], axis=1)
        gate = jnp.dot(normed, gates, preferred_element_type=jnp.float32)
        up = jnp.dot(normed, ups, preferred_element_type=jnp.float32)
        act = gate / (1.0 + jnp.exp(-gate)) * up
        out_ref[lax.rem(x_ref[0] + ahead, pieces)] = act.astype(jnp.bfloat16)


def hidden_units(x, rows, gain, *weights):
    peers, count, share = rows.shape
    model, hidden = weights[0].shape
    vmem = pl.BlockSpec(memory_space=pltpu.VMEM)
    anywhere = pl.BlockSpec(memory_space=pl.ANY)
    return pl.pallas_call(
        hidden_body,
        in_specs=[pl.BlockSpec(memory_space=pltpu.SMEM), vmem, vmem] + [anywhere] * len(weights),
        out_specs=vmem,
        out_shape=jax.ShapeDtypeStruct((4, count, hidden), jnp.bfloat16),
        scratch_shapes=[
            pltpu.VMEM((count, peers * share), jnp.bfloat16),
            pltpu.VMEM((4, 4, model, hidden // 2), jnp.bfloat16),
            pltpu.SemaphoreType.DMA((8,)),
        ],
        compiler_params=pltpu.CompilerParams(vmem_limit_bytes=24 * 2**20),
        name="hidden",
    )(x, rows, gain, *weights)


def down_body(x_ref, units_ref, own_ref, right_ref, far_ref, left_ref, out_ref, downs, sems):
    blocks, count, hidden = units_ref.shape
    pieces = out_ref.shape[0]
    share = own_ref.shape[1]
    parts = sems.shape[0]
    step = own_ref.shape[0] // parts
    copies = []
    for c in range(parts):
        rows = pl.ds(c * step, step)
        for k, source in enumerate((own_ref, right_ref, far_ref, left_ref)):
            copy = pltpu.make_async_copy(source.at[rows], downs.at[k, rows], sems.at[c, k])
            copy.start()
            copies.append(copy)
    first = jnp.zeros((count, 2 * share), jnp.float32)
    second = jnp.zeros((count, 2 * share), jnp.float32)
    for p in range(blocks):
        if p % (blocks // parts) == 0:
            c = p // (blocks // parts)
            for copy in copies[c * pieces : (c + 1) * pieces]:
                copy.wait()
        rows = slice(p * hidden, (p + 1) * hidden)
        units = units_ref[p]
        near = jnp.concatenate([downs[0, rows], downs[1, rows]], axis=1)
        rest = jnp.concatenate([downs[2, rows], downs[3, rows]], axis=1)
        first += jnp.dot(units, near, preferred_element_type=jnp.float32)
        second += jnp.dot(units, rest, preferred_element_type=jnp.float32)
    at = [lax.rem(x_ref[0] + ahead, pieces) for ahead in range(pieces)]
    out_ref[at[0]] = first[:, :share].astype(jnp.bfloat16)
    out_ref[at[1]] = first[:, share:].astype(jnp.bfloat16)
    out_ref[at[2]] = second[:, :share].astype(jnp.bfloat16)
    out_ref[at[3]] = second[:, share:].astype(jnp.bfloat16)


def down_product(x, units, *downs):
    _, count, _ = units.shape
    total, share = downs[0].shape
    vmem = pl.BlockSpec(memory_space=pltpu.VMEM)
    anywhere = pl.BlockSpec(memory_space=pl.ANY)
    return pl.pallas_call(
        down_body,
        in_specs=[pl.BlockSpec(memory_space=pltpu.SMEM), vmem] + [anywhere] * len(downs),
        out_specs=vmem,
        out_shape=jax.ShapeDtypeStruct((4, count, share), jnp.bfloat16),
        scratch_shapes=[
            pltpu.VMEM((4, total, share), jnp.bfloat16),
            pltpu.SemaphoreType.DMA((4, 4)),
        ],
        compiler_params=pltpu.CompilerParams(vmem_limit_bytes=24 * 2**20),
        name="down",
    )(x, units, *downs)


def assemble_body(whole_ref, out_ref, sems):
    peers, _, share = whole_ref.shape
    copies = [
        pltpu.make_async_copy(
            whole_ref.at[p], out_ref.at[:, pl.ds(p * share, share)], sems.at[p]
        )
        for p in range(peers)
    ]
    for copy in copies:
        copy.start()
    for copy in copies:
        copy.wait()


def assemble(whole):
    peers, tok, share = whole.shape
    anywhere = pl.BlockSpec(memory_space=pl.ANY)
    return pl.pallas_call(
        assemble_body,
        in_specs=[anywhere],
        out_specs=anywhere,
        out_shape=jax.ShapeDtypeStruct((tok, peers * share), whole.dtype),
        scratch_shapes=[pltpu.SemaphoreType.DMA((peers,))],
        name="assemble",
    )(whole)


def gathered(array, axes, axis, scale):
    sent = (array.astype(jnp.float32) * scale).astype(jnp.float16)
    whole = lax.all_gather(sent, axes, axis=axis, tiled=True)
    return (whole.astype(jnp.float32) * (1.0 / scale)).astype(jnp.bfloat16)


def from_everyone(array, axes):
    peers = lax.axis_size(axes)
    return lax.all_to_all(
        jnp.broadcast_to(array[None], (peers, *array.shape)), axes, 0, 0, tiled=True
    )


def shards(
    residual,
    queries,
    key_vectors,
    value_rows,
    head_lambda,
    head_gain,
    out_weight,
    ffn_gain,
    expert_gate,
    expert_up,
    expert_down,
    routing,
    route_weight,
):
    tok, _, _ = queries.shape
    experts = lax.axis_size("sp")
    across = lax.axis_size("x")
    along = lax.axis_size("y")
    tp = ("y", "x")
    peers = across * along
    model = residual.shape[1]
    share = model // peers
    where = lax.axis_index("sp").astype(jnp.int32)[None]
    x_at = lax.axis_index("x").astype(jnp.int32)[None]
    column = (lax.axis_index("y") * across + lax.axis_index("x")) * share

    ahead = [(i, (i + 1) % across) for i in range(across)]
    behind = [(i, (i - 1) % across) for i in range(across)]
    gate, up, down = expert_gate[0], expert_up[0], expert_down[0]
    both = pack(gate, up)
    left = lax.ppermute(both, "x", ahead)
    right = lax.ppermute(both, "x", behind)
    gate_2 = lax.ppermute(left[:2], "x", ahead)
    up_2 = lax.ppermute(right[2:], "x", behind)
    down_left = lax.ppermute(down, "x", ahead)
    down_right = lax.ppermute(down, "x", behind)
    down_2 = lax.ppermute(down_left, "x", ahead)

    kv = jnp.concatenate([key_vectors[:, 0], value_rows[:, 0]], axis=1)
    kv_all = gathered(kv, "sp", 0, SHIFT)
    own_residual = lax.dynamic_slice_in_dim(residual, column, share, 1)

    capacity = tok // (experts // GROUPS)
    order = jnp.arange(tok, dtype=jnp.int32)
    ids = jnp.arange(experts, dtype=jnp.int32)
    named = routing[:, :, None] == ids
    member = jnp.any(named, axis=1)
    strict = (order[None, :] < order[:, None]).astype(jnp.bfloat16)
    earlier = jnp.dot(
        strict, member.astype(jnp.bfloat16), preferred_element_type=jnp.float32
    ).astype(jnp.int32)
    slot = jnp.arange(capacity, dtype=jnp.int32)
    place = jnp.where(member, earlier, -1).T
    take = [
        (named[:, k, :, None] & (earlier[:, :, None] == slot))
        .reshape(tok, experts * capacity)
        .astype(jnp.bfloat16)
        for k in range(routing.shape[1])
    ]

    partial = attention(
        where, head_lambda, queries[:, 0], kv_all, head_gain[None], out_weight, peers
    )
    parts = lax.all_to_all(partial, tp, 0, 0, tiled=True)
    own_stream, outgoing = project(parts, own_residual, place)
    landed = lax.all_to_all(
        outgoing.reshape(experts, capacity, share), "sp", 0, 0, tiled=True
    )
    count = experts * capacity // across
    quarters = jnp.broadcast_to(
        landed.reshape(1, across, count, share), (along, across, count, share)
    )
    rows = lax.all_to_all(quarters.reshape(peers, count, share), tp, 0, 0, tiled=True)
    units = hidden_units(
        x_at, rows, ffn_gain[None], gate, up, left, right, gate_2, up_2
    )
    all_units = gathered(units, "y", 0, 0.25)
    made = down_product(x_at, all_units, down, down_right, down_2, down_left)
    expert_out = lax.all_to_all(made, "x", 0, 0, tiled=True)
    back = lax.all_to_all(
        expert_out.reshape(experts, capacity, share), "sp", 0, 0, tiled=True
    ).reshape(experts * capacity, share)
    moe = sum(
        route_weight[:, k : k + 1] * jnp.dot(take[k], back, preferred_element_type=jnp.float32)
        for k in range(routing.shape[1])
    )
    own_out = (own_stream + moe).astype(jnp.bfloat16)
    whole = from_everyone(own_out, tp)
    return assemble(whole)


def solution(mesh):
    sizes = mesh.devices.shape
    split = jax.sharding.Mesh(
        mesh.devices.reshape(sizes[0], sizes[1] // 4, 4), ("sp", "y", "x")
    )
    tp = ("y", "x")
    in_specs = (
        P("sp", None),
        P("sp", tp, None),
        P("sp", tp, None),
        P("sp", tp, None),
        P(tp),
        P(),
        P(tp, None),
        P(),
        P("sp", None, tp),
        P("sp", None, tp),
        P("sp", None, tp),
        P("sp", None),
        P("sp", None),
    )
    return jax.shard_map(
        shards, mesh=split, in_specs=in_specs, out_specs=P("sp", None), check_vma=False
    )
```

```python
import jax
import jax.numpy as jnp
from jax import lax
from jax.experimental import pallas as pl
from jax.experimental.pallas import tpu as pltpu
from jax.sharding import PartitionSpec as P

norm_eps = 1e-06
KEY_BLOCK = 2048
ROW_BLOCK = 128
SHIFT = 4096.0
GROUPS = 4


def attention_body(where_ref, lam_ref, q_ref, kv_ref, gain_ref, weight_ref, out_ref, stacked, highest, accum, parts, sems):
    tok, width = q_ref.shape
    first_query = where_ref[0] * tok
    last = (first_query + tok - 1) // KEY_BLOCK
    scaled = q_ref[...] * jnp.asarray((width // 2) ** -0.5, jnp.bfloat16)
    low = lax.broadcasted_iota(jnp.int32, scaled.shape, 1) < width // 2
    zero = jnp.zeros_like(scaled)
    stacked[:tok] = jnp.where(low, scaled, zero)
    stacked[tok:] = jnp.where(low, zero, scaled)
    highest[...] = jnp.full(highest.shape, -1e30, jnp.float32)
    accum[...] = jnp.zeros(accum.shape, jnp.float32)

    def update(step, masked):
        block = kv_ref[pl.ds(pl.multiple_of(step * KEY_BLOCK, KEY_BLOCK), KEY_BLOCK), :]
        keys, values = block[:, :width], block[:, width:]
        wide = jnp.concatenate([values, jnp.ones_like(values)], axis=1)
        for at in range(0, 2 * tok, ROW_BLOCK):
            rows = slice(at, at + ROW_BLOCK)
            scores = lax.dot_general(
                stacked[rows], keys, (((1,), (1,)), ((), ())), preferred_element_type=jnp.float32
            )
            if masked:
                row = lax.broadcasted_iota(jnp.int32, scores.shape, 0) + at % tok
                col = lax.broadcasted_iota(jnp.int32, scores.shape, 1)
                scores = jnp.where(
                    col - row <= first_query - step * KEY_BLOCK, scores, -1e30
                )
            before = highest[rows]
            now = jnp.maximum(before, jnp.max(scores, axis=1, keepdims=True))
            weights = jnp.exp(scores - now[:, :1])
            shrink = jnp.exp(before - now)[:, :1]
            blended = jnp.dot(weights.astype(jnp.bfloat16), wide, preferred_element_type=jnp.float32)
            accum[rows] = accum[rows] * shrink + blended
            highest[rows] = now

    def whole(step, carry):
        update(step, False)
        return carry

    lax.fori_loop(0, last, whole, 0)
    update(last, True)
    both = accum[:, :width] / accum[:, width:]
    combined = both[:tok] - lam_ref[0] * both[tok:]
    square = jnp.mean(combined * combined, axis=1, keepdims=True)
    attended = (combined * lax.rsqrt(square + norm_eps) * gain_ref[...]).astype(jnp.bfloat16)
    share = out_ref.shape[2]
    copies = []
    for p in range(0, out_ref.shape[0], 2):
        cols = weight_ref[:, p * share : (p + 2) * share]
        part = jnp.dot(attended, cols, preferred_element_type=jnp.float32).astype(jnp.bfloat16)
        parts[p] = part[:, :share]
        parts[p + 1] = part[:, share:]
        copy = pltpu.make_async_copy(
            parts.at[pl.ds(p, 2)], out_ref.at[pl.ds(p, 2)], sems.at[p // 2]
        )
        copy.start()
        copies.append(copy)
    for copy in copies:
        copy.wait()


def attention(where, lam, q, kv, gain, weight, peers):
    tok, width = q.shape
    share = weight.shape[1] // peers
    vmem = pl.BlockSpec(memory_space=pltpu.VMEM)
    smem = pl.BlockSpec(memory_space=pltpu.SMEM)
    return pl.pallas_call(
        attention_body,
        in_specs=[smem, smem, vmem, vmem, vmem, vmem],
        out_specs=pl.BlockSpec(memory_space=pltpu.HBM),
        out_shape=jax.ShapeDtypeStruct((peers, tok, share), jnp.bfloat16),
        scratch_shapes=[
            pltpu.VMEM((2 * tok, width), jnp.bfloat16),
            pltpu.VMEM((2 * tok, 128), jnp.float32),
            pltpu.VMEM((2 * tok, 2 * width), jnp.float32),
            pltpu.VMEM((peers, tok, share), jnp.bfloat16),
            pltpu.SemaphoreType.DMA((peers // 2,)),
        ],
        compiler_params=pltpu.CompilerParams(vmem_limit_bytes=24 * 2**20),
        name="attention",
    )(where, lam, q, kv, gain, weight)


def pack_body(gate_ref, up_ref, down_ref, out_ref):
    width = out_ref.shape[2]
    out_ref[0] = gate_ref[:, :width]
    out_ref[1] = gate_ref[:, width:]
    out_ref[2] = up_ref[:, :width]
    out_ref[3] = up_ref[:, width:]
    out_ref[4] = down_ref[0]
    out_ref[5] = down_ref[1]


def pack(gate, up, down):
    model, hidden = gate.shape
    width = hidden // 2
    tile = model // 4
    return pl.pallas_call(
        pack_body,
        grid=(4,),
        in_specs=[
            pl.BlockSpec((tile, hidden), lambda i: (i, 0)),
            pl.BlockSpec((tile, hidden), lambda i: (i, 0)),
            pl.BlockSpec((2, tile, width), lambda i: (0, i, 0)),
        ],
        out_specs=pl.BlockSpec((6, tile, width), lambda i: (0, i, 0)),
        out_shape=jax.ShapeDtypeStruct((6, model, width), gate.dtype),
        compiler_params=pltpu.CompilerParams(
            dimension_semantics=("arbitrary",), vmem_limit_bytes=16 * 2**20
        ),
        name="pack",
    )(gate, up, down.reshape(2, model, width))


def project_body(parts_ref, residual_ref, place_ref, stream_ref, out_ref):
    total = residual_ref[...].astype(jnp.float32)
    for p in range(parts_ref.shape[0]):
        total += parts_ref[p].astype(jnp.float32)
    stream_ref[...] = total
    rows = total.astype(jnp.bfloat16)
    experts, tok = place_ref.shape
    capacity = out_ref.shape[0] // experts
    slot = lax.broadcasted_iota(jnp.int32, (capacity, tok), 0)
    for first in range(0, experts, 8):
        send = [
            jnp.where(place_ref[e : e + 1, :] == slot, 1.0, 0.0).astype(jnp.bfloat16)
            for e in range(first, first + 8)
        ]
        picked = jnp.dot(jnp.concatenate(send, axis=0), rows, preferred_element_type=jnp.float32)
        out_ref[first * capacity : (first + 8) * capacity] = picked.astype(jnp.bfloat16)


def project(parts, residual, place):
    _, tok, share = parts.shape
    experts = place.shape[0]
    slots = tok // (experts // GROUPS) * experts
    vmem = pl.BlockSpec(memory_space=pltpu.VMEM)
    return pl.pallas_call(
        project_body,
        in_specs=[vmem] * 3,
        out_specs=[vmem] * 2,
        out_shape=[
            jax.ShapeDtypeStruct((tok, share), jnp.float32),
            jax.ShapeDtypeStruct((slots, share), jnp.bfloat16),
        ],
        compiler_params=pltpu.CompilerParams(vmem_limit_bytes=16 * 2**20),
        name="project",
    )(parts, residual, place)


def hidden_body(x_ref, rows_ref, gain_ref, own_ref, left_ref, right_ref, gate_2_ref, up_2_ref, out_ref, normed_ref, weights, sems):
    peers, count, share = rows_ref.shape
    pieces = out_ref.shape[0]
    near, far, both = pl.ds(0, 2), pl.ds(2, 2), pl.ds(0, 4)
    groups = [
        [(own_ref.at[both], weights.at[0])],
        [(right_ref.at[both], weights.at[1])],
        [(left_ref.at[both], weights.at[3])],
        [(gate_2_ref, weights.at[2, near]), (up_2_ref, weights.at[2, far])],
    ]
    copies, at = [], 0
    for group in groups:
        started = []
        for source, target in group:
            copy = pltpu.make_async_copy(source, target, sems.at[at])
            copy.start()
            started.append(copy)
            at += 1
        copies.append(started)
    total = jnp.zeros((count, 1), jnp.float32)
    for p in range(peers):
        part = rows_ref[p].astype(jnp.float32)
        total += jnp.sum(part * part, axis=1, keepdims=True)
    scale = lax.rsqrt(total / (peers * share) + norm_eps)
    for p in range(peers):
        cols = slice(p * share, (p + 1) * share)
        normed_ref[:, cols] = (rows_ref[p].astype(jnp.float32) * scale * gain_ref[:, cols]).astype(
            jnp.bfloat16
        )
    for ahead, started in zip((0, 1, 3, 2), copies):
        for copy in started:
            copy.wait()
        normed = normed_ref[...]
        gates = jnp.concatenate([weights[ahead, 0], weights[ahead, 1]], axis=1)
        ups = jnp.concatenate([weights[ahead, 2], weights[ahead, 3]], axis=1)
        gate = jnp.dot(normed, gates, preferred_element_type=jnp.float32)
        up = jnp.dot(normed, ups, preferred_element_type=jnp.float32)
        act = gate / (1.0 + jnp.exp(-gate)) * up
        out_ref[lax.rem(x_ref[0] + ahead, pieces)] = act.astype(jnp.bfloat16)


def hidden_units(x, rows, gain, *weights):
    peers, count, share = rows.shape
    _, model, half = weights[0].shape
    vmem = pl.BlockSpec(memory_space=pltpu.VMEM)
    anywhere = pl.BlockSpec(memory_space=pltpu.HBM)
    return pl.pallas_call(
        hidden_body,
        in_specs=[pl.BlockSpec(memory_space=pltpu.SMEM), vmem, vmem] + [anywhere] * len(weights),
        out_specs=vmem,
        out_shape=jax.ShapeDtypeStruct((4, count, 2 * half), jnp.bfloat16),
        scratch_shapes=[
            pltpu.VMEM((count, peers * share), jnp.bfloat16),
            pltpu.VMEM((4, 4, model, half), jnp.bfloat16),
            pltpu.SemaphoreType.DMA((5,)),
        ],
        compiler_params=pltpu.CompilerParams(vmem_limit_bytes=24 * 2**20),
        name="hidden",
    )(x, rows, gain, *weights)


def down_body(x_ref, units_ref, own_ref, right_ref, far_ref, left_ref, out_ref, downs, sems):
    blocks, count, hidden = units_ref.shape
    chips, pieces, rows_each, _ = out_ref.shape
    parts = sems.shape[0]
    half, share = own_ref.shape[1:]
    step = 2 * half // parts
    copies = []
    for c in range(parts):
        at = c * step
        rows = pl.ds(at, step)
        inner = pl.ds(at % half, step)
        page = at // half
        sources = (
            own_ref.at[4 + page, inner],
            right_ref.at[4 + page, inner],
            far_ref.at[page, inner],
            left_ref.at[4 + page, inner],
        )
        for k, source in enumerate(sources):
            copy = pltpu.make_async_copy(source, downs.at[k, rows], sems.at[c, k])
            copy.start()
            copies.append(copy)
    first = jnp.zeros((count, 2 * share), jnp.float32)
    second = jnp.zeros((count, 2 * share), jnp.float32)
    for p in range(blocks):
        if p % (blocks // parts) == 0:
            c = p // (blocks // parts)
            for copy in copies[c * pieces : (c + 1) * pieces]:
                copy.wait()
        rows = slice(p * hidden, (p + 1) * hidden)
        units = units_ref[p]
        near = jnp.concatenate([downs[0, rows], downs[1, rows]], axis=1)
        rest = jnp.concatenate([downs[2, rows], downs[3, rows]], axis=1)
        first += jnp.dot(units, near, preferred_element_type=jnp.float32)
        second += jnp.dot(units, rest, preferred_element_type=jnp.float32)
    made = (first[:, :share], first[:, share:], second[:, :share], second[:, share:])
    for ahead, value in enumerate(made):
        at = lax.rem(x_ref[0] + ahead, pieces)
        out_ref[:, at] = value.reshape(chips, rows_each, share).astype(jnp.bfloat16)


def down_product(x, units, chips, *downs):
    _, count, _ = units.shape
    _, half, share = downs[0].shape
    vmem = pl.BlockSpec(memory_space=pltpu.VMEM)
    anywhere = pl.BlockSpec(memory_space=pltpu.HBM)
    return pl.pallas_call(
        down_body,
        in_specs=[pl.BlockSpec(memory_space=pltpu.SMEM), vmem] + [anywhere] * len(downs),
        out_specs=vmem,
        out_shape=jax.ShapeDtypeStruct((chips, 4, count // chips, share), jnp.bfloat16),
        scratch_shapes=[
            pltpu.VMEM((4, 2 * half, share), jnp.bfloat16),
            pltpu.SemaphoreType.DMA((4, 4)),
        ],
        compiler_params=pltpu.CompilerParams(vmem_limit_bytes=24 * 2**20),
        name="down",
    )(x, units, *downs)


def assemble_body(whole_ref, out_ref):
    peers, _, share = whole_ref.shape
    for p in range(peers):
        out_ref[:, p * share : (p + 1) * share] = whole_ref[p]


def assemble(whole):
    peers, tok, share = whole.shape
    tile = tok // 4
    return pl.pallas_call(
        assemble_body,
        grid=(4,),
        in_specs=[pl.BlockSpec((peers, tile, share), lambda i: (0, i, 0))],
        out_specs=pl.BlockSpec((tile, peers * share), lambda i: (i, 0)),
        out_shape=jax.ShapeDtypeStruct((tok, peers * share), whole.dtype),
        compiler_params=pltpu.CompilerParams(
            dimension_semantics=("arbitrary",), vmem_limit_bytes=16 * 2**20
        ),
        name="assemble",
    )(whole)


def gathered(array, axes, axis, scale):
    sent = (array.astype(jnp.float32) * scale).astype(jnp.float16)
    whole = lax.all_gather(sent, axes, axis=axis, tiled=True)
    return (whole.astype(jnp.float32) * (1.0 / scale)).astype(jnp.bfloat16)


def from_everyone(array, axes):
    peers = lax.axis_size(axes)
    return lax.all_to_all(
        jnp.broadcast_to(array[None], (peers, *array.shape)), axes, 0, 0, tiled=True
    )


def shards(
    residual,
    queries,
    key_vectors,
    value_rows,
    head_lambda,
    head_gain,
    out_weight,
    ffn_gain,
    expert_gate,
    expert_up,
    expert_down,
    routing,
    route_weight,
):
    tok, _, _ = queries.shape
    experts = lax.axis_size("sp")
    across = lax.axis_size("x")
    along = lax.axis_size("y")
    tp = ("y", "x")
    peers = across * along
    model = residual.shape[1]
    share = model // peers
    where = lax.axis_index("sp").astype(jnp.int32)[None]
    x_at = lax.axis_index("x").astype(jnp.int32)[None]
    column = (lax.axis_index("y") * across + lax.axis_index("x")) * share

    ahead = [(i, (i + 1) % across) for i in range(across)]
    behind = [(i, (i - 1) % across) for i in range(across)]
    gate, up, down = expert_gate[0], expert_up[0], expert_down[0]
    packed = pack(gate, up, down)
    left = lax.ppermute(packed, "x", ahead)
    right = lax.ppermute(packed, "x", behind)
    gate_2 = lax.ppermute(left[:2], "x", ahead)
    up_2 = lax.ppermute(right[2:4], "x", behind)
    down_2 = lax.ppermute(left[4:], "x", ahead)

    kv = jnp.concatenate([key_vectors[:, 0], value_rows[:, 0]], axis=1)
    kv_all = gathered(kv, "sp", 0, SHIFT)
    own_residual = lax.dynamic_slice_in_dim(residual, column, share, 1)

    capacity = tok // (experts // GROUPS)
    order = jnp.arange(tok, dtype=jnp.int32)
    ids = jnp.arange(experts, dtype=jnp.int32)
    named = routing[:, :, None] == ids
    member = jnp.any(named, axis=1)
    strict = (order[None, :] < order[:, None]).astype(jnp.bfloat16)
    earlier = jnp.dot(
        strict, member.astype(jnp.bfloat16), preferred_element_type=jnp.float32
    ).astype(jnp.int32)
    slot = jnp.arange(capacity, dtype=jnp.int32)
    place = jnp.where(member, earlier, -1).T
    take = [
        (named[:, k, :, None] & (earlier[:, :, None] == slot))
        .reshape(tok, experts * capacity)
        .astype(jnp.bfloat16)
        for k in range(routing.shape[1])
    ]

    partial = attention(
        where, head_lambda, queries[:, 0], kv_all, head_gain[None], out_weight, peers
    )
    parts = lax.all_to_all(partial, tp, 0, 0, tiled=True)
    own_stream, outgoing = project(parts, own_residual, place)
    targets = experts * across
    each = capacity // across
    landed = lax.all_to_all(outgoing.reshape(targets, each, share), ("sp", "x"), 0, 0, tiled=True)
    landed = landed.reshape(experts, across, each, share).swapaxes(0, 1)
    rows = gathered(landed.reshape(across, experts * each, share), "y", 0, 64.0)
    units = hidden_units(
        x_at, rows, ffn_gain[None], packed, left, right, gate_2, up_2
    )
    all_units = gathered(units, "y", 0, 0.25)
    made = down_product(x_at, all_units, experts, packed, right, down_2, left)
    back = lax.all_to_all(
        made.reshape(targets, each, share), ("sp", "x"), 0, 0, tiled=True
    )
    back = back.reshape(experts * capacity, share)
    moe = sum(
        route_weight[:, k : k + 1] * jnp.dot(take[k], back, preferred_element_type=jnp.float32)
        for k in range(routing.shape[1])
    )
    own_out = (own_stream + moe).astype(jnp.bfloat16)
    whole = from_everyone(own_out, tp)
    return assemble(whole)


def solution(mesh):
    sizes = mesh.devices.shape
    split = jax.sharding.Mesh(
        mesh.devices.reshape(sizes[0], sizes[1] // 4, 4), ("sp", "y", "x")
    )
    tp = ("y", "x")
    in_specs = (
        P("sp", None),
        P("sp", tp, None),
        P("sp", tp, None),
        P("sp", tp, None),
        P(tp),
        P(),
        P(tp, None),
        P(),
        P("sp", None, tp),
        P("sp", None, tp),
        P("sp", None, tp),
        P("sp", None),
        P("sp", None),
    )
    return jax.shard_map(
        shards, mesh=split, in_specs=in_specs, out_specs=P("sp", None), check_vma=False
    )
```

```python
import jax
import jax.numpy as jnp
from jax import lax
from jax.experimental import pallas as pl
from jax.experimental.pallas import tpu as pltpu
from jax.sharding import PartitionSpec as P

norm_eps = 1e-06
KEY_BLOCK = 2048
ROW_BLOCK = 128
SHIFT = 4096.0
GROUPS = 4


def attention_body(where_ref, lam_ref, q_ref, kv_ref, gain_ref, weight_ref, out_ref, stacked, highest, accum, parts, sems):
    tok, width = q_ref.shape
    first_query = where_ref[0] * tok
    last = (first_query + tok - 1) // KEY_BLOCK
    scaled = q_ref[...] * jnp.asarray((width // 2) ** -0.5, jnp.bfloat16)
    low = lax.broadcasted_iota(jnp.int32, scaled.shape, 1) < width // 2
    zero = jnp.zeros_like(scaled)
    stacked[:tok] = jnp.where(low, scaled, zero)
    stacked[tok:] = jnp.where(low, zero, scaled)
    highest[...] = jnp.full(highest.shape, -1e30, jnp.float32)
    accum[...] = jnp.zeros(accum.shape, jnp.float32)

    def update(step, masked):
        block = kv_ref[pl.ds(pl.multiple_of(step * KEY_BLOCK, KEY_BLOCK), KEY_BLOCK), :]
        keys, values = block[:, :width], block[:, width:]
        wide = jnp.concatenate([values, jnp.ones_like(values)], axis=1)
        for at in range(0, 2 * tok, ROW_BLOCK):
            rows = slice(at, at + ROW_BLOCK)
            scores = lax.dot_general(
                stacked[rows], keys, (((1,), (1,)), ((), ())), preferred_element_type=jnp.float32
            )
            if masked:
                row = lax.broadcasted_iota(jnp.int32, scores.shape, 0) + at % tok
                col = lax.broadcasted_iota(jnp.int32, scores.shape, 1)
                scores = jnp.where(
                    col - row <= first_query - step * KEY_BLOCK, scores, -1e30
                )
            before = highest[rows]
            now = jnp.maximum(before, jnp.max(scores, axis=1, keepdims=True))
            weights = jnp.exp(scores - now[:, :1])
            shrink = jnp.exp(before - now)[:, :1]
            blended = jnp.dot(weights.astype(jnp.bfloat16), wide, preferred_element_type=jnp.float32)
            accum[rows] = accum[rows] * shrink + blended
            highest[rows] = now

    def whole(step, carry):
        update(step, False)
        return carry

    lax.fori_loop(0, last, whole, 0)
    update(last, True)
    both = accum[:, :width] / accum[:, width:]
    combined = both[:tok] - lam_ref[0] * both[tok:]
    square = jnp.mean(combined * combined, axis=1, keepdims=True)
    attended = (combined * lax.rsqrt(square + norm_eps) * gain_ref[...]).astype(jnp.bfloat16)
    share = out_ref.shape[2]
    copies = []
    for p in range(0, out_ref.shape[0], 2):
        cols = weight_ref[:, p * share : (p + 2) * share]
        part = jnp.dot(attended, cols, preferred_element_type=jnp.float32).astype(jnp.bfloat16)
        parts[p] = part[:, :share]
        parts[p + 1] = part[:, share:]
        copy = pltpu.make_async_copy(
            parts.at[pl.ds(p, 2)], out_ref.at[pl.ds(p, 2)], sems.at[p // 2]
        )
        copy.start()
        copies.append(copy)
    for copy in copies:
        copy.wait()


def attention(where, lam, q, kv, gain, weight, peers):
    tok, width = q.shape
    share = weight.shape[1] // peers
    vmem = pl.BlockSpec(memory_space=pltpu.VMEM)
    smem = pl.BlockSpec(memory_space=pltpu.SMEM)
    return pl.pallas_call(
        attention_body,
        in_specs=[smem, smem, vmem, vmem, vmem, vmem],
        out_specs=pl.BlockSpec(memory_space=pltpu.HBM),
        out_shape=jax.ShapeDtypeStruct((peers, tok, share), jnp.bfloat16),
        scratch_shapes=[
            pltpu.VMEM((2 * tok, width), jnp.bfloat16),
            pltpu.VMEM((2 * tok, 128), jnp.float32),
            pltpu.VMEM((2 * tok, 2 * width), jnp.float32),
            pltpu.VMEM((peers, tok, share), jnp.bfloat16),
            pltpu.SemaphoreType.DMA((peers // 2,)),
        ],
        compiler_params=pltpu.CompilerParams(vmem_limit_bytes=24 * 2**20),
        name="attention",
    )(where, lam, q, kv, gain, weight)


def pack_body(gate_ref, up_ref, down_ref, out_ref, sems):
    rows, width = out_ref.shape[1:]
    low, high = pl.ds(0, width), pl.ds(width, width)
    sources = (
        gate_ref.at[:, low],
        gate_ref.at[:, high],
        down_ref.at[pl.ds(0, rows)],
        down_ref.at[pl.ds(rows, rows)],
        up_ref.at[:, low],
        up_ref.at[:, high],
    )
    copies = [
        pltpu.make_async_copy(source, out_ref.at[k], sems.at[k])
        for k, source in enumerate(sources)
    ]
    for copy in copies:
        copy.start()
    for copy in copies:
        copy.wait()


def pack(gate, up, down):
    model, hidden = gate.shape
    return pl.pallas_call(
        pack_body,
        in_specs=[pl.BlockSpec(memory_space=pltpu.HBM)] * 3,
        out_specs=pl.BlockSpec(memory_space=pltpu.HBM),
        out_shape=jax.ShapeDtypeStruct((6, model, hidden // 2), gate.dtype),
        scratch_shapes=[pltpu.SemaphoreType.DMA((6,))],
        compiler_params=pltpu.CompilerParams(vmem_limit_bytes=16 * 2**20),
        name="pack",
    )(gate, up, down)


def project_body(parts_ref, residual_ref, place_ref, slots_ref, factors_ref, stream_ref, out_ref, slots_out, factors_out):
    slots_out[...] = slots_ref[...]
    factors_out[...] = factors_ref[...]
    total = residual_ref[...].astype(jnp.float32)
    for p in range(parts_ref.shape[0]):
        total += parts_ref[p].astype(jnp.float32)
    stream_ref[...] = total
    rows = total.astype(jnp.bfloat16)
    experts, tok = place_ref.shape
    capacity = out_ref.shape[0] // experts
    slot = lax.broadcasted_iota(jnp.int32, (capacity, tok), 0)
    for first in range(0, experts, 8):
        send = [
            jnp.where(place_ref[e : e + 1, :] == slot, 1.0, 0.0).astype(jnp.bfloat16)
            for e in range(first, first + 8)
        ]
        picked = jnp.dot(jnp.concatenate(send, axis=0), rows, preferred_element_type=jnp.float32)
        out_ref[first * capacity : (first + 8) * capacity] = picked.astype(jnp.bfloat16)


def project(parts, residual, place, slots, factors):
    _, tok, share = parts.shape
    experts = place.shape[0]
    rows = tok // (experts // GROUPS) * experts
    vmem = pl.BlockSpec(memory_space=pltpu.VMEM)
    return pl.pallas_call(
        project_body,
        in_specs=[vmem] * 5,
        out_specs=[vmem] * 4,
        out_shape=[
            jax.ShapeDtypeStruct((tok, share), jnp.float32),
            jax.ShapeDtypeStruct((rows, share), jnp.bfloat16),
            jax.ShapeDtypeStruct(slots.shape, slots.dtype),
            jax.ShapeDtypeStruct(factors.shape, factors.dtype),
        ],
        compiler_params=pltpu.CompilerParams(vmem_limit_bytes=16 * 2**20),
        name="project",
    )(parts, residual, place, slots, factors)


def combine_body(back_ref, stream_ref, slots_ref, factors_ref, out_ref):
    tok = stream_ref.shape[0]
    rows = back_ref.shape[0]
    slot = lax.broadcasted_iota(jnp.int32, (tok, rows), 1)
    total = stream_ref[...]
    for k in range(slots_ref.shape[1]):
        take = jnp.where(slots_ref[:, k : k + 1] == slot, 1.0, 0.0).astype(jnp.bfloat16)
        found = jnp.dot(take, back_ref[...], preferred_element_type=jnp.float32)
        total += factors_ref[:, k : k + 1] * found
    done = total.astype(jnp.bfloat16)
    for p in range(out_ref.shape[0]):
        out_ref[p] = done


def combine(back, stream, slots, factors, peers):
    tok, share = stream.shape
    vmem = pl.BlockSpec(memory_space=pltpu.VMEM)
    return pl.pallas_call(
        combine_body,
        in_specs=[vmem] * 4,
        out_specs=vmem,
        out_shape=jax.ShapeDtypeStruct((peers, tok, share), jnp.bfloat16),
        compiler_params=pltpu.CompilerParams(vmem_limit_bytes=16 * 2**20),
        name="combine",
    )(back, stream, slots, factors)


def hidden_body(x_ref, rows_ref, gain_ref, own_ref, left_ref, right_ref, far_ref, far_up_ref, out_ref, normed_ref, weights, sems):
    peers, count, share = rows_ref.shape
    pieces = out_ref.shape[0]
    gate, up = pl.ds(0, 2), pl.ds(4, 2)
    first, second = pl.ds(0, 2), pl.ds(2, 2)
    groups = [
        [(source.at[gate], weights.at[k, first]), (source.at[up], weights.at[k, second])]
        for k, source in ((0, own_ref), (1, right_ref), (3, left_ref))
    ]
    groups.append(
        [(far_ref.at[gate], weights.at[2, first]), (far_up_ref, weights.at[2, second])]
    )
    copies, at = [], 0
    for group in groups:
        started = []
        for source, target in group:
            copy = pltpu.make_async_copy(source, target, sems.at[at])
            copy.start()
            started.append(copy)
            at += 1
        copies.append(started)
    total = jnp.zeros((count, 1), jnp.float32)
    for p in range(peers):
        part = rows_ref[p].astype(jnp.float32)
        total += jnp.sum(part * part, axis=1, keepdims=True)
    scale = lax.rsqrt(total / (peers * share) + norm_eps)
    for p in range(peers):
        cols = slice(p * share, (p + 1) * share)
        normed_ref[:, cols] = (rows_ref[p].astype(jnp.float32) * scale * gain_ref[:, cols]).astype(
            jnp.bfloat16
        )
    for ahead, started in zip((0, 1, 3, 2), copies):
        for copy in started:
            copy.wait()
        normed = normed_ref[...]
        gates = jnp.concatenate([weights[ahead, 0], weights[ahead, 1]], axis=1)
        ups = jnp.concatenate([weights[ahead, 2], weights[ahead, 3]], axis=1)
        gate = jnp.dot(normed, gates, preferred_element_type=jnp.float32)
        up = jnp.dot(normed, ups, preferred_element_type=jnp.float32)
        act = gate / (1.0 + jnp.exp(-gate)) * up
        out_ref[lax.rem(x_ref[0] + ahead, pieces)] = act.astype(jnp.bfloat16)


def hidden_units(x, rows, gain, *weights):
    peers, count, share = rows.shape
    _, model, half = weights[0].shape
    vmem = pl.BlockSpec(memory_space=pltpu.VMEM)
    anywhere = pl.BlockSpec(memory_space=pltpu.HBM)
    return pl.pallas_call(
        hidden_body,
        in_specs=[pl.BlockSpec(memory_space=pltpu.SMEM), vmem, vmem] + [anywhere] * len(weights),
        out_specs=vmem,
        out_shape=jax.ShapeDtypeStruct((4, count, 2 * half), jnp.bfloat16),
        scratch_shapes=[
            pltpu.VMEM((count, peers * share), jnp.bfloat16),
            pltpu.VMEM((4, 4, model, half), jnp.bfloat16),
            pltpu.SemaphoreType.DMA((8,)),
        ],
        compiler_params=pltpu.CompilerParams(vmem_limit_bytes=24 * 2**20),
        name="hidden",
    )(x, rows, gain, *weights)


def down_body(x_ref, units_ref, own_ref, right_ref, far_ref, left_ref, out_ref, downs, sems):
    blocks, count, hidden = units_ref.shape
    chips, pieces, rows_each, _ = out_ref.shape
    parts = sems.shape[0]
    half, share = own_ref.shape[1:]
    step = 2 * half // parts
    copies = []
    for c in range(parts):
        at = c * step
        rows = pl.ds(at, step)
        inner = pl.ds(at % half, step)
        page = at // half
        sources = (
            own_ref.at[2 + page, inner],
            right_ref.at[2 + page, inner],
            far_ref.at[2 + page, inner],
            left_ref.at[2 + page, inner],
        )
        for k, source in enumerate(sources):
            copy = pltpu.make_async_copy(source, downs.at[k, rows], sems.at[c, k])
            copy.start()
            copies.append(copy)
    first = jnp.zeros((count, 2 * share), jnp.float32)
    second = jnp.zeros((count, 2 * share), jnp.float32)
    for p in range(blocks):
        if p % (blocks // parts) == 0:
            c = p // (blocks // parts)
            for copy in copies[c * pieces : (c + 1) * pieces]:
                copy.wait()
        rows = slice(p * hidden, (p + 1) * hidden)
        units = units_ref[p]
        near = jnp.concatenate([downs[0, rows], downs[1, rows]], axis=1)
        rest = jnp.concatenate([downs[2, rows], downs[3, rows]], axis=1)
        first += jnp.dot(units, near, preferred_element_type=jnp.float32)
        second += jnp.dot(units, rest, preferred_element_type=jnp.float32)
    made = (first[:, :share], first[:, share:], second[:, :share], second[:, share:])
    for ahead, value in enumerate(made):
        at = lax.rem(x_ref[0] + ahead, pieces)
        out_ref[:, at] = value.reshape(chips, rows_each, share).astype(jnp.bfloat16)


def down_product(x, units, chips, *downs):
    _, count, _ = units.shape
    _, half, share = downs[0].shape
    vmem = pl.BlockSpec(memory_space=pltpu.VMEM)
    anywhere = pl.BlockSpec(memory_space=pltpu.HBM)
    return pl.pallas_call(
        down_body,
        in_specs=[pl.BlockSpec(memory_space=pltpu.SMEM), vmem] + [anywhere] * len(downs),
        out_specs=vmem,
        out_shape=jax.ShapeDtypeStruct((chips, 4, count // chips, share), jnp.bfloat16),
        scratch_shapes=[
            pltpu.VMEM((4, 2 * half, share), jnp.bfloat16),
            pltpu.SemaphoreType.DMA((4, 4)),
        ],
        compiler_params=pltpu.CompilerParams(vmem_limit_bytes=24 * 2**20),
        name="down",
    )(x, units, *downs)


def assemble_body(whole_ref, out_ref):
    peers, _, share = whole_ref.shape
    for p in range(peers):
        out_ref[:, p * share : (p + 1) * share] = whole_ref[p]


def assemble(whole):
    peers, tok, share = whole.shape
    tile = tok // 4
    return pl.pallas_call(
        assemble_body,
        grid=(4,),
        in_specs=[pl.BlockSpec((peers, tile, share), lambda i: (0, i, 0))],
        out_specs=pl.BlockSpec((tile, peers * share), lambda i: (i, 0)),
        out_shape=jax.ShapeDtypeStruct((tok, peers * share), whole.dtype),
        compiler_params=pltpu.CompilerParams(
            dimension_semantics=("arbitrary",), vmem_limit_bytes=16 * 2**20
        ),
        name="assemble",
    )(whole)


def gathered(array, axes, axis, scale):
    sent = (array.astype(jnp.float32) * scale).astype(jnp.float16)
    whole = lax.all_gather(sent, axes, axis=axis, tiled=True)
    return (whole.astype(jnp.float32) * (1.0 / scale)).astype(jnp.bfloat16)


def shards(
    residual,
    queries,
    key_vectors,
    value_rows,
    head_lambda,
    head_gain,
    out_weight,
    ffn_gain,
    expert_gate,
    expert_up,
    expert_down,
    routing,
    route_weight,
):
    tok, _, _ = queries.shape
    experts = lax.axis_size("sp")
    across = lax.axis_size("x")
    along = lax.axis_size("y")
    tp = ("y", "x")
    peers = across * along
    model = residual.shape[1]
    share = model // peers
    where = lax.axis_index("sp").astype(jnp.int32)[None]
    x_at = lax.axis_index("x").astype(jnp.int32)[None]
    column = (lax.axis_index("y") * across + lax.axis_index("x")) * share

    ahead = [(i, (i + 1) % across) for i in range(across)]
    behind = [(i, (i - 1) % across) for i in range(across)]
    gate, up, down = expert_gate[0], expert_up[0], expert_down[0]
    packed = pack(gate, up, down)
    left = lax.ppermute(packed, "x", ahead)
    right = lax.ppermute(packed, "x", behind)
    far = lax.ppermute(left[:4], "x", ahead)
    far_up = lax.ppermute(right[4:], "x", behind)

    kv = jnp.concatenate([key_vectors[:, 0], value_rows[:, 0]], axis=1)
    kv_all = gathered(kv, "sp", 0, SHIFT)
    own_residual = lax.dynamic_slice_in_dim(residual, column, share, 1)

    capacity = tok // (experts // GROUPS)
    order = jnp.arange(tok, dtype=jnp.int32)
    ids = jnp.arange(experts, dtype=jnp.int32)
    named = routing[:, :, None] == ids
    member = jnp.any(named, axis=1)
    strict = (order[None, :] < order[:, None]).astype(jnp.bfloat16)
    earlier = jnp.dot(
        strict, member.astype(jnp.bfloat16), preferred_element_type=jnp.float32
    ).astype(jnp.int32)
    place = jnp.where(member, earlier, -1).T
    picked = jnp.sum(jnp.where(named, earlier[:, None, :], 0), axis=2)
    slots = routing * capacity + picked

    partial = attention(
        where, head_lambda, queries[:, 0], kv_all, head_gain[None], out_weight, peers
    )
    parts = lax.all_to_all(partial, tp, 0, 0, tiled=True)
    own_stream, outgoing, slots, factors = project(
        parts, own_residual, place, slots, route_weight
    )
    targets = experts * across
    each = capacity // across
    landed = lax.all_to_all(outgoing.reshape(targets, each, share), ("sp", "x"), 0, 0, tiled=True)
    landed = landed.reshape(experts, across, each, share).swapaxes(0, 1)
    rows = gathered(landed.reshape(across, experts * each, share), "y", 0, 64.0)
    units = hidden_units(
        x_at, rows, ffn_gain[None], packed, left, right, far, far_up
    )
    all_units = gathered(units, "y", 0, 0.25)
    made = down_product(x_at, all_units, experts, packed, right, far, left)
    back = lax.all_to_all(
        made.reshape(targets, each, share), ("sp", "x"), 0, 0, tiled=True
    )
    back = back.reshape(experts * capacity, share)
    spread = combine(back, own_stream, slots, factors, peers)
    whole = lax.all_to_all(spread, tp, 0, 0, tiled=True)
    return assemble(whole)


def solution(mesh):
    sizes = mesh.devices.shape
    split = jax.sharding.Mesh(
        mesh.devices.reshape(sizes[0], sizes[1] // 4, 4), ("sp", "y", "x")
    )
    tp = ("y", "x")
    in_specs = (
        P("sp", None),
        P("sp", tp, None),
        P("sp", tp, None),
        P("sp", tp, None),
        P(tp),
        P(),
        P(tp, None),
        P(),
        P("sp", None, tp),
        P("sp", None, tp),
        P("sp", None, tp),
        P("sp", None),
        P("sp", None),
    )
    return jax.shard_map(
        shards, mesh=split, in_specs=in_specs, out_specs=P("sp", None), check_vma=False
    )
```

```python
import jax
import jax.numpy as jnp
from jax import lax
from jax.experimental import pallas as pl
from jax.experimental.pallas import tpu as pltpu
from jax.sharding import PartitionSpec as P

norm_eps = 1e-06
KEY_BLOCK = 2048
ROW_BLOCK = 128
SHIFT = 4096.0
GROUPS = 4


def attention_body(where_ref, lam_ref, q_ref, kv_ref, gain_ref, weight_ref, out_ref, stacked, highest, accum, parts, sems):
    tok, width = q_ref.shape
    first_query = where_ref[0] * tok
    last = (first_query + tok - 1) // KEY_BLOCK
    scaled = q_ref[...] * jnp.asarray((width // 2) ** -0.5, jnp.bfloat16)
    low = lax.broadcasted_iota(jnp.int32, scaled.shape, 1) < width // 2
    zero = jnp.zeros_like(scaled)
    stacked[:tok] = jnp.where(low, scaled, zero)
    stacked[tok:] = jnp.where(low, zero, scaled)
    highest[...] = jnp.full(highest.shape, -1e30, jnp.float32)
    accum[...] = jnp.zeros(accum.shape, jnp.float32)

    def update(step, masked):
        block = kv_ref[pl.ds(pl.multiple_of(step * KEY_BLOCK, KEY_BLOCK), KEY_BLOCK), :]
        keys, values = block[:, :width], block[:, width:]
        wide = jnp.concatenate([values, jnp.ones_like(values)], axis=1)
        for at in range(0, 2 * tok, ROW_BLOCK):
            rows = slice(at, at + ROW_BLOCK)
            scores = lax.dot_general(
                stacked[rows], keys, (((1,), (1,)), ((), ())), preferred_element_type=jnp.float32
            )
            if masked:
                row = lax.broadcasted_iota(jnp.int32, scores.shape, 0) + at % tok
                col = lax.broadcasted_iota(jnp.int32, scores.shape, 1)
                scores = jnp.where(
                    col - row <= first_query - step * KEY_BLOCK, scores, -1e30
                )
            before = highest[rows]
            now = jnp.maximum(before, jnp.max(scores, axis=1, keepdims=True))
            weights = jnp.exp(scores - now[:, :1])
            shrink = jnp.exp(before - now)[:, :1]
            blended = jnp.dot(weights.astype(jnp.bfloat16), wide, preferred_element_type=jnp.float32)
            accum[rows] = accum[rows] * shrink + blended
            highest[rows] = now

    def whole(step, carry):
        update(step, False)
        return carry

    lax.fori_loop(0, last, whole, 0)
    update(last, True)
    both = accum[:, :width] / accum[:, width:]
    combined = both[:tok] - lam_ref[0] * both[tok:]
    square = jnp.mean(combined * combined, axis=1, keepdims=True)
    attended = (combined * lax.rsqrt(square + norm_eps) * gain_ref[...]).astype(jnp.bfloat16)
    share = out_ref.shape[2]
    copies = []
    for p in range(0, out_ref.shape[0], 2):
        cols = weight_ref[:, p * share : (p + 2) * share]
        part = jnp.dot(attended, cols, preferred_element_type=jnp.float32).astype(jnp.bfloat16)
        parts[p] = part[:, :share]
        parts[p + 1] = part[:, share:]
        copy = pltpu.make_async_copy(
            parts.at[pl.ds(p, 2)], out_ref.at[pl.ds(p, 2)], sems.at[p // 2]
        )
        copy.start()
        copies.append(copy)
    for copy in copies:
        copy.wait()


def attention(where, lam, q, kv, gain, weight, peers):
    tok, width = q.shape
    share = weight.shape[1] // peers
    vmem = pl.BlockSpec(memory_space=pltpu.VMEM)
    smem = pl.BlockSpec(memory_space=pltpu.SMEM)
    return pl.pallas_call(
        attention_body,
        in_specs=[smem, smem, vmem, vmem, vmem, vmem],
        out_specs=pl.BlockSpec(memory_space=pltpu.HBM),
        out_shape=jax.ShapeDtypeStruct((peers, tok, share), jnp.bfloat16),
        scratch_shapes=[
            pltpu.VMEM((2 * tok, width), jnp.bfloat16),
            pltpu.VMEM((2 * tok, 128), jnp.float32),
            pltpu.VMEM((2 * tok, 2 * width), jnp.float32),
            pltpu.VMEM((peers, tok, share), jnp.bfloat16),
            pltpu.SemaphoreType.DMA((peers // 2,)),
        ],
        compiler_params=pltpu.CompilerParams(vmem_limit_bytes=14 * 2**20),
        name="attention",
    )(where, lam, q, kv, gain, weight)


def pack_body(gate_ref, up_ref, down_ref, out_ref, sems):
    rows, width = out_ref.shape[1:]
    low, high = pl.ds(0, width), pl.ds(width, width)
    sources = (
        gate_ref.at[:, low],
        gate_ref.at[:, high],
        down_ref.at[pl.ds(0, rows)],
        down_ref.at[pl.ds(rows, rows)],
        up_ref.at[:, low],
        up_ref.at[:, high],
    )
    copies = [
        pltpu.make_async_copy(source, out_ref.at[k], sems.at[k])
        for k, source in enumerate(sources)
    ]
    for copy in copies:
        copy.start()
    for copy in copies:
        copy.wait()


def pack(gate, up, down):
    model, hidden = gate.shape
    vmem = pl.BlockSpec(memory_space=pltpu.VMEM)
    return pl.pallas_call(
        pack_body,
        in_specs=[vmem] * 3,
        out_specs=pl.BlockSpec(memory_space=pltpu.HBM),
        out_shape=jax.ShapeDtypeStruct((6, model, hidden // 2), gate.dtype),
        scratch_shapes=[pltpu.SemaphoreType.DMA((6,))],
        compiler_params=pltpu.CompilerParams(vmem_limit_bytes=8 * 2**20),
        name="pack",
    )(gate, up, down)


def arrange_body(landed_ref, out_ref):
    for k in range(out_ref.shape[0]):
        out_ref[k] = landed_ref[:, k]


def arrange(landed):
    experts, across, each, share = landed.shape
    vmem = pl.BlockSpec(memory_space=pltpu.VMEM)
    return pl.pallas_call(
        arrange_body,
        in_specs=[vmem],
        out_specs=vmem,
        out_shape=jax.ShapeDtypeStruct((across, experts, each, share), landed.dtype),
        compiler_params=pltpu.CompilerParams(vmem_limit_bytes=2 * 2**20),
        name="arrange",
    )(landed)


def project_body(parts_ref, residual_ref, place_ref, slots_ref, factors_ref, stream_ref, out_ref, slots_out, factors_out):
    slots_out[...] = slots_ref[...]
    factors_out[...] = factors_ref[...]
    total = residual_ref[...].astype(jnp.float32)
    for p in range(parts_ref.shape[0]):
        total += parts_ref[p].astype(jnp.float32)
    stream_ref[...] = total
    rows = total.astype(jnp.bfloat16)
    experts, tok = place_ref.shape
    capacity = out_ref.shape[0] // experts
    slot = lax.broadcasted_iota(jnp.int32, (capacity, tok), 0)
    for first in range(0, experts, 8):
        send = [
            jnp.where(place_ref[e : e + 1, :] == slot, 1.0, 0.0).astype(jnp.bfloat16)
            for e in range(first, first + 8)
        ]
        picked = jnp.dot(jnp.concatenate(send, axis=0), rows, preferred_element_type=jnp.float32)
        out_ref[first * capacity : (first + 8) * capacity] = picked.astype(jnp.bfloat16)


def project(parts, residual, place, slots, factors):
    _, tok, share = parts.shape
    experts = place.shape[0]
    rows = tok // (experts // GROUPS) * experts
    vmem = pl.BlockSpec(memory_space=pltpu.VMEM)
    return pl.pallas_call(
        project_body,
        in_specs=[vmem] * 5,
        out_specs=[vmem] * 4,
        out_shape=[
            jax.ShapeDtypeStruct((tok, share), jnp.float32),
            jax.ShapeDtypeStruct((rows, share), jnp.bfloat16),
            jax.ShapeDtypeStruct(slots.shape, slots.dtype),
            jax.ShapeDtypeStruct(factors.shape, factors.dtype),
        ],
        compiler_params=pltpu.CompilerParams(vmem_limit_bytes=16 * 2**20),
        name="project",
    )(parts, residual, place, slots, factors)


def combine_body(back_ref, stream_ref, slots_ref, factors_ref, out_ref):
    tok = stream_ref.shape[0]
    rows = back_ref.shape[0]
    slot = lax.broadcasted_iota(jnp.int32, (tok, rows), 1)
    total = stream_ref[...]
    for k in range(slots_ref.shape[1]):
        take = jnp.where(slots_ref[:, k : k + 1] == slot, 1.0, 0.0).astype(jnp.bfloat16)
        found = jnp.dot(take, back_ref[...], preferred_element_type=jnp.float32)
        total += factors_ref[:, k : k + 1] * found
    done = total.astype(jnp.bfloat16)
    for p in range(out_ref.shape[0]):
        out_ref[p] = done


def combine(back, stream, slots, factors, peers):
    tok, share = stream.shape
    vmem = pl.BlockSpec(memory_space=pltpu.VMEM)
    return pl.pallas_call(
        combine_body,
        in_specs=[vmem] * 4,
        out_specs=vmem,
        out_shape=jax.ShapeDtypeStruct((peers, tok, share), jnp.bfloat16),
        compiler_params=pltpu.CompilerParams(vmem_limit_bytes=16 * 2**20),
        name="combine",
    )(back, stream, slots, factors)


def hidden_body(turn_ref, rows_ref, gain_ref, own_ref, one_ref, two_ref, three_ref, out_ref, normed_ref, weights, sems):
    peers, count, share = rows_ref.shape
    pieces = out_ref.shape[0]
    gate, up = pl.ds(0, 2), pl.ds(4, 2)
    first, second = pl.ds(0, 2), pl.ds(2, 2)
    groups = [
        [(source.at[gate], weights.at[k, first]), (source.at[up], weights.at[k, second])]
        for k, source in enumerate((own_ref, one_ref, two_ref, three_ref))
    ]
    copies, at = [], 0
    for group in groups:
        started = []
        for source, target in group:
            copy = pltpu.make_async_copy(source, target, sems.at[at])
            copy.start()
            started.append(copy)
            at += 1
        copies.append(started)
    total = jnp.zeros((count, 1), jnp.float32)
    for p in range(peers):
        part = rows_ref[p].astype(jnp.float32)
        total += jnp.sum(part * part, axis=1, keepdims=True)
    scale = lax.rsqrt(total / (peers * share) + norm_eps)
    for p in range(peers):
        cols = slice(p * share, (p + 1) * share)
        normed_ref[:, cols] = (rows_ref[p].astype(jnp.float32) * scale * gain_ref[:, cols]).astype(
            jnp.bfloat16
        )
    for k, started in enumerate(copies):
        for copy in started:
            copy.wait()
        normed = normed_ref[...]
        gates = jnp.concatenate([weights[k, 0], weights[k, 1]], axis=1)
        ups = jnp.concatenate([weights[k, 2], weights[k, 3]], axis=1)
        gate = jnp.dot(normed, gates, preferred_element_type=jnp.float32)
        up = jnp.dot(normed, ups, preferred_element_type=jnp.float32)
        act = gate / (1.0 + jnp.exp(-gate)) * up
        out_ref[lax.rem(turn_ref[0] + k * turn_ref[1], pieces)] = act.astype(jnp.bfloat16)


def hidden_units(turn, rows, gain, *weights):
    peers, count, share = rows.shape
    _, model, half = weights[0].shape
    vmem = pl.BlockSpec(memory_space=pltpu.VMEM)
    anywhere = pl.BlockSpec(memory_space=pltpu.HBM)
    return pl.pallas_call(
        hidden_body,
        in_specs=[pl.BlockSpec(memory_space=pltpu.SMEM), vmem, vmem] + [anywhere] * len(weights),
        out_specs=vmem,
        out_shape=jax.ShapeDtypeStruct((4, count, 2 * half), jnp.bfloat16),
        scratch_shapes=[
            pltpu.VMEM((count, peers * share), jnp.bfloat16),
            pltpu.VMEM((4, 4, model, half), jnp.bfloat16),
            pltpu.SemaphoreType.DMA((8,)),
        ],
        compiler_params=pltpu.CompilerParams(vmem_limit_bytes=24 * 2**20),
        name="hidden",
    )(turn, rows, gain, *weights)


def down_body(turn_ref, units_ref, own_ref, one_ref, two_ref, three_ref, out_ref, downs, sems):
    blocks, count, hidden = units_ref.shape
    chips, pieces, rows_each, _ = out_ref.shape
    parts = sems.shape[0]
    half, share = own_ref.shape[1:]
    step = 2 * half // parts
    copies = []
    for c in range(parts):
        at = c * step
        rows = pl.ds(at, step)
        inner = pl.ds(at % half, step)
        page = at // half
        sources = [
            source.at[2 + page, inner] for source in (own_ref, one_ref, two_ref, three_ref)
        ]
        for k, source in enumerate(sources):
            copy = pltpu.make_async_copy(source, downs.at[k, rows], sems.at[c, k])
            copy.start()
            copies.append(copy)
    first = jnp.zeros((count, 2 * share), jnp.float32)
    second = jnp.zeros((count, 2 * share), jnp.float32)
    for p in range(blocks):
        if p % (blocks // parts) == 0:
            c = p // (blocks // parts)
            for copy in copies[c * pieces : (c + 1) * pieces]:
                copy.wait()
        rows = slice(p * hidden, (p + 1) * hidden)
        units = units_ref[p]
        near = jnp.concatenate([downs[0, rows], downs[1, rows]], axis=1)
        rest = jnp.concatenate([downs[2, rows], downs[3, rows]], axis=1)
        first += jnp.dot(units, near, preferred_element_type=jnp.float32)
        second += jnp.dot(units, rest, preferred_element_type=jnp.float32)
    made = (first[:, :share], first[:, share:], second[:, :share], second[:, share:])
    for k, value in enumerate(made):
        at = lax.rem(turn_ref[0] + k * turn_ref[1], pieces)
        out_ref[:, at] = value.reshape(chips, rows_each, share).astype(jnp.bfloat16)


def down_product(turn, units, chips, *downs):
    _, count, _ = units.shape
    _, half, share = downs[0].shape
    vmem = pl.BlockSpec(memory_space=pltpu.VMEM)
    anywhere = pl.BlockSpec(memory_space=pltpu.HBM)
    return pl.pallas_call(
        down_body,
        in_specs=[pl.BlockSpec(memory_space=pltpu.SMEM), vmem] + [anywhere] * len(downs),
        out_specs=vmem,
        out_shape=jax.ShapeDtypeStruct((chips, 4, count // chips, share), jnp.bfloat16),
        scratch_shapes=[
            pltpu.VMEM((4, 2 * half, share), jnp.bfloat16),
            pltpu.SemaphoreType.DMA((4, 4)),
        ],
        compiler_params=pltpu.CompilerParams(vmem_limit_bytes=24 * 2**20),
        name="down",
    )(turn, units, *downs)


def assemble_body(whole_ref, out_ref):
    peers, _, share = whole_ref.shape
    for p in range(peers):
        out_ref[:, p * share : (p + 1) * share] = whole_ref[p]


def assemble(whole):
    peers, tok, share = whole.shape
    tile = tok // 4
    return pl.pallas_call(
        assemble_body,
        grid=(4,),
        in_specs=[pl.BlockSpec((peers, tile, share), lambda i: (0, i, 0))],
        out_specs=pl.BlockSpec((tile, peers * share), lambda i: (i, 0)),
        out_shape=jax.ShapeDtypeStruct((tok, peers * share), whole.dtype),
        compiler_params=pltpu.CompilerParams(
            dimension_semantics=("arbitrary",), vmem_limit_bytes=16 * 2**20
        ),
        name="assemble",
    )(whole)


def gathered(array, axes, axis, scale):
    sent = (array.astype(jnp.float32) * scale).astype(jnp.float16)
    whole = lax.all_gather(sent, axes, axis=axis, tiled=True)
    return (whole.astype(jnp.float32) * (1.0 / scale)).astype(jnp.bfloat16)


def shards(
    residual,
    queries,
    key_vectors,
    value_rows,
    head_lambda,
    head_gain,
    out_weight,
    ffn_gain,
    expert_gate,
    expert_up,
    expert_down,
    routing,
    route_weight,
):
    tok, _, _ = queries.shape
    sp = ("z", "c")
    experts = lax.axis_size(sp)
    across = lax.axis_size("x")
    along = lax.axis_size("y")
    tp = ("y", "x")
    peers = across * along
    model = residual.shape[1]
    share = model // peers
    where = lax.axis_index(sp).astype(jnp.int32)[None]
    core = lax.axis_index("c")
    turn = jnp.stack([lax.axis_index("x"), 3 - 2 * core]).astype(jnp.int32)
    column = (lax.axis_index("y") * across + lax.axis_index("x")) * share

    round_x = [(i, (i + 1) % across) for i in range(across)]
    round_x += [(across + i, across + (i - 1) % across) for i in range(across)]
    packed = pack(expert_gate[0], expert_up[0], expert_down[0])
    one = lax.ppermute(packed, ("c", "x"), round_x)
    two = lax.ppermute(one, ("c", "x"), round_x)
    three = lax.ppermute(two, ("c", "x"), round_x)

    kv = jnp.concatenate([key_vectors[:, 0], value_rows[:, 0]], axis=1)
    kv_all = gathered(kv, sp, 0, SHIFT)
    own_residual = lax.dynamic_slice_in_dim(residual, column, share, 1)

    capacity = tok // (experts // GROUPS)
    order = jnp.arange(tok, dtype=jnp.int32)
    ids = jnp.arange(experts, dtype=jnp.int32)
    named = routing[:, :, None] == ids
    member = jnp.any(named, axis=1)
    strict = (order[None, :] < order[:, None]).astype(jnp.bfloat16)
    earlier = jnp.dot(
        strict, member.astype(jnp.bfloat16), preferred_element_type=jnp.float32
    ).astype(jnp.int32)
    place = jnp.where(member, earlier, -1).T
    picked = jnp.sum(jnp.where(named, earlier[:, None, :], 0), axis=2)
    slots = routing * capacity + picked

    partial = attention(
        where, head_lambda, queries[:, 0], kv_all, head_gain[None], out_weight, peers
    )
    parts = lax.all_to_all(partial, tp, 0, 0, tiled=True)
    own_stream, outgoing, slots, factors = project(
        parts, own_residual, place, slots, route_weight
    )
    targets = experts * across
    each = capacity // across
    landed = lax.all_to_all(
        outgoing.reshape(targets, each, share), ("z", "c", "x"), 0, 0, tiled=True
    )
    landed = arrange(landed.reshape(experts, across, each, share))
    rows = gathered(landed.reshape(across, experts * each, share), "y", 0, 64.0)
    units = hidden_units(
        turn, rows, ffn_gain[None], packed, one, two, three
    )
    all_units = gathered(units, "y", 0, 0.25)
    made = down_product(turn, all_units, experts, packed, one, two, three)
    back = lax.all_to_all(
        made.reshape(targets, each, share), ("z", "c", "x"), 0, 0, tiled=True
    )
    back = back.reshape(experts * capacity, share)
    spread = combine(back, own_stream, slots, factors, peers)
    whole = lax.all_to_all(spread, tp, 0, 0, tiled=True)
    return assemble(whole)


def solution(mesh):
    sizes = mesh.devices.shape
    split = jax.sharding.Mesh(
        mesh.devices.reshape(sizes[0] // 2, 2, sizes[1] // 4, 4), ("z", "c", "y", "x")
    )
    sp, tp = ("z", "c"), ("y", "x")
    in_specs = (
        P(sp, None),
        P(sp, tp, None),
        P(sp, tp, None),
        P(sp, tp, None),
        P(tp),
        P(),
        P(tp, None),
        P(),
        P(sp, None, tp),
        P(sp, None, tp),
        P(sp, None, tp),
        P(sp, None),
        P(sp, None),
    )
    return jax.shard_map(
        shards, mesh=split, in_specs=in_specs, out_specs=P(sp, None), check_vma=False
    )
```

```python
import jax
import jax.numpy as jnp
from jax import lax
from jax.experimental import pallas as pl
from jax.experimental.pallas import tpu as pltpu
from jax.sharding import PartitionSpec as P

norm_eps = 1e-06
KEY_BLOCK = 2048
ROW_BLOCK = 128
SHIFT = 4096.0
GROUPS = 4


def attention_body(where_ref, lam_ref, q_ref, kv_ref, gain_ref, weight_ref, out_ref, stacked, highest, accum, parts, sems):
    tok, width = q_ref.shape
    first_query = where_ref[0] * tok
    last = (first_query + tok - 1) // KEY_BLOCK
    scaled = q_ref[...] * jnp.asarray((width // 2) ** -0.5, jnp.bfloat16)
    low = lax.broadcasted_iota(jnp.int32, scaled.shape, 1) < width // 2
    zero = jnp.zeros_like(scaled)
    stacked[:tok] = jnp.where(low, scaled, zero)
    stacked[tok:] = jnp.where(low, zero, scaled)
    highest[...] = jnp.full(highest.shape, -1e30, jnp.float32)
    accum[...] = jnp.zeros(accum.shape, jnp.float32)

    def update(step, masked):
        block = kv_ref[pl.ds(pl.multiple_of(step * KEY_BLOCK, KEY_BLOCK), KEY_BLOCK), :]
        keys, values = block[:, :width], block[:, width:]
        wide = jnp.concatenate([values, jnp.ones_like(values)], axis=1)
        for at in range(0, 2 * tok, ROW_BLOCK):
            rows = slice(at, at + ROW_BLOCK)
            scores = lax.dot_general(
                stacked[rows], keys, (((1,), (1,)), ((), ())), preferred_element_type=jnp.float32
            )
            if masked:
                row = lax.broadcasted_iota(jnp.int32, scores.shape, 0) + at % tok
                col = lax.broadcasted_iota(jnp.int32, scores.shape, 1)
                scores = jnp.where(
                    col - row <= first_query - step * KEY_BLOCK, scores, -1e30
                )
            before = highest[rows]
            now = jnp.maximum(before, jnp.max(scores, axis=1, keepdims=True))
            weights = jnp.exp(scores - now[:, :1])
            shrink = jnp.exp(before - now)[:, :1]
            blended = jnp.dot(weights.astype(jnp.bfloat16), wide, preferred_element_type=jnp.float32)
            accum[rows] = accum[rows] * shrink + blended
            highest[rows] = now

    def whole(step, carry):
        update(step, False)
        return carry

    lax.fori_loop(0, last, whole, 0)
    update(last, True)
    both = accum[:, :width] / accum[:, width:]
    combined = both[:tok] - lam_ref[0] * both[tok:]
    square = jnp.mean(combined * combined, axis=1, keepdims=True)
    attended = (combined * lax.rsqrt(square + norm_eps) * gain_ref[...]).astype(jnp.bfloat16)
    share = out_ref.shape[2]
    copies = []
    for p in range(0, out_ref.shape[0], 2):
        cols = weight_ref[:, p * share : (p + 2) * share]
        part = jnp.dot(attended, cols, preferred_element_type=jnp.float32).astype(jnp.bfloat16)
        parts[p] = part[:, :share]
        parts[p + 1] = part[:, share:]
        copy = pltpu.make_async_copy(
            parts.at[pl.ds(p, 2)], out_ref.at[pl.ds(p, 2)], sems.at[p // 2]
        )
        copy.start()
        copies.append(copy)
    for copy in copies:
        copy.wait()


def attention(where, lam, q, kv, gain, weight, peers):
    tok, width = q.shape
    share = weight.shape[1] // peers
    vmem = pl.BlockSpec(memory_space=pltpu.VMEM)
    smem = pl.BlockSpec(memory_space=pltpu.SMEM)
    return pl.pallas_call(
        attention_body,
        in_specs=[smem, smem, vmem, vmem, vmem, vmem],
        out_specs=pl.BlockSpec(memory_space=pltpu.HBM),
        out_shape=jax.ShapeDtypeStruct((peers, tok, share), jnp.bfloat16),
        scratch_shapes=[
            pltpu.VMEM((2 * tok, width), jnp.bfloat16),
            pltpu.VMEM((2 * tok, 128), jnp.float32),
            pltpu.VMEM((2 * tok, 2 * width), jnp.float32),
            pltpu.VMEM((peers, tok, share), jnp.bfloat16),
            pltpu.SemaphoreType.DMA((peers // 2,)),
        ],
        compiler_params=pltpu.CompilerParams(vmem_limit_bytes=14 * 2**20),
        name="attention",
    )(where, lam, q, kv, gain, weight)


def pack_body(gate_ref, up_ref, down_ref, out_ref, sems):
    rows, width = out_ref.shape[1:]
    low, high = pl.ds(0, width), pl.ds(width, width)
    sources = (
        gate_ref.at[:, low],
        gate_ref.at[:, high],
        down_ref.at[pl.ds(0, rows)],
        down_ref.at[pl.ds(rows, rows)],
        up_ref.at[:, low],
        up_ref.at[:, high],
    )
    copies = [
        pltpu.make_async_copy(source, out_ref.at[k], sems.at[k])
        for k, source in enumerate(sources)
    ]
    for copy in copies:
        copy.start()
    for copy in copies:
        copy.wait()


def pack(gate, up, down):
    model, hidden = gate.shape
    vmem = pl.BlockSpec(memory_space=pltpu.VMEM)
    return pl.pallas_call(
        pack_body,
        in_specs=[vmem] * 3,
        out_specs=pl.BlockSpec(memory_space=pltpu.HBM),
        out_shape=jax.ShapeDtypeStruct((6, model, hidden // 2), gate.dtype),
        scratch_shapes=[pltpu.SemaphoreType.DMA((6,))],
        compiler_params=pltpu.CompilerParams(vmem_limit_bytes=8 * 2**20),
        name="pack",
    )(gate, up, down)


def arrange_body(landed_ref, out_ref):
    for k in range(out_ref.shape[0]):
        out_ref[k] = landed_ref[:, k]


def arrange(landed):
    experts, across, each, share = landed.shape
    vmem = pl.BlockSpec(memory_space=pltpu.VMEM)
    return pl.pallas_call(
        arrange_body,
        in_specs=[vmem],
        out_specs=vmem,
        out_shape=jax.ShapeDtypeStruct((across, experts, each, share), landed.dtype),
        compiler_params=pltpu.CompilerParams(vmem_limit_bytes=2 * 2**20),
        name="arrange",
    )(landed)


def project_body(parts_ref, residual_ref, place_ref, slots_ref, factors_ref, stream_ref, out_ref, slots_out, factors_out):
    slots_out[...] = slots_ref[...]
    factors_out[...] = factors_ref[...]
    total = residual_ref[...].astype(jnp.float32)
    for p in range(parts_ref.shape[0]):
        total += parts_ref[p].astype(jnp.float32)
    stream_ref[...] = total
    rows = total.astype(jnp.bfloat16)
    experts, tok = place_ref.shape
    capacity = out_ref.shape[0] // experts
    slot = lax.broadcasted_iota(jnp.int32, (capacity, tok), 0)
    for first in range(0, experts, 8):
        send = [
            jnp.where(place_ref[e : e + 1, :] == slot, 1.0, 0.0).astype(jnp.bfloat16)
            for e in range(first, first + 8)
        ]
        picked = jnp.dot(jnp.concatenate(send, axis=0), rows, preferred_element_type=jnp.float32)
        out_ref[first * capacity : (first + 8) * capacity] = picked.astype(jnp.bfloat16)


def project(parts, residual, place, slots, factors):
    _, tok, share = parts.shape
    experts = place.shape[0]
    rows = tok // (experts // GROUPS) * experts
    vmem = pl.BlockSpec(memory_space=pltpu.VMEM)
    return pl.pallas_call(
        project_body,
        in_specs=[vmem] * 5,
        out_specs=[vmem] * 4,
        out_shape=[
            jax.ShapeDtypeStruct((tok, share), jnp.float32),
            jax.ShapeDtypeStruct((rows, share), jnp.bfloat16),
            jax.ShapeDtypeStruct(slots.shape, slots.dtype),
            jax.ShapeDtypeStruct(factors.shape, factors.dtype),
        ],
        compiler_params=pltpu.CompilerParams(vmem_limit_bytes=16 * 2**20),
        name="project",
    )(parts, residual, place, slots, factors)


def combine_body(back_ref, stream_ref, slots_ref, factors_ref, out_ref):
    tok = stream_ref.shape[0]
    rows = back_ref.shape[0]
    slot = lax.broadcasted_iota(jnp.int32, (tok, rows), 1)
    total = stream_ref[...]
    for k in range(slots_ref.shape[1]):
        take = jnp.where(slots_ref[:, k : k + 1] == slot, 1.0, 0.0).astype(jnp.bfloat16)
        found = jnp.dot(take, back_ref[...], preferred_element_type=jnp.float32)
        total += factors_ref[:, k : k + 1] * found
    done = total.astype(jnp.bfloat16)
    for p in range(out_ref.shape[0]):
        out_ref[p] = done


def combine(back, stream, slots, factors, peers):
    tok, share = stream.shape
    vmem = pl.BlockSpec(memory_space=pltpu.VMEM)
    return pl.pallas_call(
        combine_body,
        in_specs=[vmem] * 4,
        out_specs=vmem,
        out_shape=jax.ShapeDtypeStruct((peers, tok, share), jnp.bfloat16),
        compiler_params=pltpu.CompilerParams(vmem_limit_bytes=16 * 2**20),
        name="combine",
    )(back, stream, slots, factors)


def hidden_body(turn_ref, rows_ref, gain_ref, own_ref, own_up_ref, one_ref, two_ref, three_ref, out_ref, normed_ref, weights, sems):
    peers, count, share = rows_ref.shape
    pieces = out_ref.shape[0]
    gate, up = pl.ds(0, 2), pl.ds(4, 2)
    first, second = pl.ds(0, 2), pl.ds(2, 2)
    width = weights.shape[3]
    low, high = pl.ds(0, width), pl.ds(width, width)
    groups = [
        [
            (own_ref.at[:, low], weights.at[0, 0]),
            (own_ref.at[:, high], weights.at[0, 1]),
            (own_up_ref.at[:, low], weights.at[0, 2]),
            (own_up_ref.at[:, high], weights.at[0, 3]),
        ]
    ]
    groups += [
        [(source.at[gate], weights.at[k, first]), (source.at[up], weights.at[k, second])]
        for k, source in ((1, one_ref), (2, two_ref), (3, three_ref))
    ]
    copies, at = [], 0
    for group in groups:
        started = []
        for source, target in group:
            copy = pltpu.make_async_copy(source, target, sems.at[at])
            copy.start()
            started.append(copy)
            at += 1
        copies.append(started)
    total = jnp.zeros((count, 1), jnp.float32)
    for p in range(peers):
        part = rows_ref[p].astype(jnp.float32)
        total += jnp.sum(part * part, axis=1, keepdims=True)
    scale = lax.rsqrt(total / (peers * share) + norm_eps)
    for p in range(peers):
        cols = slice(p * share, (p + 1) * share)
        normed_ref[:, cols] = (rows_ref[p].astype(jnp.float32) * scale * gain_ref[:, cols]).astype(
            jnp.bfloat16
        )
    for k, started in enumerate(copies):
        for copy in started:
            copy.wait()
        normed = normed_ref[...]
        gates = jnp.concatenate([weights[k, 0], weights[k, 1]], axis=1)
        ups = jnp.concatenate([weights[k, 2], weights[k, 3]], axis=1)
        gate = jnp.dot(normed, gates, preferred_element_type=jnp.float32)
        up = jnp.dot(normed, ups, preferred_element_type=jnp.float32)
        act = gate / (1.0 + jnp.exp(-gate)) * up
        out_ref[lax.rem(turn_ref[0] + k * turn_ref[1], pieces)] = act.astype(jnp.bfloat16)


def hidden_units(turn, rows, gain, *weights):
    peers, count, share = rows.shape
    _, model, half = weights[-1].shape
    vmem = pl.BlockSpec(memory_space=pltpu.VMEM)
    anywhere = pl.BlockSpec(memory_space=pltpu.HBM)
    return pl.pallas_call(
        hidden_body,
        in_specs=[pl.BlockSpec(memory_space=pltpu.SMEM), vmem, vmem] + [anywhere] * len(weights),
        out_specs=vmem,
        out_shape=jax.ShapeDtypeStruct((4, count, 2 * half), jnp.bfloat16),
        scratch_shapes=[
            pltpu.VMEM((count, peers * share), jnp.bfloat16),
            pltpu.VMEM((4, 4, model, half), jnp.bfloat16),
            pltpu.SemaphoreType.DMA((10,)),
        ],
        compiler_params=pltpu.CompilerParams(vmem_limit_bytes=24 * 2**20),
        name="hidden",
    )(turn, rows, gain, *weights)


def down_body(turn_ref, units_ref, own_ref, one_ref, two_ref, three_ref, out_ref, downs, sems):
    blocks, count, hidden = units_ref.shape
    chips, pieces, rows_each, _ = out_ref.shape
    parts = sems.shape[0]
    half, share = one_ref.shape[1:]
    step = 2 * half // parts
    copies = []
    for c in range(parts):
        at = c * step
        rows = pl.ds(at, step)
        inner = pl.ds(at % half, step)
        page = at // half
        sources = [own_ref.at[rows]] + [
            source.at[2 + page, inner] for source in (one_ref, two_ref, three_ref)
        ]
        for k, source in enumerate(sources):
            copy = pltpu.make_async_copy(source, downs.at[k, rows], sems.at[c, k])
            copy.start()
            copies.append(copy)
    first = jnp.zeros((count, 2 * share), jnp.float32)
    second = jnp.zeros((count, 2 * share), jnp.float32)
    for p in range(blocks):
        if p % (blocks // parts) == 0:
            c = p // (blocks // parts)
            for copy in copies[c * pieces : (c + 1) * pieces]:
                copy.wait()
        rows = slice(p * hidden, (p + 1) * hidden)
        units = units_ref[p]
        near = jnp.concatenate([downs[0, rows], downs[1, rows]], axis=1)
        rest = jnp.concatenate([downs[2, rows], downs[3, rows]], axis=1)
        first += jnp.dot(units, near, preferred_element_type=jnp.float32)
        second += jnp.dot(units, rest, preferred_element_type=jnp.float32)
    made = (first[:, :share], first[:, share:], second[:, :share], second[:, share:])
    for k, value in enumerate(made):
        at = lax.rem(turn_ref[0] + k * turn_ref[1], pieces)
        out_ref[:, at] = value.reshape(chips, rows_each, share).astype(jnp.bfloat16)


def down_product(turn, units, chips, *downs):
    _, count, _ = units.shape
    _, half, share = downs[-1].shape
    vmem = pl.BlockSpec(memory_space=pltpu.VMEM)
    anywhere = pl.BlockSpec(memory_space=pltpu.HBM)
    return pl.pallas_call(
        down_body,
        in_specs=[pl.BlockSpec(memory_space=pltpu.SMEM), vmem] + [anywhere] * len(downs),
        out_specs=vmem,
        out_shape=jax.ShapeDtypeStruct((chips, 4, count // chips, share), jnp.bfloat16),
        scratch_shapes=[
            pltpu.VMEM((4, 2 * half, share), jnp.bfloat16),
            pltpu.SemaphoreType.DMA((4, 4)),
        ],
        compiler_params=pltpu.CompilerParams(vmem_limit_bytes=24 * 2**20),
        name="down",
    )(turn, units, *downs)


def assemble_body(whole_ref, out_ref):
    peers, _, share = whole_ref.shape
    for p in range(peers):
        out_ref[:, p * share : (p + 1) * share] = whole_ref[p]


def assemble(whole):
    peers, tok, share = whole.shape
    tile = tok // 4
    return pl.pallas_call(
        assemble_body,
        grid=(4,),
        in_specs=[pl.BlockSpec((peers, tile, share), lambda i: (0, i, 0))],
        out_specs=pl.BlockSpec((tile, peers * share), lambda i: (i, 0)),
        out_shape=jax.ShapeDtypeStruct((tok, peers * share), whole.dtype),
        compiler_params=pltpu.CompilerParams(
            dimension_semantics=("arbitrary",), vmem_limit_bytes=16 * 2**20
        ),
        name="assemble",
    )(whole)


def gathered(array, axes, axis, scale):
    sent = (array.astype(jnp.float32) * scale).astype(jnp.float16)
    whole = lax.all_gather(sent, axes, axis=axis, tiled=True)
    return (whole.astype(jnp.float32) * (1.0 / scale)).astype(jnp.bfloat16)


def shards(
    residual,
    queries,
    key_vectors,
    value_rows,
    head_lambda,
    head_gain,
    out_weight,
    ffn_gain,
    expert_gate,
    expert_up,
    expert_down,
    routing,
    route_weight,
):
    tok, _, _ = queries.shape
    sp = ("z", "c")
    experts = lax.axis_size(sp)
    across = lax.axis_size("x")
    along = lax.axis_size("y")
    tp = ("y", "x")
    peers = across * along
    model = residual.shape[1]
    share = model // peers
    where = lax.axis_index(sp).astype(jnp.int32)[None]
    core = lax.axis_index("c")
    turn = jnp.stack([lax.axis_index("x"), 3 - 2 * core]).astype(jnp.int32)
    column = (lax.axis_index("y") * across + lax.axis_index("x")) * share

    round_x = [(i, (i + 1) % across) for i in range(across)]
    round_x += [(across + i, across + (i - 1) % across) for i in range(across)]
    packed = pack(expert_gate[0], expert_up[0], expert_down[0])
    one = lax.ppermute(packed, ("c", "x"), round_x)
    two = lax.ppermute(one, ("c", "x"), round_x)
    three = lax.ppermute(two, ("c", "x"), round_x)

    kv = jnp.concatenate([key_vectors[:, 0], value_rows[:, 0]], axis=1)
    kv_all = gathered(kv, sp, 0, SHIFT)
    own_residual = lax.dynamic_slice_in_dim(residual, column, share, 1)

    capacity = tok // (experts // GROUPS)
    order = jnp.arange(tok, dtype=jnp.int32)
    ids = jnp.arange(experts, dtype=jnp.int32)
    named = routing[:, :, None] == ids
    member = jnp.any(named, axis=1)
    strict = (order[None, :] < order[:, None]).astype(jnp.bfloat16)
    earlier = jnp.dot(
        strict, member.astype(jnp.bfloat16), preferred_element_type=jnp.float32
    ).astype(jnp.int32)
    place = jnp.where(member, earlier, -1).T
    picked = jnp.sum(jnp.where(named, earlier[:, None, :], 0), axis=2)
    slots = routing * capacity + picked

    partial = attention(
        where, head_lambda, queries[:, 0], kv_all, head_gain[None], out_weight, peers
    )
    parts = lax.all_to_all(partial, tp, 0, 0, tiled=True)
    own_stream, outgoing, slots, factors = project(
        parts, own_residual, place, slots, route_weight
    )
    targets = experts * across
    each = capacity // across
    landed = lax.all_to_all(
        outgoing.reshape(targets, each, share), ("z", "c", "x"), 0, 0, tiled=True
    )
    landed = arrange(landed.reshape(experts, across, each, share))
    rows = gathered(landed.reshape(across, experts * each, share), "y", 0, 64.0)
    units = hidden_units(
        turn, rows, ffn_gain[None], expert_gate[0], expert_up[0], one, two, three
    )
    all_units = gathered(units, "y", 0, 0.25)
    made = down_product(turn, all_units, experts, expert_down[0], one, two, three)
    back = lax.all_to_all(
        made.reshape(targets, each, share), ("z", "c", "x"), 0, 0, tiled=True
    )
    back = back.reshape(experts * capacity, share)
    spread = combine(back, own_stream, slots, factors, peers)
    whole = lax.all_to_all(spread, tp, 0, 0, tiled=True)
    return assemble(whole)


def solution(mesh):
    sizes = mesh.devices.shape
    split = jax.sharding.Mesh(
        mesh.devices.reshape(sizes[0] // 2, 2, sizes[1] // 4, 4), ("z", "c", "y", "x")
    )
    sp, tp = ("z", "c"), ("y", "x")
    in_specs = (
        P(sp, None),
        P(sp, tp, None),
        P(sp, tp, None),
        P(sp, tp, None),
        P(tp),
        P(),
        P(tp, None),
        P(),
        P(sp, None, tp),
        P(sp, None, tp),
        P(sp, None, tp),
        P(sp, None),
        P(sp, None),
    )
    return jax.shard_map(
        shards, mesh=split, in_specs=in_specs, out_specs=P(sp, None), check_vma=False
    )
```

```python
import jax
import jax.numpy as jnp
from jax import lax
from jax.experimental import pallas as pl
from jax.experimental.pallas import tpu as pltpu
from jax.sharding import PartitionSpec as P

norm_eps = 1e-06
KEY_BLOCK = 2048
ROW_BLOCK = 128
SHIFT = 4096.0
GROUPS = 4


def attention_body(where_ref, lam_ref, q_ref, kv_ref, gain_ref, weight_ref, out_ref, stacked, highest, accum, parts, sems):
    tok, width = q_ref.shape
    first_query = where_ref[0] * tok
    last = (first_query + tok - 1) // KEY_BLOCK
    scaled = q_ref[...] * jnp.asarray((width // 2) ** -0.5, jnp.bfloat16)
    low = lax.broadcasted_iota(jnp.int32, scaled.shape, 1) < width // 2
    zero = jnp.zeros_like(scaled)
    stacked[:tok] = jnp.where(low, scaled, zero)
    stacked[tok:] = jnp.where(low, zero, scaled)
    highest[...] = jnp.full(highest.shape, -1e30, jnp.float32)
    accum[...] = jnp.zeros(accum.shape, jnp.float32)

    def update(step, masked):
        block = kv_ref[pl.ds(pl.multiple_of(step * KEY_BLOCK, KEY_BLOCK), KEY_BLOCK), :]
        keys, values = block[:, :width], block[:, width:]
        wide = jnp.concatenate([values, jnp.ones_like(values)], axis=1)
        for at in range(0, 2 * tok, ROW_BLOCK):
            rows = slice(at, at + ROW_BLOCK)
            scores = lax.dot_general(
                stacked[rows], keys, (((1,), (1,)), ((), ())), preferred_element_type=jnp.float32
            )
            if masked:
                row = lax.broadcasted_iota(jnp.int32, scores.shape, 0) + at % tok
                col = lax.broadcasted_iota(jnp.int32, scores.shape, 1)
                scores = jnp.where(
                    col - row <= first_query - step * KEY_BLOCK, scores, -1e30
                )
            before = highest[rows]
            now = jnp.maximum(before, jnp.max(scores, axis=1, keepdims=True))
            weights = jnp.exp(scores - now[:, :1])
            shrink = jnp.exp(before - now)[:, :1]
            blended = jnp.dot(weights.astype(jnp.bfloat16), wide, preferred_element_type=jnp.float32)
            accum[rows] = accum[rows] * shrink + blended
            highest[rows] = now

    def whole(step, carry):
        update(step, False)
        return carry

    lax.fori_loop(0, last, whole, 0)
    update(last, True)
    both = accum[:, :width] / accum[:, width:]
    combined = both[:tok] - lam_ref[0] * both[tok:]
    square = jnp.mean(combined * combined, axis=1, keepdims=True)
    attended = (combined * lax.rsqrt(square + norm_eps) * gain_ref[...]).astype(jnp.bfloat16)
    share = out_ref.shape[2]
    copies = []
    for p in range(0, out_ref.shape[0], 2):
        cols = weight_ref[:, p * share : (p + 2) * share]
        part = jnp.dot(attended, cols, preferred_element_type=jnp.float32).astype(jnp.bfloat16)
        parts[p] = part[:, :share]
        parts[p + 1] = part[:, share:]
        copy = pltpu.make_async_copy(
            parts.at[pl.ds(p, 2)], out_ref.at[pl.ds(p, 2)], sems.at[p // 2]
        )
        copy.start()
        copies.append(copy)
    for copy in copies:
        copy.wait()


def attention(where, lam, q, kv, gain, weight, peers):
    tok, width = q.shape
    share = weight.shape[1] // peers
    vmem = pl.BlockSpec(memory_space=pltpu.VMEM)
    smem = pl.BlockSpec(memory_space=pltpu.SMEM)
    return pl.pallas_call(
        attention_body,
        in_specs=[smem, smem, vmem, vmem, vmem, vmem],
        out_specs=pl.BlockSpec(memory_space=pltpu.HBM),
        out_shape=jax.ShapeDtypeStruct((peers, tok, share), jnp.bfloat16),
        scratch_shapes=[
            pltpu.VMEM((2 * tok, width), jnp.bfloat16),
            pltpu.VMEM((2 * tok, 128), jnp.float32),
            pltpu.VMEM((2 * tok, 2 * width), jnp.float32),
            pltpu.VMEM((peers, tok, share), jnp.bfloat16),
            pltpu.SemaphoreType.DMA((peers // 2,)),
        ],
        compiler_params=pltpu.CompilerParams(vmem_limit_bytes=14 * 2**20),
        name="attention",
    )(where, lam, q, kv, gain, weight)


def pack_body(gate_ref, up_ref, down_ref, out_ref, sems):
    rows, width = out_ref.shape[1:]
    low, high = pl.ds(0, width), pl.ds(width, width)
    sources = (
        gate_ref.at[:, low],
        gate_ref.at[:, high],
        down_ref.at[pl.ds(0, rows)],
        down_ref.at[pl.ds(rows, rows)],
        up_ref.at[:, low],
        up_ref.at[:, high],
    )
    copies = [
        pltpu.make_async_copy(source, out_ref.at[k], sems.at[k])
        for k, source in enumerate(sources)
    ]
    for copy in copies:
        copy.start()
    for copy in copies:
        copy.wait()


def pack(gate, up, down):
    model, hidden = gate.shape
    return pl.pallas_call(
        pack_body,
        in_specs=[pl.BlockSpec(memory_space=pltpu.HBM)] * 3,
        out_specs=pl.BlockSpec(memory_space=pltpu.HBM),
        out_shape=jax.ShapeDtypeStruct((6, model, hidden // 2), gate.dtype),
        scratch_shapes=[pltpu.SemaphoreType.DMA((6,))],
        compiler_params=pltpu.CompilerParams(vmem_limit_bytes=4 * 2**20),
        name="pack",
    )(gate, up, down)


def arrange_body(landed_ref, out_ref):
    for k in range(out_ref.shape[0]):
        out_ref[k] = landed_ref[:, k]


def arrange(landed):
    experts, across, each, share = landed.shape
    vmem = pl.BlockSpec(memory_space=pltpu.VMEM)
    return pl.pallas_call(
        arrange_body,
        in_specs=[vmem],
        out_specs=vmem,
        out_shape=jax.ShapeDtypeStruct((across, experts, each, share), landed.dtype),
        compiler_params=pltpu.CompilerParams(vmem_limit_bytes=2 * 2**20),
        name="arrange",
    )(landed)


def project_body(parts_ref, residual_ref, place_ref, slots_ref, factors_ref, stream_ref, out_ref, slots_out, factors_out):
    slots_out[...] = slots_ref[...]
    factors_out[...] = factors_ref[...]
    total = residual_ref[...].astype(jnp.float32)
    for p in range(parts_ref.shape[0]):
        total += parts_ref[p].astype(jnp.float32)
    stream_ref[...] = total
    rows = total.astype(jnp.bfloat16)
    experts, tok = place_ref.shape
    capacity = out_ref.shape[0] // experts
    slot = lax.broadcasted_iota(jnp.int32, (capacity, tok), 0)
    for first in range(0, experts, 8):
        send = [
            jnp.where(place_ref[e : e + 1, :] == slot, 1.0, 0.0).astype(jnp.bfloat16)
            for e in range(first, first + 8)
        ]
        picked = jnp.dot(jnp.concatenate(send, axis=0), rows, preferred_element_type=jnp.float32)
        out_ref[first * capacity : (first + 8) * capacity] = picked.astype(jnp.bfloat16)


def project(parts, residual, place, slots, factors):
    _, tok, share = parts.shape
    experts = place.shape[0]
    rows = tok // (experts // GROUPS) * experts
    vmem = pl.BlockSpec(memory_space=pltpu.VMEM)
    return pl.pallas_call(
        project_body,
        in_specs=[vmem] * 5,
        out_specs=[vmem] * 4,
        out_shape=[
            jax.ShapeDtypeStruct((tok, share), jnp.float32),
            jax.ShapeDtypeStruct((rows, share), jnp.bfloat16),
            jax.ShapeDtypeStruct(slots.shape, slots.dtype),
            jax.ShapeDtypeStruct(factors.shape, factors.dtype),
        ],
        compiler_params=pltpu.CompilerParams(vmem_limit_bytes=6 * 2**20),
        name="project",
    )(parts, residual, place, slots, factors)


def combine_body(back_ref, stream_ref, slots_ref, factors_ref, out_ref):
    tok = stream_ref.shape[0]
    rows = back_ref.shape[0]
    slot = lax.broadcasted_iota(jnp.int32, (tok, rows), 1)
    total = stream_ref[...]
    for k in range(slots_ref.shape[1]):
        take = jnp.where(slots_ref[:, k : k + 1] == slot, 1.0, 0.0).astype(jnp.bfloat16)
        found = jnp.dot(take, back_ref[...], preferred_element_type=jnp.float32)
        total += factors_ref[:, k : k + 1] * found
    done = total.astype(jnp.bfloat16)
    for p in range(out_ref.shape[0]):
        out_ref[p] = done


def combine(back, stream, slots, factors, peers):
    tok, share = stream.shape
    vmem = pl.BlockSpec(memory_space=pltpu.VMEM)
    return pl.pallas_call(
        combine_body,
        in_specs=[vmem] * 4,
        out_specs=vmem,
        out_shape=jax.ShapeDtypeStruct((peers, tok, share), jnp.bfloat16),
        compiler_params=pltpu.CompilerParams(vmem_limit_bytes=8 * 2**20),
        name="combine",
    )(back, stream, slots, factors)


def hidden_body(x_ref, rows_ref, gain_ref, own_ref, left_ref, right_ref, far_ref, far_up_ref, out_ref, normed_ref, weights, sems):
    peers, count, share = rows_ref.shape
    pieces = out_ref.shape[0]
    gate, up = pl.ds(0, 2), pl.ds(4, 2)
    first, second = pl.ds(0, 2), pl.ds(2, 2)
    groups = [
        [(source.at[gate], weights.at[k, first]), (source.at[up], weights.at[k, second])]
        for k, source in ((0, own_ref), (1, right_ref), (3, left_ref))
    ]
    groups.append(
        [(far_ref, weights.at[2, first]), (far_up_ref, weights.at[2, second])]
    )
    copies, at = [], 0
    for group in groups:
        started = []
        for source, target in group:
            copy = pltpu.make_async_copy(source, target, sems.at[at])
            copy.start()
            started.append(copy)
            at += 1
        copies.append(started)
    total = jnp.zeros((count, 1), jnp.float32)
    for p in range(peers):
        part = rows_ref[p].astype(jnp.float32)
        total += jnp.sum(part * part, axis=1, keepdims=True)
    scale = lax.rsqrt(total / (peers * share) + norm_eps)
    for p in range(peers):
        cols = slice(p * share, (p + 1) * share)
        normed_ref[:, cols] = (rows_ref[p].astype(jnp.float32) * scale * gain_ref[:, cols]).astype(
            jnp.bfloat16
        )
    for ahead, started in zip((0, 1, 3, 2), copies):
        for copy in started:
            copy.wait()
        normed = normed_ref[...]
        gates = jnp.concatenate([weights[ahead, 0], weights[ahead, 1]], axis=1)
        ups = jnp.concatenate([weights[ahead, 2], weights[ahead, 3]], axis=1)
        gate = jnp.dot(normed, gates, preferred_element_type=jnp.float32)
        up = jnp.dot(normed, ups, preferred_element_type=jnp.float32)
        act = gate / (1.0 + jnp.exp(-gate)) * up
        out_ref[lax.rem(x_ref[0] + ahead, pieces)] = act.astype(jnp.bfloat16)


def hidden_units(x, rows, gain, *weights):
    peers, count, share = rows.shape
    _, model, half = weights[0].shape
    vmem = pl.BlockSpec(memory_space=pltpu.VMEM)
    anywhere = pl.BlockSpec(memory_space=pltpu.HBM)
    return pl.pallas_call(
        hidden_body,
        in_specs=[pl.BlockSpec(memory_space=pltpu.SMEM), vmem, vmem] + [anywhere] * len(weights),
        out_specs=vmem,
        out_shape=jax.ShapeDtypeStruct((4, count, 2 * half), jnp.bfloat16),
        scratch_shapes=[
            pltpu.VMEM((count, peers * share), jnp.bfloat16),
            pltpu.VMEM((4, 4, model, half), jnp.bfloat16),
            pltpu.SemaphoreType.DMA((8,)),
        ],
        compiler_params=pltpu.CompilerParams(vmem_limit_bytes=18 * 2**20),
        name="hidden",
    )(x, rows, gain, *weights)


def down_body(x_ref, units_ref, own_ref, right_ref, far_ref, left_ref, out_ref, downs, sems):
    blocks, count, hidden = units_ref.shape
    chips, pieces, rows_each, _ = out_ref.shape
    parts = sems.shape[0]
    half, share = own_ref.shape[1:]
    step = 2 * half // parts
    copies = []
    for c in range(parts):
        at = c * step
        rows = pl.ds(at, step)
        inner = pl.ds(at % half, step)
        page = at // half
        sources = (
            own_ref.at[2 + page, inner],
            right_ref.at[2 + page, inner],
            far_ref.at[page, inner],
            left_ref.at[2 + page, inner],
        )
        for k, source in enumerate(sources):
            copy = pltpu.make_async_copy(source, downs.at[k, rows], sems.at[c, k])
            copy.start()
            copies.append(copy)
    first = jnp.zeros((count, 2 * share), jnp.float32)
    second = jnp.zeros((count, 2 * share), jnp.float32)
    for p in range(blocks):
        if p % (blocks // parts) == 0:
            c = p // (blocks // parts)
            for copy in copies[c * pieces : (c + 1) * pieces]:
                copy.wait()
        rows = slice(p * hidden, (p + 1) * hidden)
        units = units_ref[p]
        near = jnp.concatenate([downs[0, rows], downs[1, rows]], axis=1)
        rest = jnp.concatenate([downs[2, rows], downs[3, rows]], axis=1)
        first += jnp.dot(units, near, preferred_element_type=jnp.float32)
        second += jnp.dot(units, rest, preferred_element_type=jnp.float32)
    made = (first[:, :share], first[:, share:], second[:, :share], second[:, share:])
    for ahead, value in enumerate(made):
        at = lax.rem(x_ref[0] + ahead, pieces)
        out_ref[:, at] = value.reshape(chips, rows_each, share).astype(jnp.bfloat16)


def down_product(x, units, chips, *downs):
    _, count, _ = units.shape
    _, half, share = downs[0].shape
    vmem = pl.BlockSpec(memory_space=pltpu.VMEM)
    anywhere = pl.BlockSpec(memory_space=pltpu.HBM)
    return pl.pallas_call(
        down_body,
        in_specs=[pl.BlockSpec(memory_space=pltpu.SMEM), vmem] + [anywhere] * len(downs),
        out_specs=vmem,
        out_shape=jax.ShapeDtypeStruct((chips, 4, count // chips, share), jnp.bfloat16),
        scratch_shapes=[
            pltpu.VMEM((4, 2 * half, share), jnp.bfloat16),
            pltpu.SemaphoreType.DMA((4, 4)),
        ],
        compiler_params=pltpu.CompilerParams(vmem_limit_bytes=10 * 2**20),
        name="down",
    )(x, units, *downs)


def assemble_body(whole_ref, out_ref):
    peers, _, share = whole_ref.shape
    for p in range(peers):
        out_ref[:, p * share : (p + 1) * share] = whole_ref[p]


def assemble(whole):
    peers, tok, share = whole.shape
    tile = tok // 4
    return pl.pallas_call(
        assemble_body,
        grid=(4,),
        in_specs=[pl.BlockSpec((peers, tile, share), lambda i: (0, i, 0))],
        out_specs=pl.BlockSpec((tile, peers * share), lambda i: (i, 0)),
        out_shape=jax.ShapeDtypeStruct((tok, peers * share), whole.dtype),
        compiler_params=pltpu.CompilerParams(
            dimension_semantics=("arbitrary",), vmem_limit_bytes=6 * 2**20
        ),
        name="assemble",
    )(whole)


def gathered(array, axes, axis, scale):
    sent = (array.astype(jnp.float32) * scale).astype(jnp.float16)
    whole = lax.all_gather(sent, axes, axis=axis, tiled=True)
    return (whole.astype(jnp.float32) * (1.0 / scale)).astype(jnp.bfloat16)


def shards(
    residual,
    queries,
    key_vectors,
    value_rows,
    head_lambda,
    head_gain,
    out_weight,
    ffn_gain,
    expert_gate,
    expert_up,
    expert_down,
    routing,
    route_weight,
):
    tok, _, _ = queries.shape
    experts = lax.axis_size("sp")
    across = lax.axis_size("x")
    along = lax.axis_size("y")
    tp = ("y", "x")
    peers = across * along
    model = residual.shape[1]
    share = model // peers
    where = lax.axis_index("sp").astype(jnp.int32)[None]
    x_at = lax.axis_index("x").astype(jnp.int32)[None]
    column = (lax.axis_index("y") * across + lax.axis_index("x")) * share

    ahead = [(i, (i + 1) % across) for i in range(across)]
    behind = [(i, (i - 1) % across) for i in range(across)]
    gate, up, down = expert_gate[0], expert_up[0], expert_down[0]
    packed = pack(gate, up, down)
    left = lax.ppermute(packed, "x", ahead)
    right = lax.ppermute(packed, "x", behind)
    gate_2 = lax.ppermute(left[:2], "x", ahead)
    up_2 = lax.ppermute(right[4:], "x", behind)
    down_2 = lax.ppermute(left[2:4], "x", ahead)

    kv = jnp.concatenate([key_vectors[:, 0], value_rows[:, 0]], axis=1)
    kv_all = gathered(kv, "sp", 0, SHIFT)
    own_residual = lax.dynamic_slice_in_dim(residual, column, share, 1)

    capacity = tok // (experts // GROUPS)
    order = jnp.arange(tok, dtype=jnp.int32)
    ids = jnp.arange(experts, dtype=jnp.int32)
    named = routing[:, :, None] == ids
    member = jnp.any(named, axis=1)
    strict = (order[None, :] < order[:, None]).astype(jnp.bfloat16)
    earlier = jnp.dot(
        strict, member.astype(jnp.bfloat16), preferred_element_type=jnp.float32
    ).astype(jnp.int32)
    place = jnp.where(member, earlier, -1).T
    picked = jnp.sum(jnp.where(named, earlier[:, None, :], 0), axis=2)
    slots = routing * capacity + picked

    partial = attention(
        where, head_lambda, queries[:, 0], kv_all, head_gain[None], out_weight, peers
    )
    parts = lax.all_to_all(partial, tp, 0, 0, tiled=True)
    own_stream, outgoing, slots, factors = project(
        parts, own_residual, place, slots, route_weight
    )
    targets = experts * across
    each = capacity // across
    landed = lax.all_to_all(outgoing.reshape(targets, each, share), ("sp", "x"), 0, 0, tiled=True)
    landed = arrange(landed.reshape(experts, across, each, share))
    rows = gathered(landed.reshape(across, experts * each, share), "y", 0, 64.0)
    units = hidden_units(
        x_at, rows, ffn_gain[None], packed, left, right, gate_2, up_2
    )
    all_units = gathered(units, "y", 0, 0.25)
    made = down_product(x_at, all_units, experts, packed, right, down_2, left)
    back = lax.all_to_all(
        made.reshape(targets, each, share), ("sp", "x"), 0, 0, tiled=True
    )
    back = back.reshape(experts * capacity, share)
    spread = combine(back, own_stream, slots, factors, peers)
    whole = lax.all_to_all(spread, tp, 0, 0, tiled=True)
    return assemble(whole)


def solution(mesh):
    sizes = mesh.devices.shape
    split = jax.sharding.Mesh(
        mesh.devices.reshape(sizes[0], sizes[1] // 4, 4), ("sp", "y", "x")
    )
    tp = ("y", "x")
    in_specs = (
        P("sp", None),
        P("sp", tp, None),
        P("sp", tp, None),
        P("sp", tp, None),
        P(tp),
        P(),
        P(tp, None),
        P(),
        P("sp", None, tp),
        P("sp", None, tp),
        P("sp", None, tp),
        P("sp", None),
        P("sp", None),
    )
    return jax.shard_map(
        shards, mesh=split, in_specs=in_specs, out_specs=P("sp", None), check_vma=False
    )
```

```python
import jax
import jax.numpy as jnp
from jax import lax
from jax.experimental import pallas as pl
from jax.experimental.pallas import tpu as pltpu
from jax.sharding import PartitionSpec as P

norm_eps = 1e-06
KEY_BLOCK = 2048
ROW_BLOCK = 128
SHIFT = 4096.0
GROUPS = 4


def attention_body(where_ref, lam_ref, q_ref, kv_ref, gain_ref, weight_ref, out_ref, stacked, highest, accum, parts, sems):
    tok, width = q_ref.shape
    first_query = where_ref[0] * tok
    last = (first_query + tok - 1) // KEY_BLOCK
    scaled = q_ref[...] * jnp.asarray((width // 2) ** -0.5, jnp.bfloat16)
    low = lax.broadcasted_iota(jnp.int32, scaled.shape, 1) < width // 2
    zero = jnp.zeros_like(scaled)
    stacked[:tok] = jnp.where(low, scaled, zero)
    stacked[tok:] = jnp.where(low, zero, scaled)
    highest[...] = jnp.full(highest.shape, -1e30, jnp.float32)
    accum[...] = jnp.zeros(accum.shape, jnp.float32)

    def update(step, masked):
        block = kv_ref[pl.ds(pl.multiple_of(step * KEY_BLOCK, KEY_BLOCK), KEY_BLOCK), :]
        keys, values = block[:, :width], block[:, width:]
        wide = jnp.concatenate([values, jnp.ones_like(values)], axis=1)
        for at in range(0, 2 * tok, ROW_BLOCK):
            rows = slice(at, at + ROW_BLOCK)
            scores = lax.dot_general(
                stacked[rows], keys, (((1,), (1,)), ((), ())), preferred_element_type=jnp.float32
            )
            if masked:
                row = lax.broadcasted_iota(jnp.int32, scores.shape, 0) + at % tok
                col = lax.broadcasted_iota(jnp.int32, scores.shape, 1)
                scores = jnp.where(
                    col - row <= first_query - step * KEY_BLOCK, scores, -1e30
                )
            before = highest[rows]
            now = jnp.maximum(before, jnp.max(scores, axis=1, keepdims=True))
            weights = jnp.exp(scores - now[:, :1])
            shrink = jnp.exp(before - now)[:, :1]
            blended = jnp.dot(weights.astype(jnp.bfloat16), wide, preferred_element_type=jnp.float32)
            accum[rows] = accum[rows] * shrink + blended
            highest[rows] = now

    def whole(step, carry):
        update(step, False)
        return carry

    lax.fori_loop(0, last, whole, 0)
    update(last, True)
    both = accum[:, :width] / accum[:, width:]
    combined = both[:tok] - lam_ref[0] * both[tok:]
    square = jnp.mean(combined * combined, axis=1, keepdims=True)
    attended = (combined * lax.rsqrt(square + norm_eps) * gain_ref[...]).astype(jnp.bfloat16)
    share = out_ref.shape[2]
    copies = []
    for p in range(0, out_ref.shape[0], 2):
        cols = weight_ref[:, p * share : (p + 2) * share]
        part = jnp.dot(attended, cols, preferred_element_type=jnp.float32).astype(jnp.bfloat16)
        parts[p] = part[:, :share]
        parts[p + 1] = part[:, share:]
        copy = pltpu.make_async_copy(
            parts.at[pl.ds(p, 2)], out_ref.at[pl.ds(p, 2)], sems.at[p // 2]
        )
        copy.start()
        copies.append(copy)
    for copy in copies:
        copy.wait()


def attention(where, lam, q, kv, gain, weight, peers):
    tok, width = q.shape
    share = weight.shape[1] // peers
    vmem = pl.BlockSpec(memory_space=pltpu.VMEM)
    smem = pl.BlockSpec(memory_space=pltpu.SMEM)
    return pl.pallas_call(
        attention_body,
        in_specs=[smem, smem, vmem, vmem, vmem, vmem],
        out_specs=pl.BlockSpec(memory_space=pltpu.HBM),
        out_shape=jax.ShapeDtypeStruct((peers, tok, share), jnp.bfloat16),
        scratch_shapes=[
            pltpu.VMEM((2 * tok, width), jnp.bfloat16),
            pltpu.VMEM((2 * tok, 128), jnp.float32),
            pltpu.VMEM((2 * tok, 2 * width), jnp.float32),
            pltpu.VMEM((peers, tok, share), jnp.bfloat16),
            pltpu.SemaphoreType.DMA((peers // 2,)),
        ],
        compiler_params=pltpu.CompilerParams(vmem_limit_bytes=14 * 2**20),
        name="attention",
    )(where, lam, q, kv, gain, weight)


def pack_body(gate_ref, up_ref, down_ref, out_ref, sems):
    rows, width = out_ref.shape[1:]
    low, high = pl.ds(0, width), pl.ds(width, width)
    sources = (
        gate_ref.at[:, low],
        gate_ref.at[:, high],
        down_ref.at[pl.ds(0, rows)],
        down_ref.at[pl.ds(rows, rows)],
        up_ref.at[:, low],
        up_ref.at[:, high],
    )
    copies = [
        pltpu.make_async_copy(source, out_ref.at[k], sems.at[k])
        for k, source in enumerate(sources)
    ]
    for copy in copies:
        copy.start()
    for copy in copies:
        copy.wait()


def pack(gate, up, down):
    model, hidden = gate.shape
    return pl.pallas_call(
        pack_body,
        in_specs=[pl.BlockSpec(memory_space=pltpu.HBM)] * 3,
        out_specs=pl.BlockSpec(memory_space=pltpu.HBM),
        out_shape=jax.ShapeDtypeStruct((6, model, hidden // 2), gate.dtype),
        scratch_shapes=[pltpu.SemaphoreType.DMA((6,))],
        compiler_params=pltpu.CompilerParams(vmem_limit_bytes=4 * 2**20),
        name="pack",
    )(gate, up, down)


def arrange_body(landed_ref, out_ref):
    for k in range(out_ref.shape[0]):
        out_ref[k] = landed_ref[:, k]


def arrange(landed):
    experts, across, each, share = landed.shape
    vmem = pl.BlockSpec(memory_space=pltpu.VMEM)
    return pl.pallas_call(
        arrange_body,
        in_specs=[vmem],
        out_specs=vmem,
        out_shape=jax.ShapeDtypeStruct((across, experts, each, share), landed.dtype),
        compiler_params=pltpu.CompilerParams(vmem_limit_bytes=2 * 2**20),
        name="arrange",
    )(landed)


def project_body(parts_ref, residual_ref, place_ref, slots_ref, factors_ref, stream_ref, out_ref, slots_out, factors_out):
    slots_out[...] = slots_ref[...]
    factors_out[...] = factors_ref[...]
    total = residual_ref[...].astype(jnp.float32)
    for p in range(parts_ref.shape[0]):
        total += parts_ref[p].astype(jnp.float32)
    stream_ref[...] = total
    rows = total.astype(jnp.bfloat16)
    experts, tok = place_ref.shape
    capacity = out_ref.shape[0] // experts
    slot = lax.broadcasted_iota(jnp.int32, (capacity, tok), 0)
    for first in range(0, experts, 8):
        send = [
            jnp.where(place_ref[e : e + 1, :] == slot, 1.0, 0.0).astype(jnp.bfloat16)
            for e in range(first, first + 8)
        ]
        picked = jnp.dot(jnp.concatenate(send, axis=0), rows, preferred_element_type=jnp.float32)
        out_ref[first * capacity : (first + 8) * capacity] = picked.astype(jnp.bfloat16)


def project(parts, residual, place, slots, factors):
    _, tok, share = parts.shape
    experts = place.shape[0]
    rows = tok // (experts // GROUPS) * experts
    vmem = pl.BlockSpec(memory_space=pltpu.VMEM)
    return pl.pallas_call(
        project_body,
        in_specs=[vmem] * 5,
        out_specs=[vmem] * 4,
        out_shape=[
            jax.ShapeDtypeStruct((tok, share), jnp.float32),
            jax.ShapeDtypeStruct((rows, share), jnp.bfloat16),
            jax.ShapeDtypeStruct(slots.shape, slots.dtype),
            jax.ShapeDtypeStruct(factors.shape, factors.dtype),
        ],
        compiler_params=pltpu.CompilerParams(vmem_limit_bytes=6 * 2**20),
        name="project",
    )(parts, residual, place, slots, factors)


def combine_body(back_ref, stream_ref, slots_ref, factors_ref, out_ref):
    tok = stream_ref.shape[0]
    rows = back_ref.shape[0]
    slot = lax.broadcasted_iota(jnp.int32, (tok, rows), 1)
    total = stream_ref[...]
    for k in range(slots_ref.shape[1]):
        take = jnp.where(slots_ref[:, k : k + 1] == slot, 1.0, 0.0).astype(jnp.bfloat16)
        found = jnp.dot(take, back_ref[...], preferred_element_type=jnp.float32)
        total += factors_ref[:, k : k + 1] * found
    done = total.astype(jnp.bfloat16)
    for p in range(out_ref.shape[0]):
        out_ref[p] = done


def combine(back, stream, slots, factors, peers):
    tok, share = stream.shape
    vmem = pl.BlockSpec(memory_space=pltpu.VMEM)
    return pl.pallas_call(
        combine_body,
        in_specs=[vmem] * 4,
        out_specs=vmem,
        out_shape=jax.ShapeDtypeStruct((peers, tok, share), jnp.bfloat16),
        compiler_params=pltpu.CompilerParams(vmem_limit_bytes=8 * 2**20),
        name="combine",
    )(back, stream, slots, factors)


def swiglu(normed, pages):
    gates = jnp.concatenate([pages[0], pages[1]], axis=1)
    ups = jnp.concatenate([pages[2], pages[3]], axis=1)
    gate = jnp.dot(normed, gates, preferred_element_type=jnp.float32)
    up = jnp.dot(normed, ups, preferred_element_type=jnp.float32)
    return (gate / (1.0 + jnp.exp(-gate)) * up).astype(jnp.bfloat16)


def near_body(rows_ref, gain_ref, own_ref, right_ref, left_ref, out_ref, normed_ref, weights, sems):
    peers, count, share = rows_ref.shape
    gate, up = pl.ds(0, 2), pl.ds(4, 2)
    first, second = pl.ds(0, 2), pl.ds(2, 2)
    copies = []
    for k, source in enumerate((own_ref, right_ref, left_ref)):
        pair = (
            pltpu.make_async_copy(source.at[gate], weights.at[k, first], sems.at[k, 0]),
            pltpu.make_async_copy(source.at[up], weights.at[k, second], sems.at[k, 1]),
        )
        for copy in pair:
            copy.start()
        copies.append(pair)
    total = jnp.zeros((count, 1), jnp.float32)
    for p in range(peers):
        part = rows_ref[p].astype(jnp.float32)
        total += jnp.sum(part * part, axis=1, keepdims=True)
    scale = lax.rsqrt(total / (peers * share) + norm_eps)
    for p in range(peers):
        cols = slice(p * share, (p + 1) * share)
        normed_ref[:, cols] = (rows_ref[p].astype(jnp.float32) * scale * gain_ref[:, cols]).astype(
            jnp.bfloat16
        )
    for k, pair in enumerate(copies):
        for copy in pair:
            copy.wait()
        out_ref[k] = swiglu(normed_ref[...], [weights[k, page] for page in range(4)])


def near_units(rows, gain, *sources):
    peers, count, share = rows.shape
    _, model, half = sources[0].shape
    vmem = pl.BlockSpec(memory_space=pltpu.VMEM)
    anywhere = pl.BlockSpec(memory_space=pltpu.HBM)
    return pl.pallas_call(
        near_body,
        in_specs=[vmem, vmem] + [anywhere] * len(sources),
        out_specs=[vmem, vmem],
        out_shape=[
            jax.ShapeDtypeStruct((len(sources), count, 2 * half), jnp.bfloat16),
            jax.ShapeDtypeStruct((count, peers * share), jnp.bfloat16),
        ],
        scratch_shapes=[
            pltpu.VMEM((len(sources), 4, model, half), jnp.bfloat16),
            pltpu.SemaphoreType.DMA((len(sources), 2)),
        ],
        compiler_params=pltpu.CompilerParams(vmem_limit_bytes=16 * 2**20),
        name="near",
    )(rows, gain, *sources)


def far_body(normed_ref, gate_ref, up_ref, out_ref, weights, sems):
    copies = (
        pltpu.make_async_copy(gate_ref, weights.at[pl.ds(0, 2)], sems.at[0]),
        pltpu.make_async_copy(up_ref, weights.at[pl.ds(2, 2)], sems.at[1]),
    )
    for copy in copies:
        copy.start()
    for copy in copies:
        copy.wait()
    out_ref[0] = swiglu(normed_ref[...], [weights[page] for page in range(4)])


def far_units(normed, gate, up):
    count = normed.shape[0]
    _, model, half = gate.shape
    vmem = pl.BlockSpec(memory_space=pltpu.VMEM)
    anywhere = pl.BlockSpec(memory_space=pltpu.HBM)
    return pl.pallas_call(
        far_body,
        in_specs=[vmem, anywhere, anywhere],
        out_specs=vmem,
        out_shape=jax.ShapeDtypeStruct((1, count, 2 * half), jnp.bfloat16),
        scratch_shapes=[
            pltpu.VMEM((4, model, half), jnp.bfloat16),
            pltpu.SemaphoreType.DMA((2,)),
        ],
        compiler_params=pltpu.CompilerParams(vmem_limit_bytes=8 * 2**20),
        name="far",
    )(normed, gate, up)


def down_body(x_ref, units_ref, own_ref, right_ref, far_ref, left_ref, out_ref, downs, sems):
    blocks, count, hidden = units_ref.shape
    chips, pieces, rows_each, _ = out_ref.shape
    parts = sems.shape[0]
    half, share = own_ref.shape[1:]
    step = 2 * half // parts
    copies = []
    for c in range(parts):
        at = c * step
        rows = pl.ds(at, step)
        inner = pl.ds(at % half, step)
        page = at // half
        sources = (
            own_ref.at[2 + page, inner],
            right_ref.at[2 + page, inner],
            far_ref.at[page, inner],
            left_ref.at[2 + page, inner],
        )
        for k, source in enumerate(sources):
            copy = pltpu.make_async_copy(source, downs.at[k, rows], sems.at[c, k])
            copy.start()
            copies.append(copy)
    first = jnp.zeros((count, 2 * share), jnp.float32)
    second = jnp.zeros((count, 2 * share), jnp.float32)
    for p in range(blocks):
        if p % (blocks // parts) == 0:
            c = p // (blocks // parts)
            for copy in copies[c * pieces : (c + 1) * pieces]:
                copy.wait()
        ahead = (0, 1, 3, 2)[p % pieces]
        block = p // pieces * pieces + lax.rem(x_ref[0] + ahead, pieces)
        rows = pl.ds(pl.multiple_of(block * hidden, hidden), hidden)
        units = units_ref[p]
        near = jnp.concatenate([downs[0, rows], downs[1, rows]], axis=1)
        rest = jnp.concatenate([downs[2, rows], downs[3, rows]], axis=1)
        first += jnp.dot(units, near, preferred_element_type=jnp.float32)
        second += jnp.dot(units, rest, preferred_element_type=jnp.float32)
    made = (first[:, :share], first[:, share:], second[:, :share], second[:, share:])
    for ahead, value in enumerate(made):
        at = lax.rem(x_ref[0] + ahead, pieces)
        out_ref[:, at] = value.reshape(chips, rows_each, share).astype(jnp.bfloat16)


def down_product(x, units, chips, *downs):
    _, count, _ = units.shape
    _, half, share = downs[0].shape
    vmem = pl.BlockSpec(memory_space=pltpu.VMEM)
    anywhere = pl.BlockSpec(memory_space=pltpu.HBM)
    return pl.pallas_call(
        down_body,
        in_specs=[pl.BlockSpec(memory_space=pltpu.SMEM), vmem] + [anywhere] * len(downs),
        out_specs=vmem,
        out_shape=jax.ShapeDtypeStruct((chips, 4, count // chips, share), jnp.bfloat16),
        scratch_shapes=[
            pltpu.VMEM((4, 2 * half, share), jnp.bfloat16),
            pltpu.SemaphoreType.DMA((4, 4)),
        ],
        compiler_params=pltpu.CompilerParams(vmem_limit_bytes=10 * 2**20),
        name="down",
    )(x, units, *downs)


def assemble_body(whole_ref, out_ref):
    peers, _, share = whole_ref.shape
    for p in range(peers):
        out_ref[:, p * share : (p + 1) * share] = whole_ref[p]


def assemble(whole):
    peers, tok, share = whole.shape
    tile = tok // 4
    return pl.pallas_call(
        assemble_body,
        grid=(4,),
        in_specs=[pl.BlockSpec((peers, tile, share), lambda i: (0, i, 0))],
        out_specs=pl.BlockSpec((tile, peers * share), lambda i: (i, 0)),
        out_shape=jax.ShapeDtypeStruct((tok, peers * share), whole.dtype),
        compiler_params=pltpu.CompilerParams(
            dimension_semantics=("arbitrary",), vmem_limit_bytes=6 * 2**20
        ),
        name="assemble",
    )(whole)


def gathered(array, axes, axis, scale):
    sent = (array.astype(jnp.float32) * scale).astype(jnp.float16)
    whole = lax.all_gather(sent, axes, axis=axis, tiled=True)
    return (whole.astype(jnp.float32) * (1.0 / scale)).astype(jnp.bfloat16)


def shards(
    residual,
    queries,
    key_vectors,
    value_rows,
    head_lambda,
    head_gain,
    out_weight,
    ffn_gain,
    expert_gate,
    expert_up,
    expert_down,
    routing,
    route_weight,
):
    tok, _, _ = queries.shape
    experts = lax.axis_size("sp")
    across = lax.axis_size("x")
    along = lax.axis_size("y")
    tp = ("y", "x")
    peers = across * along
    model = residual.shape[1]
    share = model // peers
    where = lax.axis_index("sp").astype(jnp.int32)[None]
    x_at = lax.axis_index("x").astype(jnp.int32)[None]
    column = (lax.axis_index("y") * across + lax.axis_index("x")) * share

    ahead = [(i, (i + 1) % across) for i in range(across)]
    behind = [(i, (i - 1) % across) for i in range(across)]
    gate, up, down = expert_gate[0], expert_up[0], expert_down[0]
    packed = pack(gate, up, down)
    left = lax.ppermute(packed, "x", ahead)
    right = lax.ppermute(packed, "x", behind)
    gate_2 = lax.ppermute(left[:2], "x", ahead)
    up_2 = lax.ppermute(right[4:], "x", behind)
    down_2 = lax.ppermute(left[2:4], "x", ahead)

    kv = jnp.concatenate([key_vectors[:, 0], value_rows[:, 0]], axis=1)
    kv_all = gathered(kv, "sp", 0, SHIFT)
    own_residual = lax.dynamic_slice_in_dim(residual, column, share, 1)

    capacity = tok // (experts // GROUPS)
    order = jnp.arange(tok, dtype=jnp.int32)
    ids = jnp.arange(experts, dtype=jnp.int32)
    named = routing[:, :, None] == ids
    member = jnp.any(named, axis=1)
    strict = (order[None, :] < order[:, None]).astype(jnp.bfloat16)
    earlier = jnp.dot(
        strict, member.astype(jnp.bfloat16), preferred_element_type=jnp.float32
    ).astype(jnp.int32)
    place = jnp.where(member, earlier, -1).T
    picked = jnp.sum(jnp.where(named, earlier[:, None, :], 0), axis=2)
    slots = routing * capacity + picked

    partial = attention(
        where, head_lambda, queries[:, 0], kv_all, head_gain[None], out_weight, peers
    )
    parts = lax.all_to_all(partial, tp, 0, 0, tiled=True)
    own_stream, outgoing, slots, factors = project(
        parts, own_residual, place, slots, route_weight
    )
    targets = experts * across
    each = capacity // across
    landed = lax.all_to_all(outgoing.reshape(targets, each, share), ("sp", "x"), 0, 0, tiled=True)
    landed = arrange(landed.reshape(experts, across, each, share))
    rows = gathered(landed.reshape(across, experts * each, share), "y", 0, 64.0)
    near, normed = near_units(rows, ffn_gain[None], packed, right, left)
    far = far_units(normed, gate_2, up_2)
    units = jnp.concatenate([near, far], axis=0)
    all_units = gathered(units, "y", 0, 0.25)
    made = down_product(x_at, all_units, experts, packed, right, down_2, left)
    back = lax.all_to_all(
        made.reshape(targets, each, share), ("sp", "x"), 0, 0, tiled=True
    )
    back = back.reshape(experts * capacity, share)
    spread = combine(back, own_stream, slots, factors, peers)
    whole = lax.all_to_all(spread, tp, 0, 0, tiled=True)
    return assemble(whole)


def solution(mesh):
    sizes = mesh.devices.shape
    split = jax.sharding.Mesh(
        mesh.devices.reshape(sizes[0], sizes[1] // 4, 4), ("sp", "y", "x")
    )
    tp = ("y", "x")
    in_specs = (
        P("sp", None),
        P("sp", tp, None),
        P("sp", tp, None),
        P("sp", tp, None),
        P(tp),
        P(),
        P(tp, None),
        P(),
        P("sp", None, tp),
        P("sp", None, tp),
        P("sp", None, tp),
        P("sp", None),
        P("sp", None),
    )
    return jax.shard_map(
        shards, mesh=split, in_specs=in_specs, out_specs=P("sp", None), check_vma=False
    )
```

```python
import jax
import jax.numpy as jnp
from jax import lax
from jax.experimental import pallas as pl
from jax.experimental.pallas import tpu as pltpu
from jax.sharding import PartitionSpec as P

norm_eps = 1e-06
KEY_BLOCK = 2048
ROW_BLOCK = 128
SHIFT = 4096.0
GROUPS = 4


def attention_body(where_ref, lam_ref, q_ref, kv_ref, gain_ref, weight_ref, out_ref, stacked, highest, accum, parts, sems):
    tok, width = q_ref.shape
    first_query = where_ref[0] * tok
    last = (first_query + tok - 1) // KEY_BLOCK
    scaled = q_ref[...] * jnp.asarray((width // 2) ** -0.5, jnp.bfloat16)
    low = lax.broadcasted_iota(jnp.int32, scaled.shape, 1) < width // 2
    zero = jnp.zeros_like(scaled)
    stacked[:tok] = jnp.where(low, scaled, zero)
    stacked[tok:] = jnp.where(low, zero, scaled)
    highest[...] = jnp.full(highest.shape, -1e30, jnp.float32)
    accum[...] = jnp.zeros(accum.shape, jnp.float32)

    def update(step, masked):
        block = kv_ref[pl.ds(pl.multiple_of(step * KEY_BLOCK, KEY_BLOCK), KEY_BLOCK), :]
        keys, values = block[:, :width], block[:, width:]
        wide = jnp.concatenate([values, jnp.ones_like(values)], axis=1)
        for at in range(0, 2 * tok, ROW_BLOCK):
            rows = slice(at, at + ROW_BLOCK)
            scores = lax.dot_general(
                stacked[rows], keys, (((1,), (1,)), ((), ())), preferred_element_type=jnp.float32
            )
            if masked:
                row = lax.broadcasted_iota(jnp.int32, scores.shape, 0) + at % tok
                col = lax.broadcasted_iota(jnp.int32, scores.shape, 1)
                scores = jnp.where(
                    col - row <= first_query - step * KEY_BLOCK, scores, -1e30
                )
            before = highest[rows]
            now = jnp.maximum(before, jnp.max(scores, axis=1, keepdims=True))
            weights = jnp.exp(scores - now[:, :1])
            shrink = jnp.exp(before - now)[:, :1]
            blended = jnp.dot(weights.astype(jnp.bfloat16), wide, preferred_element_type=jnp.float32)
            accum[rows] = accum[rows] * shrink + blended
            highest[rows] = now

    def whole(step, carry):
        update(step, False)
        return carry

    lax.fori_loop(0, last, whole, 0)
    update(last, True)
    both = accum[:, :width] / accum[:, width:]
    combined = both[:tok] - lam_ref[0] * both[tok:]
    square = jnp.mean(combined * combined, axis=1, keepdims=True)
    attended = (combined * lax.rsqrt(square + norm_eps) * gain_ref[...]).astype(jnp.bfloat16)
    share = out_ref.shape[2]
    copies = []
    for p in range(0, out_ref.shape[0], 2):
        cols = weight_ref[:, p * share : (p + 2) * share]
        part = jnp.dot(attended, cols, preferred_element_type=jnp.float32).astype(jnp.bfloat16)
        parts[p] = part[:, :share]
        parts[p + 1] = part[:, share:]
        copy = pltpu.make_async_copy(
            parts.at[pl.ds(p, 2)], out_ref.at[pl.ds(p, 2)], sems.at[p // 2]
        )
        copy.start()
        copies.append(copy)
    for copy in copies:
        copy.wait()


def attention(where, lam, q, kv, gain, weight, peers):
    tok, width = q.shape
    share = weight.shape[1] // peers
    vmem = pl.BlockSpec(memory_space=pltpu.VMEM)
    smem = pl.BlockSpec(memory_space=pltpu.SMEM)
    return pl.pallas_call(
        attention_body,
        in_specs=[smem, smem, vmem, vmem, vmem, vmem],
        out_specs=pl.BlockSpec(memory_space=pltpu.HBM),
        out_shape=jax.ShapeDtypeStruct((peers, tok, share), jnp.bfloat16),
        scratch_shapes=[
            pltpu.VMEM((2 * tok, width), jnp.bfloat16),
            pltpu.VMEM((2 * tok, 128), jnp.float32),
            pltpu.VMEM((2 * tok, 2 * width), jnp.float32),
            pltpu.VMEM((peers, tok, share), jnp.bfloat16),
            pltpu.SemaphoreType.DMA((peers // 2,)),
        ],
        compiler_params=pltpu.CompilerParams(vmem_limit_bytes=14 * 2**20),
        name="attention",
    )(where, lam, q, kv, gain, weight)


def pack_body(gate_ref, up_ref, down_ref, out_ref, sems):
    rows, width = out_ref.shape[1:]
    low, high = pl.ds(0, width), pl.ds(width, width)
    sources = (
        gate_ref.at[:, low],
        gate_ref.at[:, high],
        down_ref.at[pl.ds(0, rows)],
        down_ref.at[pl.ds(rows, rows)],
        up_ref.at[:, low],
        up_ref.at[:, high],
    )
    copies = [
        pltpu.make_async_copy(source, out_ref.at[k], sems.at[k])
        for k, source in enumerate(sources)
    ]
    for copy in copies:
        copy.start()
    for copy in copies:
        copy.wait()


def pack(gate, up, down):
    model, hidden = gate.shape
    return pl.pallas_call(
        pack_body,
        in_specs=[pl.BlockSpec(memory_space=pltpu.HBM)] * 3,
        out_specs=pl.BlockSpec(memory_space=pltpu.HBM),
        out_shape=jax.ShapeDtypeStruct((6, model, hidden // 2), gate.dtype),
        scratch_shapes=[pltpu.SemaphoreType.DMA((6,))],
        compiler_params=pltpu.CompilerParams(vmem_limit_bytes=4 * 2**20),
        name="pack",
    )(gate, up, down)


def cut_body(left_ref, right_ref, gate_ref, down_ref, up_ref, sems):
    copies = (
        pltpu.make_async_copy(left_ref.at[pl.ds(0, 2)], gate_ref, sems.at[0]),
        pltpu.make_async_copy(right_ref.at[pl.ds(4, 2)], up_ref, sems.at[1]),
        pltpu.make_async_copy(left_ref.at[pl.ds(2, 2)], down_ref, sems.at[2]),
    )
    for copy in copies:
        copy.start()
    for copy in copies:
        copy.wait()


def cut(left, right):
    _, model, half = left.shape
    anywhere = pl.BlockSpec(memory_space=pltpu.HBM)
    return pl.pallas_call(
        cut_body,
        in_specs=[anywhere] * 2,
        out_specs=[pl.BlockSpec(memory_space=pltpu.VMEM)] * 3,
        out_shape=[jax.ShapeDtypeStruct((2, model, half), left.dtype)] * 3,
        scratch_shapes=[pltpu.SemaphoreType.DMA((3,))],
        compiler_params=pltpu.CompilerParams(vmem_limit_bytes=6 * 2**20),
        name="cut",
    )(left, right)


def arrange_body(landed_ref, out_ref):
    for k in range(out_ref.shape[0]):
        out_ref[k] = landed_ref[:, k]


def arrange(landed):
    experts, across, each, share = landed.shape
    vmem = pl.BlockSpec(memory_space=pltpu.VMEM)
    return pl.pallas_call(
        arrange_body,
        in_specs=[vmem],
        out_specs=vmem,
        out_shape=jax.ShapeDtypeStruct((across, experts, each, share), landed.dtype),
        compiler_params=pltpu.CompilerParams(vmem_limit_bytes=2 * 2**20),
        name="arrange",
    )(landed)


def project_body(parts_ref, residual_ref, place_ref, slots_ref, factors_ref, stream_ref, out_ref, slots_out, factors_out):
    slots_out[...] = slots_ref[...]
    factors_out[...] = factors_ref[...]
    total = residual_ref[...].astype(jnp.float32)
    for p in range(parts_ref.shape[0]):
        total += parts_ref[p].astype(jnp.float32)
    stream_ref[...] = total
    rows = total.astype(jnp.bfloat16)
    experts, tok = place_ref.shape
    capacity = out_ref.shape[0] // experts
    slot = lax.broadcasted_iota(jnp.int32, (capacity, tok), 0)
    for first in range(0, experts, 8):
        send = [
            jnp.where(place_ref[e : e + 1, :] == slot, 1.0, 0.0).astype(jnp.bfloat16)
            for e in range(first, first + 8)
        ]
        picked = jnp.dot(jnp.concatenate(send, axis=0), rows, preferred_element_type=jnp.float32)
        out_ref[first * capacity : (first + 8) * capacity] = picked.astype(jnp.bfloat16)


def project(parts, residual, place, slots, factors):
    _, tok, share = parts.shape
    experts = place.shape[0]
    rows = tok // (experts // GROUPS) * experts
    vmem = pl.BlockSpec(memory_space=pltpu.VMEM)
    return pl.pallas_call(
        project_body,
        in_specs=[vmem] * 5,
        out_specs=[vmem] * 4,
        out_shape=[
            jax.ShapeDtypeStruct((tok, share), jnp.float32),
            jax.ShapeDtypeStruct((rows, share), jnp.bfloat16),
            jax.ShapeDtypeStruct(slots.shape, slots.dtype),
            jax.ShapeDtypeStruct(factors.shape, factors.dtype),
        ],
        compiler_params=pltpu.CompilerParams(vmem_limit_bytes=6 * 2**20),
        name="project",
    )(parts, residual, place, slots, factors)


def combine_body(back_ref, stream_ref, slots_ref, factors_ref, out_ref):
    tok = stream_ref.shape[0]
    rows = back_ref.shape[0]
    slot = lax.broadcasted_iota(jnp.int32, (tok, rows), 1)
    total = stream_ref[...]
    for k in range(slots_ref.shape[1]):
        take = jnp.where(slots_ref[:, k : k + 1] == slot, 1.0, 0.0).astype(jnp.bfloat16)
        found = jnp.dot(take, back_ref[...], preferred_element_type=jnp.float32)
        total += factors_ref[:, k : k + 1] * found
    done = total.astype(jnp.bfloat16)
    for p in range(out_ref.shape[0]):
        out_ref[p] = done


def combine(back, stream, slots, factors, peers):
    tok, share = stream.shape
    vmem = pl.BlockSpec(memory_space=pltpu.VMEM)
    return pl.pallas_call(
        combine_body,
        in_specs=[vmem] * 4,
        out_specs=vmem,
        out_shape=jax.ShapeDtypeStruct((peers, tok, share), jnp.bfloat16),
        compiler_params=pltpu.CompilerParams(vmem_limit_bytes=8 * 2**20),
        name="combine",
    )(back, stream, slots, factors)


def swiglu(normed, pages):
    gates = jnp.concatenate([pages[0], pages[1]], axis=1)
    ups = jnp.concatenate([pages[2], pages[3]], axis=1)
    gate = jnp.dot(normed, gates, preferred_element_type=jnp.float32)
    up = jnp.dot(normed, ups, preferred_element_type=jnp.float32)
    return (gate / (1.0 + jnp.exp(-gate)) * up).astype(jnp.bfloat16)


def near_body(rows_ref, gain_ref, own_ref, right_ref, left_ref, out_ref, normed_ref, weights, sems):
    peers, count, share = rows_ref.shape
    gate, up = pl.ds(0, 2), pl.ds(4, 2)
    first, second = pl.ds(0, 2), pl.ds(2, 2)
    copies = []
    for k, source in enumerate((own_ref, right_ref, left_ref)):
        pair = (
            pltpu.make_async_copy(source.at[gate], weights.at[k, first], sems.at[k, 0]),
            pltpu.make_async_copy(source.at[up], weights.at[k, second], sems.at[k, 1]),
        )
        for copy in pair:
            copy.start()
        copies.append(pair)
    total = jnp.zeros((count, 1), jnp.float32)
    for p in range(peers):
        part = rows_ref[p].astype(jnp.float32)
        total += jnp.sum(part * part, axis=1, keepdims=True)
    scale = lax.rsqrt(total / (peers * share) + norm_eps)
    for p in range(peers):
        cols = slice(p * share, (p + 1) * share)
        normed_ref[:, cols] = (rows_ref[p].astype(jnp.float32) * scale * gain_ref[:, cols]).astype(
            jnp.bfloat16
        )
    for k, pair in enumerate(copies):
        for copy in pair:
            copy.wait()
        out_ref[k] = swiglu(normed_ref[...], [weights[k, page] for page in range(4)])


def near_units(rows, gain, *sources):
    peers, count, share = rows.shape
    _, model, half = sources[0].shape
    vmem = pl.BlockSpec(memory_space=pltpu.VMEM)
    anywhere = pl.BlockSpec(memory_space=pltpu.HBM)
    return pl.pallas_call(
        near_body,
        in_specs=[vmem, vmem] + [anywhere] * len(sources),
        out_specs=[vmem, vmem],
        out_shape=[
            jax.ShapeDtypeStruct((len(sources), count, 2 * half), jnp.bfloat16),
            jax.ShapeDtypeStruct((count, peers * share), jnp.bfloat16),
        ],
        scratch_shapes=[
            pltpu.VMEM((len(sources), 4, model, half), jnp.bfloat16),
            pltpu.SemaphoreType.DMA((len(sources), 2)),
        ],
        compiler_params=pltpu.CompilerParams(vmem_limit_bytes=16 * 2**20),
        name="near",
    )(rows, gain, *sources)


def far_body(normed_ref, gate_ref, up_ref, out_ref, weights, sems):
    copies = (
        pltpu.make_async_copy(gate_ref, weights.at[pl.ds(0, 2)], sems.at[0]),
        pltpu.make_async_copy(up_ref, weights.at[pl.ds(2, 2)], sems.at[1]),
    )
    for copy in copies:
        copy.start()
    for copy in copies:
        copy.wait()
    out_ref[0] = swiglu(normed_ref[...], [weights[page] for page in range(4)])


def far_units(normed, gate, up):
    count = normed.shape[0]
    _, model, half = gate.shape
    vmem = pl.BlockSpec(memory_space=pltpu.VMEM)
    anywhere = pl.BlockSpec(memory_space=pltpu.HBM)
    return pl.pallas_call(
        far_body,
        in_specs=[vmem, anywhere, anywhere],
        out_specs=vmem,
        out_shape=jax.ShapeDtypeStruct((1, count, 2 * half), jnp.bfloat16),
        scratch_shapes=[
            pltpu.VMEM((4, model, half), jnp.bfloat16),
            pltpu.SemaphoreType.DMA((2,)),
        ],
        compiler_params=pltpu.CompilerParams(vmem_limit_bytes=8 * 2**20),
        name="far",
    )(normed, gate, up)


def down_body(x_ref, units_ref, own_ref, right_ref, far_ref, left_ref, out_ref, downs, sems):
    blocks, count, hidden = units_ref.shape
    chips, pieces, rows_each, _ = out_ref.shape
    parts = sems.shape[0]
    half, share = own_ref.shape[1:]
    step = 2 * half // parts
    copies = []
    for c in range(parts):
        at = c * step
        rows = pl.ds(at, step)
        inner = pl.ds(at % half, step)
        page = at // half
        sources = (
            own_ref.at[2 + page, inner],
            right_ref.at[2 + page, inner],
            far_ref.at[page, inner],
            left_ref.at[2 + page, inner],
        )
        for k, source in enumerate(sources):
            copy = pltpu.make_async_copy(source, downs.at[k, rows], sems.at[c, k])
            copy.start()
            copies.append(copy)
    first = jnp.zeros((count, 2 * share), jnp.float32)
    second = jnp.zeros((count, 2 * share), jnp.float32)
    for p in range(blocks):
        if p % (blocks // parts) == 0:
            c = p // (blocks // parts)
            for copy in copies[c * pieces : (c + 1) * pieces]:
                copy.wait()
        ahead = (0, 1, 3, 2)[p % pieces]
        block = p // pieces * pieces + lax.rem(x_ref[0] + ahead, pieces)
        rows = pl.ds(pl.multiple_of(block * hidden, hidden), hidden)
        units = units_ref[p]
        near = jnp.concatenate([downs[0, rows], downs[1, rows]], axis=1)
        rest = jnp.concatenate([downs[2, rows], downs[3, rows]], axis=1)
        first += jnp.dot(units, near, preferred_element_type=jnp.float32)
        second += jnp.dot(units, rest, preferred_element_type=jnp.float32)
    made = (first[:, :share], first[:, share:], second[:, :share], second[:, share:])
    for ahead, value in enumerate(made):
        at = lax.rem(x_ref[0] + ahead, pieces)
        out_ref[:, at] = value.reshape(chips, rows_each, share).astype(jnp.bfloat16)


def down_product(x, units, chips, *downs):
    _, count, _ = units.shape
    _, half, share = downs[0].shape
    vmem = pl.BlockSpec(memory_space=pltpu.VMEM)
    anywhere = pl.BlockSpec(memory_space=pltpu.HBM)
    return pl.pallas_call(
        down_body,
        in_specs=[pl.BlockSpec(memory_space=pltpu.SMEM), vmem] + [anywhere] * len(downs),
        out_specs=vmem,
        out_shape=jax.ShapeDtypeStruct((chips, 4, count // chips, share), jnp.bfloat16),
        scratch_shapes=[
            pltpu.VMEM((4, 2 * half, share), jnp.bfloat16),
            pltpu.SemaphoreType.DMA((4, 4)),
        ],
        compiler_params=pltpu.CompilerParams(vmem_limit_bytes=10 * 2**20),
        name="down",
    )(x, units, *downs)


def assemble_body(whole_ref, out_ref):
    peers, _, share = whole_ref.shape
    for p in range(peers):
        out_ref[:, p * share : (p + 1) * share] = whole_ref[p]


def assemble(whole):
    peers, tok, share = whole.shape
    tile = tok // 4
    return pl.pallas_call(
        assemble_body,
        grid=(4,),
        in_specs=[pl.BlockSpec((peers, tile, share), lambda i: (0, i, 0))],
        out_specs=pl.BlockSpec((tile, peers * share), lambda i: (i, 0)),
        out_shape=jax.ShapeDtypeStruct((tok, peers * share), whole.dtype),
        compiler_params=pltpu.CompilerParams(
            dimension_semantics=("arbitrary",), vmem_limit_bytes=6 * 2**20
        ),
        name="assemble",
    )(whole)


def gathered(array, axes, axis, scale):
    sent = (array.astype(jnp.float32) * scale).astype(jnp.float16)
    whole = lax.all_gather(sent, axes, axis=axis, tiled=True)
    return (whole.astype(jnp.float32) * (1.0 / scale)).astype(jnp.bfloat16)


def shards(
    residual,
    queries,
    key_vectors,
    value_rows,
    head_lambda,
    head_gain,
    out_weight,
    ffn_gain,
    expert_gate,
    expert_up,
    expert_down,
    routing,
    route_weight,
):
    tok, _, _ = queries.shape
    experts = lax.axis_size("sp")
    across = lax.axis_size("x")
    along = lax.axis_size("y")
    tp = ("y", "x")
    peers = across * along
    model = residual.shape[1]
    share = model // peers
    where = lax.axis_index("sp").astype(jnp.int32)[None]
    x_at = lax.axis_index("x").astype(jnp.int32)[None]
    column = (lax.axis_index("y") * across + lax.axis_index("x")) * share

    ahead = [(i, (i + 1) % across) for i in range(across)]
    behind = [(i, (i - 1) % across) for i in range(across)]
    gate, up, down = expert_gate[0], expert_up[0], expert_down[0]
    packed = pack(gate, up, down)
    left = lax.ppermute(packed, "x", ahead)
    right = lax.ppermute(packed, "x", behind)
    gate_1, down_1, up_1 = cut(left, right)
    gate_2 = lax.ppermute(gate_1, "x", ahead)
    up_2 = lax.ppermute(up_1, "x", behind)
    down_2 = lax.ppermute(down_1, "x", ahead)

    kv = jnp.concatenate([key_vectors[:, 0], value_rows[:, 0]], axis=1)
    kv_all = gathered(kv, "sp", 0, SHIFT)
    own_residual = lax.dynamic_slice_in_dim(residual, column, share, 1)

    capacity = tok // (experts // GROUPS)
    order = jnp.arange(tok, dtype=jnp.int32)
    ids = jnp.arange(experts, dtype=jnp.int32)
    named = routing[:, :, None] == ids
    member = jnp.any(named, axis=1)
    strict = (order[None, :] < order[:, None]).astype(jnp.bfloat16)
    earlier = jnp.dot(
        strict, member.astype(jnp.bfloat16), preferred_element_type=jnp.float32
    ).astype(jnp.int32)
    place = jnp.where(member, earlier, -1).T
    picked = jnp.sum(jnp.where(named, earlier[:, None, :], 0), axis=2)
    slots = routing * capacity + picked

    partial = attention(
        where, head_lambda, queries[:, 0], kv_all, head_gain[None], out_weight, peers
    )
    parts = lax.all_to_all(partial, tp, 0, 0, tiled=True)
    own_stream, outgoing, slots, factors = project(
        parts, own_residual, place, slots, route_weight
    )
    targets = experts * across
    each = capacity // across
    landed = lax.all_to_all(outgoing.reshape(targets, each, share), ("sp", "x"), 0, 0, tiled=True)
    landed = arrange(landed.reshape(experts, across, each, share))
    rows = gathered(landed.reshape(across, experts * each, share), "y", 0, 64.0)
    near, normed = near_units(rows, ffn_gain[None], packed, right, left)
    far = far_units(normed, gate_2, up_2)
    units = jnp.concatenate([near, far], axis=0)
    all_units = gathered(units, "y", 0, 0.25)
    made = down_product(x_at, all_units, experts, packed, right, down_2, left)
    back = lax.all_to_all(
        made.reshape(targets, each, share), ("sp", "x"), 0, 0, tiled=True
    )
    back = back.reshape(experts * capacity, share)
    spread = combine(back, own_stream, slots, factors, peers)
    whole = lax.all_to_all(spread, tp, 0, 0, tiled=True)
    return assemble(whole)


def solution(mesh):
    sizes = mesh.devices.shape
    split = jax.sharding.Mesh(
        mesh.devices.reshape(sizes[0], sizes[1] // 4, 4), ("sp", "y", "x")
    )
    tp = ("y", "x")
    in_specs = (
        P("sp", None),
        P("sp", tp, None),
        P("sp", tp, None),
        P("sp", tp, None),
        P(tp),
        P(),
        P(tp, None),
        P(),
        P("sp", None, tp),
        P("sp", None, tp),
        P("sp", None, tp),
        P("sp", None),
        P("sp", None),
    )
    return jax.shard_map(
        shards, mesh=split, in_specs=in_specs, out_specs=P("sp", None), check_vma=False
    )
```

```python
import jax
import jax.numpy as jnp
from jax import lax
from jax.experimental import pallas as pl
from jax.experimental.pallas import tpu as pltpu
from jax.sharding import PartitionSpec as P

norm_eps = 1e-06
KEY_BLOCK = 2048
ROW_BLOCK = 128
SHIFT = 4096.0
GROUPS = 4


def attention_body(where_ref, lam_ref, q_ref, kv_ref, gain_ref, weight_ref, out_ref, stacked, highest, accum, parts, sems):
    tok, width = q_ref.shape
    first_query = where_ref[0] * tok
    last = (first_query + tok - 1) // KEY_BLOCK
    scaled = q_ref[...] * jnp.asarray((width // 2) ** -0.5, jnp.bfloat16)
    low = lax.broadcasted_iota(jnp.int32, scaled.shape, 1) < width // 2
    zero = jnp.zeros_like(scaled)
    stacked[:tok] = jnp.where(low, scaled, zero)
    stacked[tok:] = jnp.where(low, zero, scaled)
    highest[...] = jnp.full(highest.shape, -1e30, jnp.float32)
    accum[...] = jnp.zeros(accum.shape, jnp.float32)

    def update(step, masked):
        block = kv_ref[pl.ds(pl.multiple_of(step * KEY_BLOCK, KEY_BLOCK), KEY_BLOCK), :]
        keys, values = block[:, :width], block[:, width:]
        wide = jnp.concatenate([values, jnp.ones_like(values)], axis=1)
        for at in range(0, 2 * tok, ROW_BLOCK):
            rows = slice(at, at + ROW_BLOCK)
            scores = lax.dot_general(
                stacked[rows], keys, (((1,), (1,)), ((), ())), preferred_element_type=jnp.float32
            )
            if masked:
                row = lax.broadcasted_iota(jnp.int32, scores.shape, 0) + at % tok
                col = lax.broadcasted_iota(jnp.int32, scores.shape, 1)
                scores = jnp.where(
                    col - row <= first_query - step * KEY_BLOCK, scores, -1e30
                )
            before = highest[rows]
            now = jnp.maximum(before, jnp.max(scores, axis=1, keepdims=True))
            weights = jnp.exp(scores - now[:, :1])
            shrink = jnp.exp(before - now)[:, :1]
            blended = jnp.dot(weights.astype(jnp.bfloat16), wide, preferred_element_type=jnp.float32)
            accum[rows] = accum[rows] * shrink + blended
            highest[rows] = now

    def whole(step, carry):
        update(step, False)
        return carry

    lax.fori_loop(0, last, whole, 0)
    update(last, True)
    both = accum[:, :width] / accum[:, width:]
    combined = both[:tok] - lam_ref[0] * both[tok:]
    square = jnp.mean(combined * combined, axis=1, keepdims=True)
    attended = (combined * lax.rsqrt(square + norm_eps) * gain_ref[...]).astype(jnp.bfloat16)
    share = out_ref.shape[2]
    copies = []
    for p in range(0, out_ref.shape[0], 2):
        cols = weight_ref[:, p * share : (p + 2) * share]
        part = jnp.dot(attended, cols, preferred_element_type=jnp.float32).astype(jnp.bfloat16)
        parts[p] = part[:, :share]
        parts[p + 1] = part[:, share:]
        copy = pltpu.make_async_copy(
            parts.at[pl.ds(p, 2)], out_ref.at[pl.ds(p, 2)], sems.at[p // 2]
        )
        copy.start()
        copies.append(copy)
    for copy in copies:
        copy.wait()


def attention(where, lam, q, kv, gain, weight, peers):
    tok, width = q.shape
    share = weight.shape[1] // peers
    vmem = pl.BlockSpec(memory_space=pltpu.VMEM)
    smem = pl.BlockSpec(memory_space=pltpu.SMEM)
    return pl.pallas_call(
        attention_body,
        in_specs=[smem, smem, vmem, vmem, vmem, vmem],
        out_specs=pl.BlockSpec(memory_space=pltpu.HBM),
        out_shape=jax.ShapeDtypeStruct((peers, tok, share), jnp.bfloat16),
        scratch_shapes=[
            pltpu.VMEM((2 * tok, width), jnp.bfloat16),
            pltpu.VMEM((2 * tok, 128), jnp.float32),
            pltpu.VMEM((2 * tok, 2 * width), jnp.float32),
            pltpu.VMEM((peers, tok, share), jnp.bfloat16),
            pltpu.SemaphoreType.DMA((peers // 2,)),
        ],
        compiler_params=pltpu.CompilerParams(vmem_limit_bytes=14 * 2**20),
        name="attention",
    )(where, lam, q, kv, gain, weight)


def pack_body(gate_ref, up_ref, down_ref, out_ref, sems):
    rows, width = out_ref.shape[1:]
    low, high = pl.ds(0, width), pl.ds(width, width)
    sources = (
        gate_ref.at[:, low],
        gate_ref.at[:, high],
        down_ref.at[pl.ds(0, rows)],
        down_ref.at[pl.ds(rows, rows)],
        up_ref.at[:, low],
        up_ref.at[:, high],
    )
    copies = [
        pltpu.make_async_copy(source, out_ref.at[k], sems.at[k])
        for k, source in enumerate(sources)
    ]
    for copy in copies:
        copy.start()
    for copy in copies:
        copy.wait()


def pack(gate, up, down):
    model, hidden = gate.shape
    return pl.pallas_call(
        pack_body,
        in_specs=[pl.BlockSpec(memory_space=pltpu.HBM)] * 3,
        out_specs=pl.BlockSpec(memory_space=pltpu.HBM),
        out_shape=jax.ShapeDtypeStruct((6, model, hidden // 2), gate.dtype),
        scratch_shapes=[pltpu.SemaphoreType.DMA((6,))],
        compiler_params=pltpu.CompilerParams(vmem_limit_bytes=4 * 2**20),
        name="pack",
    )(gate, up, down)


def cut_body(left_ref, right_ref, gate_ref, down_ref, up_ref, sems):
    copies = (
        pltpu.make_async_copy(left_ref.at[pl.ds(0, 2)], gate_ref, sems.at[0]),
        pltpu.make_async_copy(right_ref.at[pl.ds(4, 2)], up_ref, sems.at[1]),
        pltpu.make_async_copy(left_ref.at[pl.ds(2, 2)], down_ref, sems.at[2]),
    )
    for copy in copies:
        copy.start()
    for copy in copies:
        copy.wait()


def cut(left, right):
    _, model, half = left.shape
    anywhere = pl.BlockSpec(memory_space=pltpu.HBM)
    return pl.pallas_call(
        cut_body,
        in_specs=[anywhere] * 2,
        out_specs=[pl.BlockSpec(memory_space=pltpu.VMEM)] * 3,
        out_shape=[jax.ShapeDtypeStruct((2, model, half), left.dtype)] * 3,
        scratch_shapes=[pltpu.SemaphoreType.DMA((3,))],
        compiler_params=pltpu.CompilerParams(vmem_limit_bytes=6 * 2**20),
        name="cut",
    )(left, right)


def arrange_body(landed_ref, out_ref):
    for k in range(out_ref.shape[0]):
        out_ref[k] = landed_ref[:, k]


def arrange(landed):
    experts, across, each, share = landed.shape
    vmem = pl.BlockSpec(memory_space=pltpu.VMEM)
    return pl.pallas_call(
        arrange_body,
        in_specs=[vmem],
        out_specs=vmem,
        out_shape=jax.ShapeDtypeStruct((across, experts, each, share), landed.dtype),
        compiler_params=pltpu.CompilerParams(vmem_limit_bytes=2 * 2**20),
        name="arrange",
    )(landed)


def project_body(parts_ref, residual_ref, place_ref, slots_ref, factors_ref, stream_ref, out_ref, slots_out, factors_out):
    slots_out[...] = slots_ref[...]
    factors_out[...] = factors_ref[...]
    total = residual_ref[...].astype(jnp.float32)
    for p in range(parts_ref.shape[0]):
        total += parts_ref[p].astype(jnp.float32)
    stream_ref[...] = total
    rows = total.astype(jnp.bfloat16)
    experts, tok = place_ref.shape
    capacity = out_ref.shape[0] // experts
    slot = lax.broadcasted_iota(jnp.int32, (capacity, tok), 0)
    for first in range(0, experts, 8):
        send = [
            jnp.where(place_ref[e : e + 1, :] == slot, 1.0, 0.0).astype(jnp.bfloat16)
            for e in range(first, first + 8)
        ]
        picked = jnp.dot(jnp.concatenate(send, axis=0), rows, preferred_element_type=jnp.float32)
        out_ref[first * capacity : (first + 8) * capacity] = picked.astype(jnp.bfloat16)


def project(parts, residual, place, slots, factors):
    _, tok, share = parts.shape
    experts = place.shape[0]
    rows = tok // (experts // GROUPS) * experts
    vmem = pl.BlockSpec(memory_space=pltpu.VMEM)
    return pl.pallas_call(
        project_body,
        in_specs=[vmem] * 5,
        out_specs=[vmem] * 4,
        out_shape=[
            jax.ShapeDtypeStruct((tok, share), jnp.float32),
            jax.ShapeDtypeStruct((rows, share), jnp.bfloat16),
            jax.ShapeDtypeStruct(slots.shape, slots.dtype),
            jax.ShapeDtypeStruct(factors.shape, factors.dtype),
        ],
        compiler_params=pltpu.CompilerParams(vmem_limit_bytes=6 * 2**20),
        name="project",
    )(parts, residual, place, slots, factors)


def combine_body(back_ref, stream_ref, slots_ref, factors_ref, out_ref):
    tok = stream_ref.shape[0]
    rows = back_ref.shape[0]
    slot = lax.broadcasted_iota(jnp.int32, (tok, rows), 1)
    total = stream_ref[...]
    for k in range(slots_ref.shape[1]):
        take = jnp.where(slots_ref[:, k : k + 1] == slot, 1.0, 0.0).astype(jnp.bfloat16)
        found = jnp.dot(take, back_ref[...], preferred_element_type=jnp.float32)
        total += factors_ref[:, k : k + 1] * found
    done = total.astype(jnp.bfloat16)
    for p in range(out_ref.shape[0]):
        out_ref[p] = done


def combine(back, stream, slots, factors, peers):
    tok, share = stream.shape
    vmem = pl.BlockSpec(memory_space=pltpu.VMEM)
    return pl.pallas_call(
        combine_body,
        in_specs=[vmem] * 4,
        out_specs=vmem,
        out_shape=jax.ShapeDtypeStruct((peers, tok, share), jnp.bfloat16),
        compiler_params=pltpu.CompilerParams(vmem_limit_bytes=8 * 2**20),
        name="combine",
    )(back, stream, slots, factors)


def swiglu(normed, pages):
    gates = jnp.concatenate([pages[0], pages[1]], axis=1)
    ups = jnp.concatenate([pages[2], pages[3]], axis=1)
    gate = jnp.dot(normed, gates, preferred_element_type=jnp.float32)
    up = jnp.dot(normed, ups, preferred_element_type=jnp.float32)
    return (gate / (1.0 + jnp.exp(-gate)) * up).astype(jnp.bfloat16)


def near_body(rows_ref, gain_ref, own_ref, right_ref, left_ref, out_ref, normed_ref, weights, sems):
    peers, count, share = rows_ref.shape
    gate, up = pl.ds(0, 2), pl.ds(4, 2)
    first, second = pl.ds(0, 2), pl.ds(2, 2)
    copies = []
    for k, source in enumerate((own_ref, right_ref, left_ref)):
        pair = (
            pltpu.make_async_copy(source.at[gate], weights.at[k, first], sems.at[k, 0]),
            pltpu.make_async_copy(source.at[up], weights.at[k, second], sems.at[k, 1]),
        )
        for copy in pair:
            copy.start()
        copies.append(pair)
    total = jnp.zeros((count, 1), jnp.float32)
    for p in range(peers):
        part = rows_ref[p].astype(jnp.float32)
        total += jnp.sum(part * part, axis=1, keepdims=True)
    scale = lax.rsqrt(total / (peers * share) + norm_eps)
    for p in range(peers):
        cols = slice(p * share, (p + 1) * share)
        normed_ref[:, cols] = (rows_ref[p].astype(jnp.float32) * scale * gain_ref[:, cols]).astype(
            jnp.bfloat16
        )
    for k, pair in enumerate(copies):
        for copy in pair:
            copy.wait()
        out_ref[k] = swiglu(normed_ref[...], [weights[k, page] for page in range(4)])


def near_units(rows, gain, *sources):
    peers, count, share = rows.shape
    _, model, half = sources[0].shape
    vmem = pl.BlockSpec(memory_space=pltpu.VMEM)
    anywhere = pl.BlockSpec(memory_space=pltpu.HBM)
    return pl.pallas_call(
        near_body,
        in_specs=[vmem, vmem] + [anywhere] * len(sources),
        out_specs=[vmem, vmem],
        out_shape=[
            jax.ShapeDtypeStruct((len(sources), count, 2 * half), jnp.bfloat16),
            jax.ShapeDtypeStruct((count, peers * share), jnp.bfloat16),
        ],
        scratch_shapes=[
            pltpu.VMEM((len(sources), 4, model, half), jnp.bfloat16),
            pltpu.SemaphoreType.DMA((len(sources), 2)),
        ],
        compiler_params=pltpu.CompilerParams(vmem_limit_bytes=16 * 2**20),
        name="near",
    )(rows, gain, *sources)


def far_body(normed_ref, gate_ref, up_ref, out_ref, weights, sems):
    copies = (
        pltpu.make_async_copy(gate_ref, weights.at[pl.ds(0, 2)], sems.at[0]),
        pltpu.make_async_copy(up_ref, weights.at[pl.ds(2, 2)], sems.at[1]),
    )
    for copy in copies:
        copy.start()
    for copy in copies:
        copy.wait()
    out_ref[0] = swiglu(normed_ref[...], [weights[page] for page in range(4)])


def far_units(normed, gate, up):
    count = normed.shape[0]
    _, model, half = gate.shape
    vmem = pl.BlockSpec(memory_space=pltpu.VMEM)
    anywhere = pl.BlockSpec(memory_space=pltpu.HBM)
    return pl.pallas_call(
        far_body,
        in_specs=[vmem, anywhere, anywhere],
        out_specs=vmem,
        out_shape=jax.ShapeDtypeStruct((1, count, 2 * half), jnp.bfloat16),
        scratch_shapes=[
            pltpu.VMEM((4, model, half), jnp.bfloat16),
            pltpu.SemaphoreType.DMA((2,)),
        ],
        compiler_params=pltpu.CompilerParams(vmem_limit_bytes=8 * 2**20),
        name="far",
    )(normed, gate, up)


def down_body(x_ref, units_ref, own_ref, right_ref, far_ref, left_ref, out_ref, downs, sems):
    blocks, count, hidden = units_ref.shape
    chips, pieces, rows_each, _ = out_ref.shape
    parts = sems.shape[0]
    half, share = own_ref.shape[1:]
    step = 2 * half // parts
    copies = []
    for c in range(parts):
        at = c * step
        rows = pl.ds(at, step)
        inner = pl.ds(at % half, step)
        page = at // half
        sources = (
            own_ref.at[2 + page, inner],
            right_ref.at[2 + page, inner],
            far_ref.at[page, inner],
            left_ref.at[2 + page, inner],
        )
        for k, source in enumerate(sources):
            copy = pltpu.make_async_copy(source, downs.at[k, rows], sems.at[c, k])
            copy.start()
            copies.append(copy)
    first = jnp.zeros((count, 2 * share), jnp.float32)
    second = jnp.zeros((count, 2 * share), jnp.float32)
    for p in range(blocks):
        if p % (blocks // parts) == 0:
            c = p // (blocks // parts)
            for copy in copies[c * pieces : (c + 1) * pieces]:
                copy.wait()
        ahead = (0, 1, 3, 2)[p % pieces]
        block = p // pieces * pieces + lax.rem(x_ref[0] + ahead, pieces)
        rows = pl.ds(pl.multiple_of(block * hidden, hidden), hidden)
        units = units_ref[p]
        near = jnp.concatenate([downs[0, rows], downs[1, rows]], axis=1)
        rest = jnp.concatenate([downs[2, rows], downs[3, rows]], axis=1)
        first += jnp.dot(units, near, preferred_element_type=jnp.float32)
        second += jnp.dot(units, rest, preferred_element_type=jnp.float32)
    made = (first[:, :share], first[:, share:], second[:, :share], second[:, share:])
    for ahead, value in enumerate(made):
        at = lax.rem(x_ref[0] + ahead, pieces)
        out_ref[:, at] = value.reshape(chips, rows_each, share).astype(jnp.bfloat16)


def down_product(x, units, chips, *downs):
    _, count, _ = units.shape
    _, half, share = downs[0].shape
    vmem = pl.BlockSpec(memory_space=pltpu.VMEM)
    anywhere = pl.BlockSpec(memory_space=pltpu.HBM)
    return pl.pallas_call(
        down_body,
        in_specs=[pl.BlockSpec(memory_space=pltpu.SMEM), vmem] + [anywhere] * len(downs),
        out_specs=vmem,
        out_shape=jax.ShapeDtypeStruct((chips, 4, count // chips, share), jnp.bfloat16),
        scratch_shapes=[
            pltpu.VMEM((4, 2 * half, share), jnp.bfloat16),
            pltpu.SemaphoreType.DMA((4, 4)),
        ],
        compiler_params=pltpu.CompilerParams(vmem_limit_bytes=10 * 2**20),
        name="down",
    )(x, units, *downs)


def assemble_body(whole_ref, out_ref):
    peers, _, share = whole_ref.shape
    for p in range(peers):
        out_ref[:, p * share : (p + 1) * share] = whole_ref[p]


def assemble(whole):
    peers, tok, share = whole.shape
    vmem = pl.BlockSpec(memory_space=pltpu.VMEM)
    return pl.pallas_call(
        assemble_body,
        in_specs=[vmem],
        out_specs=vmem,
        out_shape=jax.ShapeDtypeStruct((tok, peers * share), whole.dtype),
        compiler_params=pltpu.CompilerParams(vmem_limit_bytes=6 * 2**20),
        name="assemble",
    )(whole)


def gathered(array, axes, axis, scale):
    sent = (array.astype(jnp.float32) * scale).astype(jnp.float16)
    whole = lax.all_gather(sent, axes, axis=axis, tiled=True)
    return (whole.astype(jnp.float32) * (1.0 / scale)).astype(jnp.bfloat16)


def shards(
    residual,
    queries,
    key_vectors,
    value_rows,
    head_lambda,
    head_gain,
    out_weight,
    ffn_gain,
    expert_gate,
    expert_up,
    expert_down,
    routing,
    route_weight,
):
    tok, _, _ = queries.shape
    experts = lax.axis_size("sp")
    across = lax.axis_size("x")
    along = lax.axis_size("y")
    tp = ("y", "x")
    peers = across * along
    model = residual.shape[1]
    share = model // peers
    where = lax.axis_index("sp").astype(jnp.int32)[None]
    x_at = lax.axis_index("x").astype(jnp.int32)[None]
    column = (lax.axis_index("y") * across + lax.axis_index("x")) * share

    ahead = [(i, (i + 1) % across) for i in range(across)]
    behind = [(i, (i - 1) % across) for i in range(across)]
    gate, up, down = expert_gate[0], expert_up[0], expert_down[0]
    packed = pack(gate, up, down)
    left = lax.ppermute(packed, "x", ahead)
    right = lax.ppermute(packed, "x", behind)
    gate_1, down_1, up_1 = cut(left, right)
    gate_2 = lax.ppermute(gate_1, "x", ahead)
    up_2 = lax.ppermute(up_1, "x", behind)
    down_2 = lax.ppermute(down_1, "x", ahead)

    kv = jnp.concatenate([key_vectors[:, 0], value_rows[:, 0]], axis=1)
    kv_all = gathered(kv, "sp", 0, SHIFT)
    own_residual = lax.dynamic_slice_in_dim(residual, column, share, 1)

    capacity = tok // (experts // GROUPS)
    order = jnp.arange(tok, dtype=jnp.int32)
    ids = jnp.arange(experts, dtype=jnp.int32)
    named = routing[:, :, None] == ids
    member = jnp.any(named, axis=1)
    strict = (order[None, :] < order[:, None]).astype(jnp.bfloat16)
    earlier = jnp.dot(
        strict, member.astype(jnp.bfloat16), preferred_element_type=jnp.float32
    ).astype(jnp.int32)
    place = jnp.where(member, earlier, -1).T
    picked = jnp.sum(jnp.where(named, earlier[:, None, :], 0), axis=2)
    slots = routing * capacity + picked

    partial = attention(
        where, head_lambda, queries[:, 0], kv_all, head_gain[None], out_weight, peers
    )
    parts = lax.all_to_all(partial, tp, 0, 0, tiled=True)
    own_stream, outgoing, slots, factors = project(
        parts, own_residual, place, slots, route_weight
    )
    targets = experts * across
    each = capacity // across
    landed = lax.all_to_all(outgoing.reshape(targets, each, share), ("sp", "x"), 0, 0, tiled=True)
    landed = arrange(landed.reshape(experts, across, each, share))
    rows = gathered(landed.reshape(across, experts * each, share), "y", 0, 64.0)
    near, normed = near_units(rows, ffn_gain[None], packed, right, left)
    far = far_units(normed, gate_2, up_2)
    units = jnp.concatenate([near, far], axis=0)
    all_units = gathered(units, "y", 0, 0.25)
    made = down_product(x_at, all_units, experts, packed, right, down_2, left)
    back = lax.all_to_all(
        made.reshape(targets, each, share), ("sp", "x"), 0, 0, tiled=True
    )
    back = back.reshape(experts * capacity, share)
    spread = combine(back, own_stream, slots, factors, peers)
    whole = lax.all_to_all(spread, tp, 0, 0, tiled=True)
    return assemble(whole)


def solution(mesh):
    sizes = mesh.devices.shape
    split = jax.sharding.Mesh(
        mesh.devices.reshape(sizes[0], sizes[1] // 4, 4), ("sp", "y", "x")
    )
    tp = ("y", "x")
    in_specs = (
        P("sp", None),
        P("sp", tp, None),
        P("sp", tp, None),
        P("sp", tp, None),
        P(tp),
        P(),
        P(tp, None),
        P(),
        P("sp", None, tp),
        P("sp", None, tp),
        P("sp", None, tp),
        P("sp", None),
        P("sp", None),
    )
    return jax.shard_map(
        shards, mesh=split, in_specs=in_specs, out_specs=P("sp", None), check_vma=False
    )
```
